512 devices in a mesh: sp: 16 (over z), fs: 4 (over y), tp: 8 (over x, core).
Axes of the slice: x: 4, y: 4, z: 16, core: 2. Of those that a mesh axis runs over, the one named last changes fastest.
Arguments:
- tokens: bfloat16 [24576, 2048], P(('fs', 'sp', 'tp')), parts along dimension 0, may hold values from -6 to 6
- norm_gain: float32 [2048], replicated, may hold values from 0.1 to 1.9
- w_input: bfloat16 [2048, 1024], P(None, 'tp'), may hold values from -0.125 to 0.125
- w_query: bfloat16 [2048, 1024], P(None, 'tp'), may hold values from -0.125 to 0.125
- w_key: bfloat16 [2048, 1024], P(None, 'tp'), may hold values from -0.125 to 0.125
- w_value: bfloat16 [2048, 1024], P(None, 'tp'), may hold values from -0.125 to 0.125
- query_gain: float32 [64], replicated, may hold values from 0.1 to 1.9
- key_gain: float32 [64], replicated, may hold values from 0.1 to 1.9
- key_bias: bfloat16 [24576, 16], P(('fs', 'sp'), 'tp'), parts along dimension 0, may hold values from -16 to 0
- eigen_real: float32 [64, 64], P('tp'), may hold values from -32 to 0
- eigen_imag: float32 [64, 64], P('tp'), may hold values from 0.31 to 201.0624
- log_step: float32 [64], P('tp'), may hold values from -6.91 to -2.3
- input_real: float32 [64, 64, 16], P('tp'), may hold values from -1 to 1
- input_imag: float32 [64, 64, 16], P('tp'), may hold values from -1 to 1
- read_real: float32 [64, 16, 64], P('tp'), may hold values from -0.75 to 0.75
- read_imag: float32 [64, 16, 64], P('tp'), may hold values from -0.75 to 0.75
- skip_gain: float32 [1024], P('tp'), may hold values from -6 to 6
- w_out_state: bfloat16 [1024, 2048], P('tp'), may hold values from -0.125 to 0.125
- w_out_attn: bfloat16 [1024, 2048], P('tp'), may hold values from -0.125 to 0.125
Outputs:
- layer_out: bfloat16 [24576, 2048], P(('fs', 'sp', 'tp')), parts along dimension 0
The draws below stay inside these ranges and needn't reach their ends.
There are 4 independent parts, one for each index of `fs`. The reference program is written for one: setup_inputs(seed, part) draws one part's arguments, and reference() takes and returns one part's arrays. A program takes and returns all parts, laid end to end along the dimension named above; an argument that names none is the same for every part. Nothing has to cross between parts.
All inputs are finite; a program needn't handle non-finite values.
Results may differ from the reference program's by a relative error of at most 0.014.
Values may be sent and summed in bfloat16 or wider, within the bound.
No kernel may reach another device: no remote copies, remote signals or barrier semaphores. Data moves between devices by JAX's collectives and lax.ppermute only.
A program may use at most 64 MiB of HBM per device.

```python
import math
import jax
import jax.numpy as jnp
from jax import lax

D = 2048
GROUP = 16
GROUPS = 64
STATE = 64
HEADS = 16
HEAD_DIM = 64
TOK_DEV = 384
STATE_WIDTH = 1024
ATTN_WIDTH = 1024
SEQ = 6144
N_SP = 16
N_TP = 8


def draw_key_bias(key, part):
    rate_key, block_key, jitter_key, place_key, size_key = jax.random.split(jax.random.fold_in(key, 31), 5)
    ceiling = math.log(1.0 / 32.0)
    log_rates = jax.random.uniform(rate_key, (HEADS,), jnp.float32, math.log(0.05 / SEQ), ceiling)
    block_shift = jax.random.uniform(block_key, (SEQ // TOK_DEV, HEADS), jnp.float32, -0.7, 0.7)
    jitter = jax.random.uniform(jitter_key, (SEQ, HEADS), jnp.float32, -0.5, 0.5)
    reference_level = log_rates[None, :] + jnp.repeat(block_shift, TOK_DEV, axis=0) + jitter
    places = jax.random.randint(place_key, (3,), 0, SEQ)
    mixing_intensity = jax.random.uniform(size_key, (3, HEADS), jnp.float32, -1.4, -0.4)
    flagged_entries = (jnp.arange(SEQ)[:, None] == places[None, :]).astype(jnp.float32)
    tallied_count = jnp.sum(flagged_entries, axis=1, keepdims=True)
    spike_groups = jnp.dot(flagged_entries, mixing_intensity) / jnp.maximum(tallied_count, 1.0)
    return jnp.where(tallied_count > 0, spike_groups, reference_level).astype(jnp.bfloat16)


def state_rates(key):
    step_key, rate_key = jax.random.split(jax.random.fold_in(key, 47))
    log_step = jax.random.uniform(step_key, (GROUPS,), jnp.float32, math.log(0.001), math.log(0.1))
    ceiling = math.log(1.0 / 32.0)
    log_rates = jax.random.uniform(rate_key, (GROUPS, STATE), jnp.float32, math.log(0.05 / SEQ), ceiling)
    return (log_step, -jnp.exp(log_rates - log_step[:, None]))


def draw_eigen_real(key, part):
    return state_rates(key)[1]


def draw_log_step(key, part):
    return state_rates(key)[0]


def draw_eigen_imag(key, part):
    offsets = jax.random.uniform(jax.random.fold_in(key, 53), (GROUPS, STATE), jnp.float32, -0.4, 0.4)
    return math.pi * (jnp.arange(STATE, dtype=jnp.float32)[None, :] + 0.5 + offsets)


def steps_of(key, dims, pieces, low, high):
    factor_of = 1.0
    for axis_at, shards_of in pieces:
        draws = jax.random.uniform(jax.random.fold_in(jax.random.fold_in(key, 6), axis_at), (shards_of,), jnp.float32, low / len(pieces), high / len(pieces))
        factor_of = factor_of * jnp.repeat(jnp.exp(draws), dims[axis_at] // shards_of).reshape((-1,) + (1,) * (len(dims) - 1 - axis_at))
    return factor_of


def noise(stream_key, dims, scale, limit, cuts=(), kind=jnp.bfloat16):
    entries = jax.random.normal(stream_key, dims, jnp.float32) * scale
    if len(cuts) > 0:
        entries = steps_of(stream_key, dims, cuts, -0.22, 0.18) * entries
    return jnp.clip(entries, min=-limit, max=limit).astype(kind)


def setup_inputs(seed: int = 0, part: int = 0) -> dict:
    splits = jax.random.split(jax.random.key(seed), 20)
    part_splits = jax.random.split(jax.random.fold_in(splits[19], part), 20)
    return {
        "tokens": noise(part_splits[0], (SEQ, D), 1.0, 6.0, ((0, 128),)),
        "norm_gain": jnp.clip(1.0 + 0.18 * jax.random.normal(splits[1], (D,), jnp.float32), 0.1, 1.9),
        "w_input": noise(splits[2], (D, STATE_WIDTH), D ** -0.5, 0.125, ((1, 8),)),
        "w_query": noise(splits[3], (D, ATTN_WIDTH), D ** -0.5, 0.125, ((1, 8),)),
        "w_key": noise(splits[4], (D, ATTN_WIDTH), D ** -0.5, 0.125, ((1, 8),)),
        "w_value": noise(splits[5], (D, ATTN_WIDTH), D ** -0.5, 0.125, ((1, 8),)),
        "query_gain": jnp.clip(1.0 + 0.18 * jax.random.normal(splits[6], (HEAD_DIM,), jnp.float32), 0.1, 1.9),
        "key_gain": jnp.clip(1.0 + 0.18 * jax.random.normal(splits[7], (HEAD_DIM,), jnp.float32), 0.1, 1.9),
        "key_bias": draw_key_bias(jax.random.fold_in(jax.random.fold_in(splits[19], part), 71), part),
        "eigen_real": draw_eigen_real(jax.random.fold_in(splits[19], 71), part),
        "eigen_imag": draw_eigen_imag(jax.random.fold_in(splits[19], 71), part),
        "log_step": draw_log_step(jax.random.fold_in(splits[19], 71), part),
        "input_real": noise(splits[12], (GROUPS, STATE, GROUP), (2 * GROUP) ** -0.5, 1.0, ((0, 8),), jnp.float32),
        "input_imag": noise(splits[13], (GROUPS, STATE, GROUP), (2 * GROUP) ** -0.5, 1.0, ((0, 8),), jnp.float32),
        "read_real": noise(splits[14], (GROUPS, GROUP, STATE), STATE ** -0.5, 0.75, ((0, 8),), jnp.float32),
        "read_imag": noise(splits[15], (GROUPS, GROUP, STATE), STATE ** -0.5, 0.75, ((0, 8),), jnp.float32),
        "skip_gain": noise(splits[16], (STATE_WIDTH,), 1.0, 6.0, ((0, 8),), jnp.float32),
        "w_out_state": noise(splits[17], (STATE_WIDTH, D), (STATE_WIDTH + ATTN_WIDTH) ** -0.5, 0.125, ((0, 8),)),
        "w_out_attn": noise(splits[18], (ATTN_WIDTH, D), (STATE_WIDTH + ATTN_WIDTH) ** -0.5, 0.125, ((0, 8),)),
    }


EPSILON = 1e-06
PRECISE = lax.Precision.HIGHEST

def combine_states(earlier, later):
    leading_real_factor, first_ai, first_br, first_bi = earlier
    second_ar, second_ai, second_br, second_bi = later
    prod_r = second_ar * leading_real_factor - second_ai * first_ai
    prod_i = second_ar * first_ai + second_ai * leading_real_factor
    state_r = second_ar * first_br - second_ai * first_bi + second_br
    state_i = second_ar * first_bi + second_ai * first_br + second_bi
    return (prod_r, prod_i, state_r, state_i)

def discretize(eigen_real, eigen_imag, log_step, input_real, input_imag):
    step_size = jnp.exp(log_step)[:, None]
    rotation = eigen_imag * step_size
    shrink = jnp.expm1(eigen_real * step_size)
    cosine = jnp.cos(rotation)
    sine_part = jnp.sin(rotation)
    decay_r = (1.0 + shrink) * cosine
    decay_i = (1.0 + shrink) * sine_part
    minus_r = shrink * cosine - 2.0 * jnp.square(jnp.sin(0.5 * rotation))
    modulus = jnp.square(eigen_real) + jnp.square(eigen_imag)
    factor_r = (minus_r * eigen_real + decay_i * eigen_imag) / modulus
    factor_i = (decay_i * eigen_real - minus_r * eigen_imag) / modulus
    drive_r = factor_r[..., None] * input_real - factor_i[..., None] * input_imag
    drive_i = factor_r[..., None] * input_imag + factor_i[..., None] * input_real
    return (decay_r, decay_i, drive_r, drive_i)

def head_scale(flat_rows, head_gain):
    row_count = flat_rows.shape[0]
    shaped = flat_rows.astype(jnp.float32).reshape(row_count, HEADS, HEAD_DIM)
    scaled = shaped * lax.rsqrt(lax.optimization_barrier(jnp.mean(jnp.square(shaped), axis=-1, keepdims=True)) + EPSILON)
    return (scaled * head_gain).astype(jnp.bfloat16)

def block_terms(queries, key_rows, value_rows, bias_rows, q_first, k_first):
    scores = jnp.einsum('qhd,khd->hqk', queries.astype(jnp.float32), key_rows.astype(jnp.float32))
    scores = scores * HEAD_DIM ** (-0.5) + jnp.transpose(bias_rows.astype(jnp.float32))[:, None, :]
    query_place = q_first + jnp.arange(queries.shape[0], dtype=jnp.int32)
    key_place = k_first + jnp.arange(key_rows.shape[0], dtype=jnp.int32)
    causal = (key_place[None, :] < query_place[:, None])[None]
    log_keep = jnp.where(causal, jax.nn.log_sigmoid(-scores), 0.0)
    trailing_sum = lax.cumsum(log_keep, axis=2, reverse=True) - log_keep
    weights = jnp.where(causal, jnp.exp(jax.nn.log_sigmoid(scores) + trailing_sum), 0.0).astype(jnp.bfloat16)
    block_out = jnp.einsum('hqk,khd->qhd', weights.astype(jnp.float32), value_rows.astype(jnp.float32))
    return (block_out, lax.optimization_barrier(jnp.sum(log_keep, axis=2)))

def attention_branch(queries, key_heads, value_heads, key_bias):
    query_blocks = queries.reshape(N_SP, TOK_DEV, HEADS, HEAD_DIM)

    def one_query_block(operands):
        block_q, index = operands
        q_first = index * TOK_DEV

        def back_step(back_idx, carried):
            accumulated, later_sum = carried
            k_first = (index - back_idx) * TOK_DEV
            block_keys = lax.dynamic_slice_in_dim(key_heads, k_first, TOK_DEV, 0)
            block_values = lax.dynamic_slice_in_dim(value_heads, k_first, TOK_DEV, 0)
            block_bias = lax.dynamic_slice_in_dim(key_bias, k_first, TOK_DEV, 0)
            block_out, totals = block_terms(block_q, block_keys, block_values, block_bias, q_first, k_first)
            accumulated = accumulated + block_out * jnp.transpose(jnp.exp(later_sum))[:, :, None]
            return (accumulated, later_sum + totals)
        start_state = (jnp.zeros((TOK_DEV, HEADS, HEAD_DIM), jnp.float32), jnp.zeros((HEADS, TOK_DEV), jnp.float32))
        accumulated, _ = lax.fori_loop(0, index + 1, back_step, start_state)
        normed = accumulated * lax.rsqrt(lax.optimization_barrier(jnp.mean(jnp.square(accumulated), axis=-1, keepdims=True)) + EPSILON)
        return normed.astype(jnp.bfloat16)
    outputs = lax.map(one_query_block, (query_blocks, jnp.arange(N_SP, dtype=jnp.int32)))
    return outputs.reshape(SEQ, HEADS * HEAD_DIM)

def state_branch(inputs, eigen_real, eigen_imag, log_step, input_real, input_imag, read_real, read_imag, skip_gain):
    decay_r, decay_i, drive_r, drive_i = discretize(eigen_real, eigen_imag, log_step, input_real, input_imag)
    inputs_wide = inputs.astype(jnp.float32)
    grouped = jnp.transpose(inputs_wide.reshape(SEQ, GROUPS, GROUP), (1, 0, 2))

    def one_group(operands):
        group_in, dec_r, dec_i, drv_r, drv_i, rd_r, rd_i = operands
        push_r = jnp.dot(group_in, jnp.transpose(drv_r), precision=PRECISE, preferred_element_type=jnp.float32)
        push_i = jnp.dot(group_in, jnp.transpose(drv_i), precision=PRECISE, preferred_element_type=jnp.float32)
        steps_r = jnp.broadcast_to(dec_r[None, :], push_r.shape)
        steps_i = jnp.broadcast_to(dec_i[None, :], push_i.shape)
        running = lax.associative_scan(combine_states, (steps_r, steps_i, push_r, push_i), axis=0)
        real_read = jnp.dot(running[2], jnp.transpose(rd_r), precision=PRECISE, preferred_element_type=jnp.float32)
        imag_read = jnp.dot(running[3], jnp.transpose(rd_i), precision=PRECISE, preferred_element_type=jnp.float32)
        return real_read - imag_read
    outputs = lax.map(one_group, (grouped, decay_r, decay_i, drive_r, drive_i, read_real, read_imag))
    readout = jnp.transpose(outputs, (1, 0, 2)).reshape(SEQ, GROUPS * GROUP)
    return jax.nn.gelu(readout + skip_gain * inputs_wide).astype(jnp.bfloat16)

def reference(tokens, norm_gain, w_input, w_query, w_key, w_value, query_gain, key_gain, key_bias, eigen_real, eigen_imag, log_step, input_real, input_imag, read_real, read_imag, skip_gain, w_out_state, w_out_attn):
    token_rows = tokens.astype(jnp.float32)
    scale_rows = lax.rsqrt(lax.optimization_barrier(jnp.mean(jnp.square(token_rows), axis=-1, keepdims=True)) + EPSILON)
    normed = (token_rows * scale_rows * norm_gain).astype(jnp.bfloat16)
    inputs = jnp.dot(normed, w_input, preferred_element_type=jnp.float32).astype(jnp.bfloat16)
    query_rows = jnp.dot(normed, w_query, preferred_element_type=jnp.float32).astype(jnp.bfloat16)
    key_rows = jnp.dot(normed, w_key, preferred_element_type=jnp.float32).astype(jnp.bfloat16)
    value_rows = jnp.dot(normed, w_value, preferred_element_type=jnp.float32).astype(jnp.bfloat16)
    queries = head_scale(query_rows, query_gain)
    key_heads = head_scale(key_rows, key_gain)
    value_heads = value_rows.reshape(SEQ, HEADS, HEAD_DIM)
    attn_out = attention_branch(queries, key_heads, value_heads, key_bias)
    state_out = state_branch(inputs, eigen_real, eigen_imag, log_step, input_real, input_imag, read_real, read_imag, skip_gain)
    state_cols = STATE_WIDTH // N_TP
    attn_cols = ATTN_WIDTH // N_TP

    def add_term(index, summed):
        state_part = lax.dynamic_slice_in_dim(state_out, index * state_cols, state_cols, 1)
        attn_part = lax.dynamic_slice_in_dim(attn_out, index * attn_cols, attn_cols, 1)
        state_weight = lax.dynamic_slice_in_dim(w_out_state, index * state_cols, state_cols, 0)
        attn_weight = lax.dynamic_slice_in_dim(w_out_attn, index * attn_cols, attn_cols, 0)
        term = jnp.dot(state_part, state_weight, preferred_element_type=jnp.float32)
        term = term + jnp.dot(attn_part, attn_weight, preferred_element_type=jnp.float32)
        term = lax.optimization_barrier(term.astype(jnp.bfloat16)).astype(jnp.float32)
        return summed + term
    summed = lax.fori_loop(0, N_TP, add_term, jnp.zeros((SEQ, D), jnp.float32))
    return summed.astype(jnp.bfloat16)
```

```python
import jax
import jax.numpy as jnp
from jax import lax
from jax.experimental import pallas as pl
from jax.experimental.pallas import tpu as pltpu
from jax.sharding import Mesh
from jax.sharding import PartitionSpec as P

GROUP = 16
STATE = 64
HEAD_DIM = 64
TP = ("tp_0", "tp_1")
FS_SP_TP = ("fs", "sp", "tp_0", "tp_1")
EPSILON = 1e-06
F32 = jnp.float32
BF16 = jnp.bfloat16


VMEM = pl.BlockSpec(memory_space=pltpu.VMEM)
SMEM = pl.BlockSpec(memory_space=pltpu.SMEM)


def discretize(eigen_real, eigen_imag, log_step, input_real, input_imag):
    step_size = jnp.exp(log_step)[:, None]
    rotation = eigen_imag * step_size
    shrink = jnp.expm1(eigen_real * step_size)
    cosine = jnp.cos(rotation)
    sine_part = jnp.sin(rotation)
    decay_r = (1.0 + shrink) * cosine
    decay_i = (1.0 + shrink) * sine_part
    minus_r = shrink * cosine - 2.0 * jnp.square(jnp.sin(0.5 * rotation))
    modulus = jnp.square(eigen_real) + jnp.square(eigen_imag)
    factor_r = (minus_r * eigen_real + decay_i * eigen_imag) / modulus
    factor_i = (decay_i * eigen_real - minus_r * eigen_imag) / modulus
    drive_r = factor_r[..., None] * input_real - factor_i[..., None] * input_imag
    drive_i = factor_r[..., None] * input_imag + factor_i[..., None] * input_real
    return (decay_r, decay_i, drive_r, drive_i)


def split(value):
    high = value.astype(BF16)
    low = (value - high.astype(F32)).astype(BF16)
    return high, low


def cmul(ar, ai, br, bi):
    return ar * br - ai * bi, ar * bi + ai * br


def nt_dot(a, b):
    return lax.dot_general(a, b, (((1,), (1,)), ((), ())), preferred_element_type=F32)


def nn_dot(a, b):
    return jnp.dot(a, b, preferred_element_type=F32)


def lanes_low(shape):
    return lax.broadcasted_iota(jnp.int32, shape, len(shape) - 1) < HEAD_DIM


def reorder_matrix(rows, chunks, inverse):
    length = rows // chunks
    r = lax.broadcasted_iota(jnp.int32, (rows, rows), 1 if inverse else 0)
    t = lax.broadcasted_iota(jnp.int32, (rows, rows), 0 if inverse else 1)
    source = (r & (chunks - 1)) * length + (r >> 3)
    return jnp.where(t == source, 1.0, 0.0).astype(BF16)


def power_kernel(decay_ref, tab_ref, chunk_ref, wide_ref, *, blocks, chunk):
    dr, di = decay_ref[0:1, :], decay_ref[1:2, :]
    width = dr.shape[1]
    half = width // 2
    squares = [(dr, di)]
    for _ in range(9):
        a, b = squares[-1]
        squares.append(cmul(a, b, a, b))

    def power(n):
        out = None
        for k in range(10):
            if n >> k & 1:
                out = squares[k] if out is None else cmul(*out, *squares[k])
        return out

    p_chunk = power(chunk)
    p_block = power(chunk * 8)
    now = (jnp.ones_like(dr), jnp.zeros_like(dr))
    for k in range(blocks):
        for j, part in enumerate(now):
            tab_ref[4 * k + 2 * j : 4 * k + 2 * j + 1, :] = part[:, :half]
            tab_ref[4 * k + 2 * j + 1 : 4 * k + 2 * j + 2, :] = part[:, half:]
        now = cmul(*now, *p_block)
    now = (dr, di)
    for c in range(8):
        chunk_ref[c : c + 1, :width] = now[0]
        chunk_ref[c : c + 1, width:] = now[1]
        now = cmul(*now, *p_chunk)
    p2 = cmul(*p_chunk, *p_chunk)
    p4 = cmul(*p2, *p2)
    for k, (a, b) in enumerate([(dr, di), p_chunk, p2, p4]):
        wide_ref[k : k + 1, :width] = a
        wide_ref[k : k + 1, width:] = b
    wide_ref[4:8, :] = jnp.zeros((4, 2 * width), F32)


def make_push(u_perm, b_hi, b_lo, push_ref):
    push_ref[...] = nn_dot(u_perm, b_hi) + nn_dot(u_perm, b_lo)


def project_kernel(
    place_ref, mine_ref, other_ref, w_ref, qg_ref, kg_ref, bias_ref, bhi_ref, blo_ref, wide_ref,
    q_ref, payload_ref, u_ref, init_ref, rows_ref, push_ref,
):
    rows = payload_ref.shape[0] - 16
    piece = rows // 8
    core = place_ref[1]
    for ref, where in ((mine_ref, core), (other_ref, 1 - core)):
        found = nn_dot(ref[...], w_ref[...]).astype(BF16)
        for a in range(4):
            at = pl.multiple_of((2 * a + where) * piece, 16)
            rows_ref[pl.ds(at, piece), :] = found[a * piece : (a + 1) * piece, :]
    low = lanes_low((rows, 2 * HEAD_DIM))

    def normed(raw, gain):
        wide = raw.astype(F32)
        square = wide * wide
        first = jnp.sum(jnp.where(low, square, 0.0), axis=1, keepdims=True)
        second = jnp.sum(jnp.where(low, 0.0, square), axis=1, keepdims=True)
        scale = jnp.where(
            low,
            lax.rsqrt(first * (1.0 / HEAD_DIM) + EPSILON),
            lax.rsqrt(second * (1.0 / HEAD_DIM) + EPSILON),
        )
        return (wide * scale * gain).astype(BF16)

    u = rows_ref[:, 0:128]
    u_perm = nn_dot(reorder_matrix(rows, 8, False), u).astype(BF16)
    u_ref[...] = u_perm
    make_push(u_perm, bhi_ref[...], blo_ref[...], push_ref)
    queries = normed(rows_ref[:, 128:256], qg_ref[...]).astype(F32) * HEAD_DIM ** (-0.5)
    q_ref[0] = jnp.where(low, queries, 0.0).astype(BF16)
    q_ref[1] = jnp.where(low, 0.0, queries).astype(BF16)
    payload_ref[0:rows, 0:128] = normed(rows_ref[:, 256:384], kg_ref[...])
    payload_ref[0:rows, 128:256] = rows_ref[:, 384:512]
    width = push_ref.shape[1] // 2
    lr = jnp.broadcast_to(wide_ref[0:1, :width], (8, width))
    li = jnp.broadcast_to(wide_ref[0:1, width:], (8, width))

    def step(k, carried):
        sr, si = carried
        at = pl.multiple_of(k * 8, 8)
        nr = lr * sr - li * si + push_ref[pl.ds(at, 8), :width]
        ni = lr * si + li * sr + push_ref[pl.ds(at, 8), width:]
        return nr, ni

    zero = jnp.zeros((8, width), F32)
    er, ei = lax.fori_loop(0, piece, step, (zero, zero), unroll=8)
    place = lax.broadcasted_iota(jnp.int32, (8, width), 0)
    for k in range(3):
        shift = 1 << k
        pr, pi = wide_ref[k + 1 : k + 2, :width], wide_ref[k + 1 : k + 2, width:]
        br = jnp.where(place >= shift, pltpu.roll(er, shift, 0), 0.0)
        bi = jnp.where(place >= shift, pltpu.roll(ei, shift, 0), 0.0)
        er, ei = er + pr * br - pi * bi, ei + pr * bi + pi * br
    init_ref[:, :width] = jnp.where(place >= 1, pltpu.roll(er, 1, 0), 0.0)
    init_ref[:, width:] = jnp.where(place >= 1, pltpu.roll(ei, 1, 0), 0.0)
    half = width // 2
    end = [er[7:8, :half], er[7:8, half:], ei[7:8, :half], ei[7:8, half:]]
    highs = [e.astype(BF16).astype(F32) for e in end]
    lows = [e - h for e, h in zip(end, highs)]
    tail = jnp.concatenate([bias_ref[...].astype(F32)] + highs + lows, axis=0)
    payload_ref[rows : rows + 16, :] = tail.astype(BF16)


def read_states(states_ref, ct_hi, ct_lo):
    high, low = split(states_ref[...])
    return nt_dot(high, ct_hi) + nt_dot(low, ct_hi) + nt_dot(high, ct_lo)


def local_state_kernel(
    u_ref, init_ref, bhi_ref, blo_ref, wide_ref, cthi_ref, ctlo_ref, skip_ref, y_ref, push_ref
):
    make_push(u_ref[...], bhi_ref[...], blo_ref[...], push_ref)
    width = push_ref.shape[1] // 2
    lr = jnp.broadcast_to(wide_ref[0:1, :width], (8, width))
    li = jnp.broadcast_to(wide_ref[0:1, width:], (8, width))

    def step(k, carried):
        sr, si = carried
        at = pl.multiple_of(k * 8, 8)
        nr = lr * sr - li * si + push_ref[pl.ds(at, 8), :width]
        ni = lr * si + li * sr + push_ref[pl.ds(at, 8), width:]
        push_ref[pl.ds(at, 8), :width] = nr
        push_ref[pl.ds(at, 8), width:] = ni
        return nr, ni

    lax.fori_loop(
        0, push_ref.shape[0] // 8, step, (init_ref[:, :width], init_ref[:, width:]), unroll=8
    )
    y_ref[...] = (
        read_states(push_ref, cthi_ref[...], ctlo_ref[...])
        + skip_ref[...] * u_ref[...].astype(F32)
    )


def score_block(q_ref, payload_ref, later_ref, diagonal):
    rows = q_ref.shape[1]
    keys, values = payload_ref[0:rows, 0:128], payload_ref[0:rows, 128:256]
    tail = payload_ref[rows : rows + 16, :].astype(F32)
    biases = (
        jnp.concatenate([tail[0:1, :], tail[1:2, 0:128]], axis=1),
        jnp.concatenate([tail[1:2, 128:256], tail[2:3, :]], axis=1),
    )
    outs, totals = [], []
    for h in range(2):
        z = nt_dot(q_ref[h], keys) + biases[h]
        loss = jnp.log(1.0 + jnp.exp(z))
        if diagonal:
            causal = lax.broadcasted_iota(jnp.int32, z.shape, 1) < lax.broadcasted_iota(
                jnp.int32, z.shape, 0
            )
            masked = jnp.where(causal, loss, 0.0)
        else:
            masked = loss
        later = nn_dot(masked.astype(BF16), later_ref[...])
        weights = jnp.exp((z - loss) - later)
        if diagonal:
            weights = jnp.where(causal, weights, 0.0)
        outs.append(nn_dot(weights.astype(BF16), values))
        totals.append(later[:, 0:1] + masked[:, 0:1])
    low = lanes_low((rows, 128))
    return jnp.where(low, outs[0], outs[1]), jnp.where(low, totals[0], totals[1])


def first_kernel(q_ref, payload_ref, later_ref, acc_ref, tot_ref):
    out, total = score_block(q_ref, payload_ref, later_ref, True)
    acc_ref[...] = out
    tot_ref[...] = total


def entering_state(payload_ref, tab_ref, carry_ref, power):
    rows = payload_ref.shape[0] - 16
    tail = payload_ref[rows : rows + 16, :].astype(F32)
    er, ei = tail[8:10] + tail[12:14], tail[10:12] + tail[14:16]
    wr, wi = tab_ref[4 * power : 4 * power + 2, :], tab_ref[4 * power + 2 : 4 * power + 4, :]
    carry_ref[0:2, :] += wr * er - wi * ei
    carry_ref[2:4, :] += wr * ei + wi * er


def step_kernel(
    place_ref, q_ref, later_ref, tab_ref, up_ref, down_ref,
    acc_in, tot_in, wrap_in, carry_in, acc_ref, tot_ref, wrap_ref, carry_ref, *, step, blocks,
):
    here = place_ref[0]
    acc_ref[...] = acc_in[...]
    tot_ref[...] = tot_in[...]
    wrap_ref[...] = wrap_in[...]
    carry_ref[...] = carry_in[...]
    if step < blocks // 2:

        @pl.when(here >= step)
        def _():
            out, total = score_block(q_ref, up_ref, later_ref, False)
            acc_ref[...] += out * jnp.exp(-tot_ref[...])
            tot_ref[...] += total
            entering_state(up_ref, tab_ref, carry_ref, step - 1)

    @pl.when(here >= blocks - step)
    def _():
        out, total = score_block(q_ref, down_ref, later_ref, False)
        wrap_ref[...] = wrap_ref[...] * jnp.exp(-total) + out
        entering_state(down_ref, tab_ref, carry_ref, blocks - 1 - step)


def finish_kernel(
    acc_ref, tot_ref, wrap_ref, carry_ref, y_ref, chunk_ref, wide_ref, cthi_ref, ctlo_ref,
    wo_ref, out_ref, states_ref,
):
    rows = acc_ref.shape[0]
    width = states_ref.shape[1] // 2
    sr = jnp.concatenate([carry_ref[0:1, :], carry_ref[1:2, :]], axis=1)
    si = jnp.concatenate([carry_ref[2:3, :], carry_ref[3:4, :]], axis=1)
    zr, zi = cmul(chunk_ref[:, :width], chunk_ref[:, width:], sr, si)
    lr = jnp.broadcast_to(wide_ref[0:1, :width], (8, width))
    li = jnp.broadcast_to(wide_ref[0:1, width:], (8, width))

    def step(k, carried):
        zr, zi = carried
        at = pl.multiple_of(k * 8, 8)
        states_ref[pl.ds(at, 8), :width] = zr
        states_ref[pl.ds(at, 8), width:] = zi
        return cmul(lr, li, zr, zi)

    lax.fori_loop(0, rows // 8, step, (zr, zi), unroll=8)
    mixed = y_ref[...] + read_states(states_ref, cthi_ref[...], ctlo_ref[...])
    state_out = jax.nn.gelu(mixed).astype(BF16)
    state_out = nn_dot(reorder_matrix(rows, 8, True), state_out).astype(BF16)
    attended = acc_ref[...] + wrap_ref[...] * jnp.exp(-tot_ref[...])
    low = lanes_low(attended.shape)
    square = attended * attended
    first = jnp.sum(jnp.where(low, square, 0.0), axis=1, keepdims=True)
    second = jnp.sum(jnp.where(low, 0.0, square), axis=1, keepdims=True)
    scale = jnp.where(
        low,
        lax.rsqrt(first * (1.0 / HEAD_DIM) + EPSILON),
        lax.rsqrt(second * (1.0 / HEAD_DIM) + EPSILON),
    )
    attn_out = (attended * scale).astype(BF16)
    both = jnp.concatenate([state_out, attn_out], axis=1)
    out_ref[...] = nn_dot(both, wo_ref[...]).astype(BF16)


def call(kernel, outs, args, scratch=(), smem=0, flops=1, aliases={}):
    return pl.pallas_call(
        kernel,
        out_shape=outs,
        in_specs=[SMEM] * smem + [VMEM] * (len(args) - smem),
        out_specs=jax.tree.map(lambda _: VMEM, outs),
        scratch_shapes=list(scratch),
        input_output_aliases=aliases,
        cost_estimate=pl.CostEstimate(flops=flops, bytes_accessed=10**6, transcendentals=0),
    )(*args)


def shape(dims, dtype=F32):
    return jax.ShapeDtypeStruct(dims, dtype)


def on_device(
    tokens,
    norm_gain,
    w_input,
    w_query,
    w_key,
    w_value,
    query_gain,
    key_gain,
    key_bias,
    eigen_real,
    eigen_imag,
    log_step,
    input_real,
    input_imag,
    read_real,
    read_imag,
    skip_gain,
    w_out_state,
    w_out_attn,
):
    blocks = lax.axis_size("sp")
    rows = key_bias.shape[0]
    piece = rows // 8
    groups = eigen_real.shape[0]
    width = groups * STATE
    channels = groups * GROUP
    place = jnp.stack([lax.axis_index("sp"), lax.axis_index("tp_1")]).astype(jnp.int32)

    token_rows = tokens.astype(F32)
    scale_rows = lax.rsqrt(jnp.mean(jnp.square(token_rows), axis=-1, keepdims=True) + EPSILON)
    normed = (token_rows * scale_rows * norm_gain).astype(BF16)
    copies = jnp.broadcast_to(normed[None], (4, *normed.shape))
    mine = lax.all_to_all(copies, "tp_0", 0, 0, tiled=True).reshape(4 * piece, -1)
    other = lax.ppermute(mine, "tp_1", [(0, 1), (1, 0)])

    w_joined = jnp.concatenate([w_input, w_query, w_key, w_value], axis=1)
    w_out = jnp.concatenate([w_out_state, w_out_attn], axis=0)
    decay_r, decay_i, drive_r, drive_i = discretize(
        eigen_real, eigen_imag, log_step, input_real, input_imag
    )
    own = (jnp.arange(channels) // GROUP)[:, None] == (jnp.arange(width) // STATE)[None, :]

    def drive_matrix(part):
        lines = jnp.transpose(part, (2, 0, 1)).reshape(GROUP, width)
        return jnp.where(own, jnp.tile(lines, (groups, 1)), 0.0)

    def read_matrix(part):
        return jnp.where(own, jnp.tile(part.reshape(channels, STATE), (1, groups)), 0.0)

    b_hi, b_lo = split(jnp.concatenate([drive_matrix(drive_r), drive_matrix(drive_i)], axis=1))
    ct_hi, ct_lo = split(jnp.concatenate([read_matrix(read_real), -read_matrix(read_imag)], axis=1))
    decay = jnp.stack([decay_r.reshape(-1), decay_i.reshape(-1)])
    tab, chunk, wide = call(
        lambda *refs: power_kernel(*refs, blocks=blocks, chunk=piece),
        (shape((4 * blocks, width // 2)), shape((8, 2 * width)), shape((8, 2 * width))),
        (decay,),
    )
    bias8 = jnp.pad(jnp.transpose(key_bias).reshape(-1, 256), ((0, 5), (0, 0)))
    index = jnp.arange(rows)
    later = (index[:, None] > index[None, :]).astype(BF16)
    gains = [jnp.tile(g, 2).reshape(1, 128) for g in (query_gain, key_gain)]

    q, payload, u_perm, init = call(
        project_kernel,
        (
            shape((2, rows, 128), BF16),
            shape((rows + 16, 256), BF16),
            shape((rows, channels), BF16),
            shape((8, 2 * width)),
        ),
        (place, mine, other, w_joined, *gains, bias8, b_hi, b_lo, wide),
        scratch=(pltpu.VMEM((rows, 512), BF16), pltpu.VMEM((rows, 2 * width), F32)),
        smem=1,
        flops=4 * 10**9,
    )

    acc, tot = call(
        first_kernel,
        (shape((rows, 128)), shape((rows, 128))),
        (q, payload, later),
        flops=2 * 10**9,
    )
    y_local = call(
        local_state_kernel,
        shape((rows, channels)),
        (u_perm, init, b_hi, b_lo, wide, ct_hi, ct_lo, skip_gain.reshape(1, -1)),
        scratch=(pltpu.VMEM((rows, 2 * width), F32),),
        flops=2 * 10**9,
    )
    wrap = jnp.zeros((rows, 128), F32)
    carry = jnp.zeros((8, width // 2), F32)
    up = down = payload
    half = blocks // 2
    for step in range(1, half + 1):
        if step < half:
            up = lax.ppermute(up, "sp", [(i - 1, i) for i in range(step, blocks)])
        down = lax.ppermute(
            down, "sp", [((j - step + 1) % blocks, (j - step) % blocks) for j in range(half)]
        )
        acc, tot, wrap, carry = call(
            lambda *refs, step=step: step_kernel(*refs, step=step, blocks=blocks),
            (shape((rows, 128)), shape((rows, 128)), shape((rows, 128)), shape(carry.shape)),
            (place, q, later, tab, up, down, acc, tot, wrap, carry),
            smem=1,
            flops=3 * 10**9,
            aliases={6: 0, 7: 1, 8: 2, 9: 3},
        )
    part = call(
        finish_kernel,
        shape((rows, w_out.shape[1]), BF16),
        (acc, tot, wrap, carry, y_local, chunk, wide, ct_hi, ct_lo, w_out),
        scratch=(pltpu.VMEM((rows, 2 * width), F32),),
        flops=3 * 10**9,
    )
    tiles = lax.all_to_all(part.reshape(8, piece, -1), TP, 0, 0, tiled=True)
    return jnp.sum(tiles.astype(F32), axis=0).astype(BF16)


def solution(mesh):
    torus = Mesh(
        mesh.devices.reshape(mesh.shape["sp"], mesh.shape["fs"], 4, 2), ("sp", "fs", "tp_0", "tp_1")
    )
    placed = (
        P(FS_SP_TP, None),
        P(),
        P(None, TP),
        P(None, TP),
        P(None, TP),
        P(None, TP),
        P(),
        P(),
        P(("fs", "sp"), TP),
        P(TP, None),
        P(TP, None),
        P(TP),
        P(TP, None, None),
        P(TP, None, None),
        P(TP, None, None),
        P(TP, None, None),
        P(TP),
        P(TP, None),
        P(TP, None),
    )
    return jax.shard_map(
        on_device, mesh=torus, in_specs=placed, out_specs=P(FS_SP_TP, None), check_vma=False
    )
```

```python
import jax
import jax.numpy as jnp
from jax import lax
from jax.experimental import pallas as pl
from jax.experimental.pallas import tpu as pltpu
from jax.sharding import Mesh
from jax.sharding import PartitionSpec as P

GROUP = 16
STATE = 64
HEAD_DIM = 64
TP = ("tp_0", "tp_1")
FS_SP_TP = ("fs", "sp", "tp_0", "tp_1")
EPSILON = 1e-06
F32 = jnp.float32
BF16 = jnp.bfloat16


VMEM = pl.BlockSpec(memory_space=pltpu.VMEM)
SMEM = pl.BlockSpec(memory_space=pltpu.SMEM)


def discretize(eigen_real, eigen_imag, log_step, input_real, input_imag):
    step_size = jnp.exp(log_step)[:, None]
    rotation = eigen_imag * step_size
    shrink = jnp.expm1(eigen_real * step_size)
    cosine = jnp.cos(rotation)
    sine_part = jnp.sin(rotation)
    decay_r = (1.0 + shrink) * cosine
    decay_i = (1.0 + shrink) * sine_part
    minus_r = shrink * cosine - 2.0 * jnp.square(jnp.sin(0.5 * rotation))
    modulus = jnp.square(eigen_real) + jnp.square(eigen_imag)
    factor_r = (minus_r * eigen_real + decay_i * eigen_imag) / modulus
    factor_i = (decay_i * eigen_real - minus_r * eigen_imag) / modulus
    drive_r = factor_r[..., None] * input_real - factor_i[..., None] * input_imag
    drive_i = factor_r[..., None] * input_imag + factor_i[..., None] * input_real
    return (decay_r, decay_i, drive_r, drive_i)


def split(value):
    high = value.astype(BF16)
    low = (value - high.astype(F32)).astype(BF16)
    return high, low


def cmul(ar, ai, br, bi):
    return ar * br - ai * bi, ar * bi + ai * br


def nt_dot(a, b):
    return lax.dot_general(a, b, (((1,), (1,)), ((), ())), preferred_element_type=F32)


def nn_dot(a, b):
    return jnp.dot(a, b, preferred_element_type=F32)


def lanes_low(shape):
    return lax.broadcasted_iota(jnp.int32, shape, len(shape) - 1) < HEAD_DIM


def reorder_matrix(rows, chunks, inverse):
    length = rows // chunks
    r = lax.broadcasted_iota(jnp.int32, (rows, rows), 1 if inverse else 0)
    t = lax.broadcasted_iota(jnp.int32, (rows, rows), 0 if inverse else 1)
    source = (r & (chunks - 1)) * length + (r >> 3)
    return jnp.where(t == source, 1.0, 0.0).astype(BF16)


def power_kernel(decay_ref, tab_ref, chunk_ref, wide_ref, *, blocks, chunk):
    dr, di = decay_ref[0:1, :], decay_ref[1:2, :]
    width = dr.shape[1]
    half = width // 2
    squares = [(dr, di)]
    for _ in range(9):
        a, b = squares[-1]
        squares.append(cmul(a, b, a, b))

    def power(n):
        out = None
        for k in range(10):
            if n >> k & 1:
                out = squares[k] if out is None else cmul(*out, *squares[k])
        return out

    p_chunk = power(chunk)
    p_block = power(chunk * 8)
    now = (jnp.ones_like(dr), jnp.zeros_like(dr))
    for k in range(blocks):
        for j, part in enumerate(now):
            tab_ref[4 * k + 2 * j : 4 * k + 2 * j + 1, :] = part[:, :half]
            tab_ref[4 * k + 2 * j + 1 : 4 * k + 2 * j + 2, :] = part[:, half:]
        now = cmul(*now, *p_block)
    now = (dr, di)
    for c in range(8):
        chunk_ref[c : c + 1, :width] = now[0]
        chunk_ref[c : c + 1, width:] = now[1]
        now = cmul(*now, *p_chunk)
    p2 = cmul(*p_chunk, *p_chunk)
    p4 = cmul(*p2, *p2)
    for k, (a, b) in enumerate([(dr, di), p_chunk, p2, p4]):
        wide_ref[k : k + 1, :width] = a
        wide_ref[k : k + 1, width:] = b
    wide_ref[4:8, :] = jnp.zeros((4, 2 * width), F32)


def make_push(u_perm, b_hi, b_lo, push_ref):
    push_ref[...] = nn_dot(u_perm, b_hi) + nn_dot(u_perm, b_lo)


def project_kernel(
    place_ref, mine_ref, other_ref, w_ref, qg_ref, kg_ref, bias_ref, bhi_ref, blo_ref, wide_ref,
    q_ref, payload_ref, u_ref, init_ref, rows_ref, push_ref,
):
    rows = payload_ref.shape[0] - 16
    piece = rows // 8
    core = place_ref[1]
    for ref, where in ((mine_ref, core), (other_ref, 1 - core)):
        found = nn_dot(ref[...], w_ref[...]).astype(BF16)
        for a in range(4):
            at = pl.multiple_of((2 * a + where) * piece, 16)
            rows_ref[pl.ds(at, piece), :] = found[a * piece : (a + 1) * piece, :]
    low = lanes_low((rows, 2 * HEAD_DIM))

    def normed(raw, gain):
        wide = raw.astype(F32)
        square = wide * wide
        first = jnp.sum(jnp.where(low, square, 0.0), axis=1, keepdims=True)
        second = jnp.sum(jnp.where(low, 0.0, square), axis=1, keepdims=True)
        scale = jnp.where(
            low,
            lax.rsqrt(first * (1.0 / HEAD_DIM) + EPSILON),
            lax.rsqrt(second * (1.0 / HEAD_DIM) + EPSILON),
        )
        return (wide * scale * gain).astype(BF16)

    u = rows_ref[:, 0:128]
    u_perm = nn_dot(reorder_matrix(rows, 8, False), u).astype(BF16)
    u_ref[...] = u_perm
    make_push(u_perm, bhi_ref[...], blo_ref[...], push_ref)
    queries = normed(rows_ref[:, 128:256], qg_ref[...]).astype(F32) * HEAD_DIM ** (-0.5)
    q_ref[0] = jnp.where(low, queries, 0.0).astype(BF16)
    q_ref[1] = jnp.where(low, 0.0, queries).astype(BF16)
    payload_ref[0:rows, 0:128] = normed(rows_ref[:, 256:384], kg_ref[...])
    payload_ref[0:rows, 128:256] = rows_ref[:, 384:512]
    width = push_ref.shape[1] // 2
    lr = jnp.broadcast_to(wide_ref[0:1, :width], (8, width))
    li = jnp.broadcast_to(wide_ref[0:1, width:], (8, width))

    def step(k, carried):
        sr, si = carried
        at = pl.multiple_of(k * 8, 8)
        nr = lr * sr - li * si + push_ref[pl.ds(at, 8), :width]
        ni = lr * si + li * sr + push_ref[pl.ds(at, 8), width:]
        return nr, ni

    zero = jnp.zeros((8, width), F32)
    er, ei = lax.fori_loop(0, piece, step, (zero, zero), unroll=8)
    place = lax.broadcasted_iota(jnp.int32, (8, width), 0)
    for k in range(3):
        shift = 1 << k
        pr, pi = wide_ref[k + 1 : k + 2, :width], wide_ref[k + 1 : k + 2, width:]
        br = jnp.where(place >= shift, pltpu.roll(er, shift, 0), 0.0)
        bi = jnp.where(place >= shift, pltpu.roll(ei, shift, 0), 0.0)
        er, ei = er + pr * br - pi * bi, ei + pr * bi + pi * br
    init_ref[:, :width] = jnp.where(place >= 1, pltpu.roll(er, 1, 0), 0.0)
    init_ref[:, width:] = jnp.where(place >= 1, pltpu.roll(ei, 1, 0), 0.0)
    half = width // 2
    end = [er[7:8, :half], er[7:8, half:], ei[7:8, :half], ei[7:8, half:]]
    highs = [e.astype(BF16).astype(F32) for e in end]
    lows = [e - h for e, h in zip(end, highs)]
    tail = jnp.concatenate([bias_ref[...].astype(F32)] + highs + lows, axis=0)
    payload_ref[rows : rows + 16, :] = tail.astype(BF16)


def read_states(states_ref, ct_hi, ct_lo):
    high, low = split(states_ref[...])
    return nt_dot(high, ct_hi) + nt_dot(low, ct_hi) + nt_dot(high, ct_lo)


def local_state_kernel(
    u_ref, init_ref, bhi_ref, blo_ref, wide_ref, cthi_ref, ctlo_ref, skip_ref, y_ref, push_ref
):
    make_push(u_ref[...], bhi_ref[...], blo_ref[...], push_ref)
    width = push_ref.shape[1] // 2
    lr = jnp.broadcast_to(wide_ref[0:1, :width], (8, width))
    li = jnp.broadcast_to(wide_ref[0:1, width:], (8, width))

    def step(k, carried):
        sr, si = carried
        at = pl.multiple_of(k * 8, 8)
        nr = lr * sr - li * si + push_ref[pl.ds(at, 8), :width]
        ni = lr * si + li * sr + push_ref[pl.ds(at, 8), width:]
        push_ref[pl.ds(at, 8), :width] = nr
        push_ref[pl.ds(at, 8), width:] = ni
        return nr, ni

    lax.fori_loop(
        0, push_ref.shape[0] // 8, step, (init_ref[:, :width], init_ref[:, width:]), unroll=8
    )
    y_ref[...] = (
        read_states(push_ref, cthi_ref[...], ctlo_ref[...])
        + skip_ref[...] * u_ref[...].astype(F32)
    )


def score_block(q_ref, payload_ref, later_ref, diagonal):
    rows = q_ref.shape[1]
    keys, values = payload_ref[0:rows, 0:128], payload_ref[0:rows, 128:256]
    tail = payload_ref[rows : rows + 16, :].astype(F32)
    biases = (
        jnp.concatenate([tail[0:1, :], tail[1:2, 0:128]], axis=1),
        jnp.concatenate([tail[1:2, 128:256], tail[2:3, :]], axis=1),
    )
    outs, totals = [], []
    for h in range(2):
        z = nt_dot(q_ref[h], keys) + biases[h]
        loss = jnp.log(1.0 + jnp.exp(z))
        if diagonal:
            causal = lax.broadcasted_iota(jnp.int32, z.shape, 1) < lax.broadcasted_iota(
                jnp.int32, z.shape, 0
            )
            masked = jnp.where(causal, loss, 0.0)
        else:
            masked = loss
        later = nn_dot(masked.astype(BF16), later_ref[...])
        weights = jnp.exp((z - loss) - later)
        if diagonal:
            weights = jnp.where(causal, weights, 0.0)
        outs.append(nn_dot(weights.astype(BF16), values))
        totals.append(later[:, 0:1] + masked[:, 0:1])
    low = lanes_low((rows, 128))
    return jnp.where(low, outs[0], outs[1]), jnp.where(low, totals[0], totals[1])


def first_kernel(q_ref, payload_ref, later_ref, acc_ref, tot_ref):
    out, total = score_block(q_ref, payload_ref, later_ref, True)
    acc_ref[...] = out
    tot_ref[...] = total


def entering_state(payload_ref, tab_ref, carry_ref, power):
    rows = payload_ref.shape[0] - 16
    tail = payload_ref[rows : rows + 16, :].astype(F32)
    er, ei = tail[8:10] + tail[12:14], tail[10:12] + tail[14:16]
    wr, wi = tab_ref[4 * power : 4 * power + 2, :], tab_ref[4 * power + 2 : 4 * power + 4, :]
    carry_ref[0:2, :] += wr * er - wi * ei
    carry_ref[2:4, :] += wr * ei + wi * er


def step_kernel(
    place_ref, q_ref, later_ref, tab_ref, up_ref, down_ref,
    acc_in, tot_in, wrap_in, carry_in, acc_ref, tot_ref, wrap_ref, carry_ref, *, step, blocks,
):
    here = place_ref[0]
    acc_ref[...] = acc_in[...]
    tot_ref[...] = tot_in[...]
    wrap_ref[...] = wrap_in[...]
    carry_ref[...] = carry_in[...]
    if step < blocks // 2:

        @pl.when(here >= step)
        def _():
            out, total = score_block(q_ref, up_ref, later_ref, False)
            acc_ref[...] += out * jnp.exp(-tot_ref[...])
            tot_ref[...] += total
            entering_state(up_ref, tab_ref, carry_ref, step - 1)

    @pl.when(here >= blocks - step)
    def _():
        out, total = score_block(q_ref, down_ref, later_ref, False)
        wrap_ref[...] = wrap_ref[...] * jnp.exp(-total) + out
        entering_state(down_ref, tab_ref, carry_ref, blocks - 1 - step)


def finish_kernel(
    acc_ref, tot_ref, wrap_ref, carry_ref, y_ref, chunk_ref, wide_ref, cthi_ref, ctlo_ref,
    wo_ref, out_ref, states_ref,
):
    rows = acc_ref.shape[0]
    width = states_ref.shape[1] // 2
    sr = jnp.concatenate([carry_ref[0:1, :], carry_ref[1:2, :]], axis=1)
    si = jnp.concatenate([carry_ref[2:3, :], carry_ref[3:4, :]], axis=1)
    zr, zi = cmul(chunk_ref[:, :width], chunk_ref[:, width:], sr, si)
    lr = jnp.broadcast_to(wide_ref[0:1, :width], (8, width))
    li = jnp.broadcast_to(wide_ref[0:1, width:], (8, width))

    def step(k, carried):
        zr, zi = carried
        at = pl.multiple_of(k * 8, 8)
        states_ref[pl.ds(at, 8), :width] = zr
        states_ref[pl.ds(at, 8), width:] = zi
        return cmul(lr, li, zr, zi)

    lax.fori_loop(0, rows // 8, step, (zr, zi), unroll=8)
    mixed = y_ref[...] + read_states(states_ref, cthi_ref[...], ctlo_ref[...])
    state_out = jax.nn.gelu(mixed).astype(BF16)
    state_out = nn_dot(reorder_matrix(rows, 8, True), state_out).astype(BF16)
    attended = acc_ref[...] + wrap_ref[...] * jnp.exp(-tot_ref[...])
    low = lanes_low(attended.shape)
    square = attended * attended
    first = jnp.sum(jnp.where(low, square, 0.0), axis=1, keepdims=True)
    second = jnp.sum(jnp.where(low, 0.0, square), axis=1, keepdims=True)
    scale = jnp.where(
        low,
        lax.rsqrt(first * (1.0 / HEAD_DIM) + EPSILON),
        lax.rsqrt(second * (1.0 / HEAD_DIM) + EPSILON),
    )
    attn_out = (attended * scale).astype(BF16)
    both = jnp.concatenate([state_out, attn_out], axis=1)
    out_ref[...] = nn_dot(both, wo_ref[...]).astype(BF16)


def call(kernel, outs, args, scratch=(), smem=0, flops=1, aliases={}, limit=16):
    return pl.pallas_call(
        kernel,
        out_shape=outs,
        in_specs=[SMEM] * smem + [VMEM] * (len(args) - smem),
        out_specs=jax.tree.map(lambda _: VMEM, outs),
        scratch_shapes=list(scratch),
        input_output_aliases=aliases,
        compiler_params=pltpu.CompilerParams(vmem_limit_bytes=limit * 2**20),
        cost_estimate=pl.CostEstimate(flops=flops, bytes_accessed=10**6, transcendentals=0),
    )(*args)


def shape(dims, dtype=F32):
    return jax.ShapeDtypeStruct(dims, dtype)


def on_device(
    tokens,
    norm_gain,
    w_input,
    w_query,
    w_key,
    w_value,
    query_gain,
    key_gain,
    key_bias,
    eigen_real,
    eigen_imag,
    log_step,
    input_real,
    input_imag,
    read_real,
    read_imag,
    skip_gain,
    w_out_state,
    w_out_attn,
):
    blocks = lax.axis_size("sp")
    rows = key_bias.shape[0]
    piece = rows // 8
    groups = eigen_real.shape[0]
    width = groups * STATE
    channels = groups * GROUP
    place = jnp.stack([lax.axis_index("sp"), lax.axis_index("tp_1")]).astype(jnp.int32)

    token_rows = tokens.astype(F32)
    scale_rows = lax.rsqrt(jnp.mean(jnp.square(token_rows), axis=-1, keepdims=True) + EPSILON)
    normed = (token_rows * scale_rows * norm_gain).astype(BF16)
    copies = jnp.broadcast_to(normed[None], (4, *normed.shape))
    mine = lax.all_to_all(copies, "tp_0", 0, 0, tiled=True).reshape(4 * piece, -1)

    w_joined = jnp.concatenate([w_input, w_query, w_key, w_value], axis=1)
    w_out = jnp.concatenate([w_out_state, w_out_attn], axis=0)
    decay_r, decay_i, drive_r, drive_i = discretize(
        eigen_real, eigen_imag, log_step, input_real, input_imag
    )
    own = (jnp.arange(channels) // GROUP)[:, None] == (jnp.arange(width) // STATE)[None, :]

    def drive_matrix(part):
        lines = jnp.transpose(part, (2, 0, 1)).reshape(GROUP, width)
        return jnp.where(own, jnp.tile(lines, (groups, 1)), 0.0)

    def read_matrix(part):
        return jnp.where(own, jnp.tile(part.reshape(channels, STATE), (1, groups)), 0.0)

    b_hi, b_lo = split(jnp.concatenate([drive_matrix(drive_r), drive_matrix(drive_i)], axis=1))
    ct_hi, ct_lo = split(jnp.concatenate([read_matrix(read_real), -read_matrix(read_imag)], axis=1))
    decay = jnp.stack([decay_r.reshape(-1), decay_i.reshape(-1)])
    tab, chunk, wide = call(
        lambda *refs: power_kernel(*refs, blocks=blocks, chunk=piece),
        (shape((4 * blocks, width // 2)), shape((8, 2 * width)), shape((8, 2 * width))),
        (decay,),
    )
    bias8 = jnp.pad(jnp.transpose(key_bias).reshape(-1, 256), ((0, 5), (0, 0)))
    index = jnp.arange(rows)
    later = (index[:, None] > index[None, :]).astype(BF16)
    gains = [jnp.tile(g, 2).reshape(1, 128) for g in (query_gain, key_gain)]

    ready = (w_joined, *gains, bias8, b_hi, b_lo, wide, chunk, tab, ct_hi, ct_lo, w_out, later)
    mine, ready = lax.optimization_barrier((mine, ready))
    (w_joined, *gains, bias8, b_hi, b_lo, wide, chunk, tab, ct_hi, ct_lo, w_out, later) = ready
    gains = list(gains)
    other = lax.ppermute(mine, "tp_1", [(0, 1), (1, 0)])

    q, payload, u_perm, init = call(
        project_kernel,
        (
            shape((2, rows, 128), BF16),
            shape((rows + 16, 256), BF16),
            shape((rows, channels), BF16),
            shape((8, 2 * width)),
        ),
        (place, mine, other, w_joined, *gains, bias8, b_hi, b_lo, wide),
        scratch=(pltpu.VMEM((rows, 512), BF16), pltpu.VMEM((rows, 2 * width), F32)),
        smem=1,
        flops=4 * 10**9,
    )

    acc, tot = call(
        first_kernel,
        (shape((rows, 128)), shape((rows, 128))),
        (q, payload, later),
        flops=2 * 10**9,
    )
    y_local = call(
        local_state_kernel,
        shape((rows, channels)),
        (u_perm, init, b_hi, b_lo, wide, ct_hi, ct_lo, skip_gain.reshape(1, -1)),
        scratch=(pltpu.VMEM((rows, 2 * width), F32),),
        flops=2 * 10**9,
    )
    wrap = jnp.zeros((rows, 128), F32)
    carry = jnp.zeros((8, width // 2), F32)
    up = down = payload
    half = blocks // 2
    for step in range(1, half + 1):
        if step < half:
            up = lax.ppermute(up, "sp", [(i - 1, i) for i in range(step, blocks)])
        down = lax.ppermute(
            down, "sp", [((j - step + 1) % blocks, (j - step) % blocks) for j in range(half)]
        )
        acc, tot, wrap, carry = call(
            lambda *refs, step=step: step_kernel(*refs, step=step, blocks=blocks),
            (shape((rows, 128)), shape((rows, 128)), shape((rows, 128)), shape(carry.shape)),
            (place, q, later, tab, up, down, acc, tot, wrap, carry),
            smem=1,
            flops=3 * 10**9,
            aliases={6: 0, 7: 1, 8: 2, 9: 3},
        )
    part = call(
        finish_kernel,
        shape((rows, w_out.shape[1]), BF16),
        (acc, tot, wrap, carry, y_local, chunk, wide, ct_hi, ct_lo, w_out),
        scratch=(pltpu.VMEM((rows, 2 * width), F32),),
        flops=3 * 10**9,
    )
    tiles = lax.all_to_all(part.reshape(8, piece, -1), TP, 0, 0, tiled=True)
    return jnp.sum(tiles.astype(F32), axis=0).astype(BF16)


def solution(mesh):
    torus = Mesh(
        mesh.devices.reshape(mesh.shape["sp"], mesh.shape["fs"], 4, 2), ("sp", "fs", "tp_0", "tp_1")
    )
    placed = (
        P(FS_SP_TP, None),
        P(),
        P(None, TP),
        P(None, TP),
        P(None, TP),
        P(None, TP),
        P(),
        P(),
        P(("fs", "sp"), TP),
        P(TP, None),
        P(TP, None),
        P(TP),
        P(TP, None, None),
        P(TP, None, None),
        P(TP, None, None),
        P(TP, None, None),
        P(TP),
        P(TP, None),
        P(TP, None),
    )
    return jax.shard_map(
        on_device, mesh=torus, in_specs=placed, out_specs=P(FS_SP_TP, None), check_vma=False
    )
```

```python
import jax
import jax.numpy as jnp
from jax import lax
from jax.experimental import pallas as pl
from jax.experimental.pallas import tpu as pltpu
from jax.sharding import Mesh
from jax.sharding import PartitionSpec as P


GROUP = 16
STATE = 64
HEAD_DIM = 64
TP = ("tp_0", "tp_1")
FS_SP_TP = ("fs", "sp", "tp_0", "tp_1")
EPSILON = 1e-06
F32 = jnp.float32
BF16 = jnp.bfloat16


MERGE_LIMIT = 16

VMEM = pl.BlockSpec(memory_space=pltpu.VMEM)
SMEM = pl.BlockSpec(memory_space=pltpu.SMEM)


def discretize(eigen_real, eigen_imag, log_step, input_real, input_imag):
    step_size = jnp.exp(log_step)[:, None]
    rotation = eigen_imag * step_size
    shrink = jnp.expm1(eigen_real * step_size)
    cosine = jnp.cos(rotation)
    sine_part = jnp.sin(rotation)
    decay_r = (1.0 + shrink) * cosine
    decay_i = (1.0 + shrink) * sine_part
    minus_r = shrink * cosine - 2.0 * jnp.square(jnp.sin(0.5 * rotation))
    modulus = jnp.square(eigen_real) + jnp.square(eigen_imag)
    factor_r = (minus_r * eigen_real + decay_i * eigen_imag) / modulus
    factor_i = (decay_i * eigen_real - minus_r * eigen_imag) / modulus
    drive_r = factor_r[..., None] * input_real - factor_i[..., None] * input_imag
    drive_i = factor_r[..., None] * input_imag + factor_i[..., None] * input_real
    return (decay_r, decay_i, drive_r, drive_i)


def split(value):
    high = value.astype(BF16)
    low = (value - high.astype(F32)).astype(BF16)
    return high, low


def cmul(ar, ai, br, bi):
    return ar * br - ai * bi, ar * bi + ai * br


def nt_dot(a, b):
    return lax.dot_general(a, b, (((1,), (1,)), ((), ())), preferred_element_type=F32)


def nn_dot(a, b):
    return jnp.dot(a, b, preferred_element_type=F32)


def lanes_low(shape):
    return lax.broadcasted_iota(jnp.int32, shape, len(shape) - 1) < HEAD_DIM


def reorder_matrix(rows, chunks, inverse):
    length = rows // chunks
    r = lax.broadcasted_iota(jnp.int32, (rows, rows), 1 if inverse else 0)
    t = lax.broadcasted_iota(jnp.int32, (rows, rows), 0 if inverse else 1)
    source = (r & (chunks - 1)) * length + (r >> 3)
    return jnp.where(t == source, 1.0, 0.0).astype(BF16)


def norm_kernel(tokens_ref, gain_ref, out_ref):
    wide = tokens_ref[...].astype(F32)
    mean = jnp.sum(wide * wide, axis=1, keepdims=True) * (1.0 / wide.shape[1])
    normed = (wide * lax.rsqrt(mean + EPSILON) * gain_ref[...]).astype(BF16)
    for k in range(out_ref.shape[0]):
        out_ref[k] = normed


def half_project_kernel(mine_ref, w_ref, found_ref):
    found_ref[...] = nn_dot(mine_ref[...], w_ref[...]).astype(BF16)


def merge_kernel(place_ref, parts_ref, mine_ref, other_ref, out_ref):
    core = place_ref[1]
    total = None
    for a in range(mine_ref.shape[0]):
        for ref, where in ((mine_ref, core), (other_ref, 1 - core)):
            term = nn_dot(parts_ref[2 * a + where], ref[a])
            total = term if total is None else total + term
    out_ref[...] = total.astype(BF16)


def block_diagonal(parts, channels, width):
    row = lax.broadcasted_iota(jnp.int32, (channels, width), 0) >> 4
    lane = lax.broadcasted_iota(jnp.int32, (channels, width), 1) >> 6
    return split(jnp.concatenate([jnp.where(row == lane, p, 0.0) for p in parts], axis=1))


def drive_matrices(lines_ref, channels):
    width = lines_ref.shape[1]
    parts = [lines_ref[j * GROUP : (j + 1) * GROUP, :] for j in range(2)]
    parts = [jnp.concatenate([p] * (channels // GROUP), axis=0) for p in parts]
    return block_diagonal(parts, channels, width)


def read_matrices(reads_ref, width):
    channels = reads_ref.shape[0] // 2
    parts = [reads_ref[j * channels : (j + 1) * channels, :] for j in range(2)]
    parts = [jnp.concatenate([p] * (width // 128), axis=1) for p in (parts[0], -parts[1])]
    return block_diagonal(parts, channels, width)


def prepare_kernel(decay_ref, tab_ref, chunk_ref, wide_ref, later_ref, *, blocks, chunk):
    rows = later_ref.shape
    below = lax.broadcasted_iota(jnp.int32, rows, 0) > lax.broadcasted_iota(jnp.int32, rows, 1)
    later_ref[...] = jnp.where(below, 1.0, 0.0).astype(BF16)
    dr, di = decay_ref[0:1, :], decay_ref[1:2, :]
    width = dr.shape[1]
    half = width // 2
    squares = [(dr, di)]
    for _ in range(9):
        a, b = squares[-1]
        squares.append(cmul(a, b, a, b))

    def power(n):
        out = None
        for k in range(10):
            if n >> k & 1:
                out = squares[k] if out is None else cmul(*out, *squares[k])
        return out

    p_chunk = power(chunk)
    p_block = power(chunk * 8)
    now = (jnp.ones_like(dr), jnp.zeros_like(dr))
    for k in range(blocks):
        for j, part in enumerate(now):
            tab_ref[4 * k + 2 * j : 4 * k + 2 * j + 1, :] = part[:, :half]
            tab_ref[4 * k + 2 * j + 1 : 4 * k + 2 * j + 2, :] = part[:, half:]
        now = cmul(*now, *p_block)
    now = (dr, di)
    for c in range(8):
        chunk_ref[c : c + 1, :width] = now[0]
        chunk_ref[c : c + 1, width:] = now[1]
        now = cmul(*now, *p_chunk)
    p2 = cmul(*p_chunk, *p_chunk)
    p4 = cmul(*p2, *p2)
    for k, (a, b) in enumerate([(dr, di), p_chunk, p2, p4]):
        wide_ref[k : k + 1, :width] = a
        wide_ref[k : k + 1, width:] = b
    wide_ref[4:8, :] = jnp.zeros((4, 2 * width), F32)


def make_push(u_perm, b_hi, b_lo, push_ref):
    push_ref[...] = nn_dot(u_perm, b_hi) + nn_dot(u_perm, b_lo)


def project_kernel(
    place_ref, found_ref, other_ref, w_ref, qg_ref, kg_ref, bias_ref, lines_ref, wide_ref,
    q_ref, payload_ref, u_ref, init_ref, rows_ref, push_ref,
):
    rows = payload_ref.shape[0] - 16
    piece = rows // 8
    core = place_ref[1]
    found_other = nn_dot(other_ref[...], w_ref[...]).astype(BF16)
    for found, where in ((found_ref[...], core), (found_other, 1 - core)):
        for a in range(4):
            at = pl.multiple_of((2 * a + where) * piece, 16)
            rows_ref[pl.ds(at, piece), :] = found[a * piece : (a + 1) * piece, :]
    low = lanes_low((rows, 2 * HEAD_DIM))

    def normed(raw, gain):
        wide = raw.astype(F32)
        square = wide * wide
        first = jnp.sum(jnp.where(low, square, 0.0), axis=1, keepdims=True)
        second = jnp.sum(jnp.where(low, 0.0, square), axis=1, keepdims=True)
        scale = jnp.where(
            low,
            lax.rsqrt(first * (1.0 / HEAD_DIM) + EPSILON),
            lax.rsqrt(second * (1.0 / HEAD_DIM) + EPSILON),
        )
        return (wide * scale * gain).astype(BF16)

    u = rows_ref[:, 0:128]
    u_perm = nn_dot(reorder_matrix(rows, 8, False), u).astype(BF16)
    u_ref[...] = u_perm
    make_push(u_perm, *drive_matrices(lines_ref, u_perm.shape[1]), push_ref)
    queries = normed(rows_ref[:, 128:256], qg_ref[...]).astype(F32) * HEAD_DIM ** (-0.5)
    q_ref[0] = jnp.where(low, queries, 0.0).astype(BF16)
    q_ref[1] = jnp.where(low, 0.0, queries).astype(BF16)
    payload_ref[0:rows, 0:128] = normed(rows_ref[:, 256:384], kg_ref[...])
    payload_ref[0:rows, 128:256] = rows_ref[:, 384:512]
    width = push_ref.shape[1] // 2
    lr = jnp.broadcast_to(wide_ref[0:1, :width], (8, width))
    li = jnp.broadcast_to(wide_ref[0:1, width:], (8, width))

    def step(k, carried):
        sr, si = carried
        at = pl.multiple_of(k * 8, 8)
        nr = lr * sr - li * si + push_ref[pl.ds(at, 8), :width]
        ni = lr * si + li * sr + push_ref[pl.ds(at, 8), width:]
        return nr, ni

    zero = jnp.zeros((8, width), F32)
    er, ei = lax.fori_loop(0, piece, step, (zero, zero), unroll=8)
    place = lax.broadcasted_iota(jnp.int32, (8, width), 0)
    for k in range(3):
        shift = 1 << k
        pr, pi = wide_ref[k + 1 : k + 2, :width], wide_ref[k + 1 : k + 2, width:]
        br = jnp.where(place >= shift, pltpu.roll(er, shift, 0), 0.0)
        bi = jnp.where(place >= shift, pltpu.roll(ei, shift, 0), 0.0)
        er, ei = er + pr * br - pi * bi, ei + pr * bi + pi * br
    init_ref[:, :width] = jnp.where(place >= 1, pltpu.roll(er, 1, 0), 0.0)
    init_ref[:, width:] = jnp.where(place >= 1, pltpu.roll(ei, 1, 0), 0.0)
    half = width // 2
    end = [er[7:8, :half], er[7:8, half:], ei[7:8, :half], ei[7:8, half:]]
    highs = [e.astype(BF16).astype(F32) for e in end]
    lows = [e - h for e, h in zip(end, highs)]
    tail = jnp.concatenate([bias_ref[...].astype(F32)] + highs + lows, axis=0)
    payload_ref[rows : rows + 16, :] = tail.astype(BF16)


def read_states(states_ref, ct_hi, ct_lo):
    high, low = split(states_ref[...])
    return nt_dot(high, ct_hi) + nt_dot(low, ct_hi) + nt_dot(high, ct_lo)


def local_state_kernel(
    u_ref, init_ref, lines_ref, wide_ref, reads_ref, skip_ref, y_ref, push_ref
):
    make_push(u_ref[...], *drive_matrices(lines_ref, u_ref.shape[1]), push_ref)
    width = push_ref.shape[1] // 2
    lr = jnp.broadcast_to(wide_ref[0:1, :width], (8, width))
    li = jnp.broadcast_to(wide_ref[0:1, width:], (8, width))

    def step(k, carried):
        sr, si = carried
        at = pl.multiple_of(k * 8, 8)
        nr = lr * sr - li * si + push_ref[pl.ds(at, 8), :width]
        ni = lr * si + li * sr + push_ref[pl.ds(at, 8), width:]
        push_ref[pl.ds(at, 8), :width] = nr
        push_ref[pl.ds(at, 8), width:] = ni
        return nr, ni

    lax.fori_loop(
        0, push_ref.shape[0] // 8, step, (init_ref[:, :width], init_ref[:, width:]), unroll=8
    )
    y_ref[...] = (
        read_states(push_ref, *read_matrices(reads_ref, width))
        + skip_ref[...] * u_ref[...].astype(F32)
    )


def score_block(q_ref, payload_ref, later_ref, diagonal):
    rows = q_ref.shape[1]
    keys, values = payload_ref[0:rows, 0:128], payload_ref[0:rows, 128:256]
    tail = payload_ref[rows : rows + 16, :].astype(F32)
    biases = (
        jnp.concatenate([tail[0:1, :], tail[1:2, 0:128]], axis=1),
        jnp.concatenate([tail[1:2, 128:256], tail[2:3, :]], axis=1),
    )
    outs, totals = [], []
    for h in range(2):
        z = nt_dot(q_ref[h], keys) + biases[h]
        loss = jnp.log(1.0 + jnp.exp(z))
        if diagonal:
            causal = lax.broadcasted_iota(jnp.int32, z.shape, 1) < lax.broadcasted_iota(
                jnp.int32, z.shape, 0
            )
            masked = jnp.where(causal, loss, 0.0)
        else:
            masked = loss
        later = nn_dot(masked.astype(BF16), later_ref[...])
        weights = jnp.exp((z - loss) - later)
        if diagonal:
            weights = jnp.where(causal, weights, 0.0)
        outs.append(nn_dot(weights.astype(BF16), values))
        totals.append(later[:, 0:1] + masked[:, 0:1])
    low = lanes_low((rows, 128))
    return jnp.where(low, outs[0], outs[1]), jnp.where(low, totals[0], totals[1])


def first_kernel(q_ref, payload_ref, later_ref, *refs):
    *state_refs, acc_ref, tot_ref, y_ref, states_ref = refs
    local_state_kernel(*state_refs, y_ref, states_ref)
    out, total = score_block(q_ref, payload_ref, later_ref, True)
    acc_ref[...] = out
    tot_ref[...] = total


def entering_state(payload_ref, tab_ref, carry_ref, power):
    rows = payload_ref.shape[0] - 16
    tail = payload_ref[rows : rows + 16, :].astype(F32)
    er, ei = tail[8:10] + tail[12:14], tail[10:12] + tail[14:16]
    wr, wi = tab_ref[4 * power : 4 * power + 2, :], tab_ref[4 * power + 2 : 4 * power + 4, :]
    carry_ref[0:2, :] += wr * er - wi * ei
    carry_ref[2:4, :] += wr * ei + wi * er


def step_kernel(
    place_ref, q_ref, later_ref, tab_ref, up_ref, down_ref,
    acc_in, tot_in, wrap_in, carry_in, acc_ref, tot_ref, wrap_ref, carry_ref, *, step, blocks,
):
    here = place_ref[0]
    acc_ref[...] = acc_in[...]
    tot_ref[...] = tot_in[...]
    wrap_ref[...] = wrap_in[...]
    carry_ref[...] = carry_in[...]
    if step < blocks // 2:

        @pl.when(here >= step)
        def _():
            out, total = score_block(q_ref, up_ref, later_ref, False)
            acc_ref[...] += out * jnp.exp(-tot_ref[...])
            tot_ref[...] += total
            entering_state(up_ref, tab_ref, carry_ref, step - 1)

    @pl.when(here >= blocks - step)
    def _():
        out, total = score_block(q_ref, down_ref, later_ref, False)
        wrap_ref[...] = wrap_ref[...] * jnp.exp(-total) + out
        entering_state(down_ref, tab_ref, carry_ref, blocks - 1 - step)


def finish_kernel(
    acc_ref, tot_ref, wrap_ref, carry_ref, y_ref, chunk_ref, wide_ref, reads_ref,
    out_ref, states_ref,
):
    rows = acc_ref.shape[0]
    width = states_ref.shape[1] // 2
    sr = jnp.concatenate([carry_ref[0:1, :], carry_ref[1:2, :]], axis=1)
    si = jnp.concatenate([carry_ref[2:3, :], carry_ref[3:4, :]], axis=1)
    zr, zi = cmul(chunk_ref[:, :width], chunk_ref[:, width:], sr, si)
    lr = jnp.broadcast_to(wide_ref[0:1, :width], (8, width))
    li = jnp.broadcast_to(wide_ref[0:1, width:], (8, width))

    def step(k, carried):
        zr, zi = carried
        at = pl.multiple_of(k * 8, 8)
        states_ref[pl.ds(at, 8), :width] = zr
        states_ref[pl.ds(at, 8), width:] = zi
        return cmul(lr, li, zr, zi)

    lax.fori_loop(0, rows // 8, step, (zr, zi), unroll=8)
    mixed = y_ref[...] + read_states(states_ref, *read_matrices(reads_ref, width))
    state_out = jax.nn.gelu(mixed).astype(BF16)
    state_out = nn_dot(reorder_matrix(rows, 8, True), state_out).astype(BF16)
    attended = acc_ref[...] + wrap_ref[...] * jnp.exp(-tot_ref[...])
    low = lanes_low(attended.shape)
    square = attended * attended
    first = jnp.sum(jnp.where(low, square, 0.0), axis=1, keepdims=True)
    second = jnp.sum(jnp.where(low, 0.0, square), axis=1, keepdims=True)
    scale = jnp.where(
        low,
        lax.rsqrt(first * (1.0 / HEAD_DIM) + EPSILON),
        lax.rsqrt(second * (1.0 / HEAD_DIM) + EPSILON),
    )
    attn_out = (attended * scale).astype(BF16)
    out_ref[:, 0:128] = state_out
    out_ref[:, 128:256] = attn_out


def call(kernel, outs, args, scratch=(), smem=0, flops=1, aliases={}, limit=16):
    return pl.pallas_call(
        kernel,
        out_shape=outs,
        in_specs=[SMEM] * smem + [VMEM] * (len(args) - smem),
        out_specs=jax.tree.map(lambda _: VMEM, outs),
        scratch_shapes=list(scratch),
        input_output_aliases=aliases,
        compiler_params=pltpu.CompilerParams(vmem_limit_bytes=limit * 2**20),
        cost_estimate=pl.CostEstimate(flops=flops, bytes_accessed=10**6, transcendentals=0),
    )(*args)


def shape(dims, dtype=F32):
    return jax.ShapeDtypeStruct(dims, dtype)


def on_device(
    tokens,
    norm_gain,
    w_input,
    w_query,
    w_key,
    w_value,
    query_gain,
    key_gain,
    key_bias,
    eigen_real,
    eigen_imag,
    log_step,
    input_real,
    input_imag,
    read_real,
    read_imag,
    skip_gain,
    w_out_state,
    w_out_attn,
):
    blocks = lax.axis_size("sp")
    rows = key_bias.shape[0]
    piece = rows // 8
    groups = eigen_real.shape[0]
    width = groups * STATE
    channels = groups * GROUP
    place = jnp.stack([lax.axis_index("sp"), lax.axis_index("tp_1")]).astype(jnp.int32)

    copies = call(
        norm_kernel,
        shape((4, *tokens.shape), BF16),
        (tokens, norm_gain.reshape(1, -1)),
    )
    mine = lax.all_to_all(copies, "tp_0", 0, 0, tiled=True).reshape(4 * piece, -1)

    w_joined = jnp.concatenate([w_input, w_query, w_key, w_value], axis=1)
    w_out = jnp.concatenate([w_out_state, w_out_attn], axis=0)
    w_out_copies = jnp.broadcast_to(w_out[None], (4, *w_out.shape))
    decay_r, decay_i, drive_r, drive_i = discretize(
        eigen_real, eigen_imag, log_step, input_real, input_imag
    )
    lines = jnp.concatenate(
        [jnp.transpose(part, (2, 0, 1)).reshape(GROUP, width) for part in (drive_r, drive_i)]
    )
    reads = [part.reshape(channels, STATE) for part in (read_real, read_imag)]
    reads = jnp.concatenate([jnp.concatenate([part, part], axis=1) for part in reads])
    decay = jnp.stack([decay_r.reshape(-1), decay_i.reshape(-1)])
    bias8 = jnp.pad(jnp.transpose(key_bias).reshape(-1, 256), ((0, 5), (0, 0)))
    gains = [jnp.tile(g, 2).reshape(1, 128) for g in (query_gain, key_gain)]
    skip = skip_gain.reshape(1, -1)
    decay, lines, reads, w_joined, w_out_copies, bias8, gains, skip, place = (
        lax.optimization_barrier(
            (decay, lines, reads, w_joined, w_out_copies, bias8, gains, skip, place)
        )
    )
    tables = call(
        lambda *refs: prepare_kernel(*refs, blocks=blocks, chunk=piece),
        (
            shape((4 * blocks, width // 2)),
            shape((8, 2 * width)),
            shape((8, 2 * width)),
            shape((rows, rows), BF16),
        ),
        (decay,),
    )
    mine, tables = lax.optimization_barrier((mine, tables))
    tab, chunk, wide, later = tables
    other = lax.ppermute(mine, "tp_1", [(0, 1), (1, 0)])

    found = call(
        half_project_kernel, shape((4 * piece, 512), BF16), (mine, w_joined), flops=10**9
    )
    q, payload, u_perm, init = call(
        project_kernel,
        (
            shape((2, rows, 128), BF16),
            shape((rows + 16, 256), BF16),
            shape((rows, channels), BF16),
            shape((8, 2 * width)),
        ),
        (place, found, other, w_joined, *gains, bias8, lines, wide),
        scratch=(pltpu.VMEM((rows, 512), BF16), pltpu.VMEM((rows, 2 * width), F32)),
        smem=1,
        flops=4 * 10**9,
    )

    acc, tot, y_local = call(
        first_kernel,
        (shape((rows, 128)), shape((rows, 128)), shape((rows, channels))),
        (q, payload, later, u_perm, init, lines, wide, reads, skip),
        scratch=(pltpu.VMEM((rows, 2 * width), F32),),
        flops=4 * 10**9,
    )
    wrap = jnp.zeros((rows, 128), F32)
    carry = jnp.zeros((8, width // 2), F32)
    up = down = payload
    half = blocks // 2
    for step in range(1, half + 1):
        if step < half:
            up = lax.ppermute(up, "sp", [(i - 1, i) for i in range(step, blocks)])
        down = lax.ppermute(
            down, "sp", [((j - step + 1) % blocks, (j - step) % blocks) for j in range(half)]
        )
        acc, tot, wrap, carry = call(
            lambda *refs, step=step: step_kernel(*refs, step=step, blocks=blocks),
            (shape((rows, 128)), shape((rows, 128)), shape((rows, 128)), shape(carry.shape)),
            (place, q, later, tab, up, down, acc, tot, wrap, carry),
            smem=1,
            flops=3 * 10**9,
            aliases={6: 0, 7: 1, 8: 2, 9: 3},
        )
        if step == 1:
            acc, w_out_copies = lax.optimization_barrier((acc, w_out_copies))
            w_out_mine = lax.all_to_all(w_out_copies, "tp_0", 0, 0, tiled=True)
        if step == half - 1:
            acc, w_out_mine = lax.optimization_barrier((acc, w_out_mine))
            w_out_other = lax.ppermute(w_out_mine, "tp_1", [(0, 1), (1, 0)])
    both = call(
        finish_kernel,
        shape((rows, 2 * channels), BF16),
        (acc, tot, wrap, carry, y_local, chunk, wide, reads),
        scratch=(pltpu.VMEM((rows, 2 * width), F32),),
        flops=3 * 10**9,
    )
    parts = lax.all_to_all(both.reshape(8, piece, -1), TP, 0, 0, tiled=True)
    return call(
        merge_kernel,
        shape((piece, w_out.shape[1]), BF16),
        (place, parts, w_out_mine, w_out_other),
        smem=1,
        flops=10**9,
        limit=MERGE_LIMIT,
    )


def solution(mesh):
    torus = Mesh(
        mesh.devices.reshape(mesh.shape["sp"], mesh.shape["fs"], 4, 2), ("sp", "fs", "tp_0", "tp_1")
    )
    placed = (
        P(FS_SP_TP, None),
        P(),
        P(None, TP),
        P(None, TP),
        P(None, TP),
        P(None, TP),
        P(),
        P(),
        P(("fs", "sp"), TP),
        P(TP, None),
        P(TP, None),
        P(TP),
        P(TP, None, None),
        P(TP, None, None),
        P(TP, None, None),
        P(TP, None, None),
        P(TP),
        P(TP, None),
        P(TP, None),
    )

    return jax.shard_map(
        on_device, mesh=torus, in_specs=placed, out_specs=P(FS_SP_TP, None), check_vma=False
    )
```

```python
import jax
import jax.numpy as jnp
from jax import lax
from jax.experimental import pallas as pl
from jax.experimental.pallas import tpu as pltpu
from jax.sharding import Mesh
from jax.sharding import PartitionSpec as P


GROUP = 16
STATE = 64
HEAD_DIM = 64
TP = ("tp_0", "tp_1")
FS_SP_TP = ("fs", "sp", "tp_0", "tp_1")
EPSILON = 1e-06
F32 = jnp.float32
BF16 = jnp.bfloat16


VMEM = pl.BlockSpec(memory_space=pltpu.VMEM)
SMEM = pl.BlockSpec(memory_space=pltpu.SMEM)


def discretize(eigen_real, eigen_imag, log_step, input_real, input_imag):
    step_size = jnp.exp(log_step)[:, None]
    rotation = eigen_imag * step_size
    shrink = jnp.expm1(eigen_real * step_size)
    cosine = jnp.cos(rotation)
    sine_part = jnp.sin(rotation)
    decay_r = (1.0 + shrink) * cosine
    decay_i = (1.0 + shrink) * sine_part
    minus_r = shrink * cosine - 2.0 * jnp.square(jnp.sin(0.5 * rotation))
    modulus = jnp.square(eigen_real) + jnp.square(eigen_imag)
    factor_r = (minus_r * eigen_real + decay_i * eigen_imag) / modulus
    factor_i = (decay_i * eigen_real - minus_r * eigen_imag) / modulus
    drive_r = factor_r[..., None] * input_real - factor_i[..., None] * input_imag
    drive_i = factor_r[..., None] * input_imag + factor_i[..., None] * input_real
    return (decay_r, decay_i, drive_r, drive_i)


def split(value):
    high = value.astype(BF16)
    low = (value - high.astype(F32)).astype(BF16)
    return high, low


def cmul(ar, ai, br, bi):
    return ar * br - ai * bi, ar * bi + ai * br


def nt_dot(a, b):
    return lax.dot_general(a, b, (((1,), (1,)), ((), ())), preferred_element_type=F32)


def nn_dot(a, b):
    return jnp.dot(a, b, preferred_element_type=F32)


def lanes_low(shape):
    return lax.broadcasted_iota(jnp.int32, shape, len(shape) - 1) < HEAD_DIM


def reorder_matrix(rows, chunks, inverse):
    length = rows // chunks
    r = lax.broadcasted_iota(jnp.int32, (rows, rows), 1 if inverse else 0)
    t = lax.broadcasted_iota(jnp.int32, (rows, rows), 0 if inverse else 1)
    source = (r & (chunks - 1)) * length + (r >> 3)
    return jnp.where(t == source, 1.0, 0.0).astype(BF16)


def norm_kernel(tokens_ref, gain_ref, out_ref):
    wide = tokens_ref[...].astype(F32)
    mean = jnp.sum(wide * wide, axis=1, keepdims=True) * (1.0 / wide.shape[1])
    normed = (wide * lax.rsqrt(mean + EPSILON) * gain_ref[...]).astype(BF16)
    for k in range(out_ref.shape[0]):
        out_ref[k] = normed


def half_project_kernel(mine_ref, w_ref, found_ref):
    found_ref[...] = nn_dot(mine_ref[...], w_ref[...]).astype(BF16)


def merge_kernel(place_ref, parts_ref, mine_ref, other_ref, out_ref, total_ref):
    a = pl.program_id(0)
    core = place_ref[1]

    @pl.when(a == 0)
    def _():
        total_ref[...] = jnp.zeros_like(total_ref)

    total_ref[...] += nn_dot(parts_ref[2 * a + core], mine_ref[0]) + nn_dot(
        parts_ref[2 * a + 1 - core], other_ref[a]
    )

    @pl.when(a == pl.num_programs(0) - 1)
    def _():
        out_ref[...] = total_ref[...].astype(BF16)


def block_diagonal(parts, channels, width):
    row = lax.broadcasted_iota(jnp.int32, (channels, width), 0) >> 4
    lane = lax.broadcasted_iota(jnp.int32, (channels, width), 1) >> 6
    return split(jnp.concatenate([jnp.where(row == lane, p, 0.0) for p in parts], axis=1))


def drive_matrices(lines_ref, channels):
    width = lines_ref.shape[1]
    parts = [lines_ref[j * GROUP : (j + 1) * GROUP, :] for j in range(2)]
    parts = [jnp.concatenate([p] * (channels // GROUP), axis=0) for p in parts]
    return block_diagonal(parts, channels, width)


def read_matrices(reads_ref, width):
    channels = reads_ref.shape[0] // 2
    parts = [reads_ref[j * channels : (j + 1) * channels, :] for j in range(2)]
    parts = [jnp.concatenate([p] * (width // 128), axis=1) for p in (parts[0], -parts[1])]
    return block_diagonal(parts, channels, width)


def prepare_kernel(decay_ref, tab_ref, chunk_ref, wide_ref, later_ref, *, blocks, chunk):
    rows = later_ref.shape
    below = lax.broadcasted_iota(jnp.int32, rows, 0) > lax.broadcasted_iota(jnp.int32, rows, 1)
    later_ref[...] = jnp.where(below, 1.0, 0.0).astype(BF16)
    dr, di = decay_ref[0:1, :], decay_ref[1:2, :]
    width = dr.shape[1]
    half = width // 2
    squares = [(dr, di)]
    for _ in range(9):
        a, b = squares[-1]
        squares.append(cmul(a, b, a, b))

    def power(n):
        out = None
        for k in range(10):
            if n >> k & 1:
                out = squares[k] if out is None else cmul(*out, *squares[k])
        return out

    p_chunk = power(chunk)
    p_block = power(chunk * 8)
    now = (jnp.ones_like(dr), jnp.zeros_like(dr))
    for k in range(blocks):
        for j, part in enumerate(now):
            tab_ref[4 * k + 2 * j : 4 * k + 2 * j + 1, :] = part[:, :half]
            tab_ref[4 * k + 2 * j + 1 : 4 * k + 2 * j + 2, :] = part[:, half:]
        now = cmul(*now, *p_block)
    now = (dr, di)
    for c in range(8):
        chunk_ref[c : c + 1, :width] = now[0]
        chunk_ref[c : c + 1, width:] = now[1]
        now = cmul(*now, *p_chunk)
    p2 = cmul(*p_chunk, *p_chunk)
    p4 = cmul(*p2, *p2)
    for k, (a, b) in enumerate([(dr, di), p_chunk, p2, p4]):
        wide_ref[k : k + 1, :width] = a
        wide_ref[k : k + 1, width:] = b
    wide_ref[4:8, :] = jnp.zeros((4, 2 * width), F32)


def make_push(u_perm, b_hi, b_lo, push_ref):
    push_ref[...] = nn_dot(u_perm, b_hi) + nn_dot(u_perm, b_lo)


def project_kernel(
    place_ref, found_ref, other_ref, w_ref, qg_ref, kg_ref, bias_ref, lines_ref, wide_ref,
    q_ref, payload_ref, u_ref, init_ref, rows_ref, push_ref,
):
    rows = payload_ref.shape[0] - 16
    piece = rows // 8
    core = place_ref[1]
    found_other = nn_dot(other_ref[...], w_ref[...]).astype(BF16)
    for found, where in ((found_ref[...], core), (found_other, 1 - core)):
        for a in range(4):
            at = pl.multiple_of((2 * a + where) * piece, 16)
            rows_ref[pl.ds(at, piece), :] = found[a * piece : (a + 1) * piece, :]
    low = lanes_low((rows, 2 * HEAD_DIM))

    def normed(raw, gain):
        wide = raw.astype(F32)
        square = wide * wide
        first = jnp.sum(jnp.where(low, square, 0.0), axis=1, keepdims=True)
        second = jnp.sum(jnp.where(low, 0.0, square), axis=1, keepdims=True)
        scale = jnp.where(
            low,
            lax.rsqrt(first * (1.0 / HEAD_DIM) + EPSILON),
            lax.rsqrt(second * (1.0 / HEAD_DIM) + EPSILON),
        )
        return (wide * scale * gain).astype(BF16)

    u = rows_ref[:, 0:128]
    u_perm = nn_dot(reorder_matrix(rows, 8, False), u).astype(BF16)
    u_ref[...] = u_perm
    make_push(u_perm, *drive_matrices(lines_ref, u_perm.shape[1]), push_ref)
    queries = normed(rows_ref[:, 128:256], qg_ref[...]).astype(F32) * HEAD_DIM ** (-0.5)
    q_ref[0] = jnp.where(low, queries, 0.0).astype(BF16)
    q_ref[1] = jnp.where(low, 0.0, queries).astype(BF16)
    payload_ref[0:rows, 0:128] = normed(rows_ref[:, 256:384], kg_ref[...])
    payload_ref[0:rows, 128:256] = rows_ref[:, 384:512]
    width = push_ref.shape[1] // 2
    lr = jnp.broadcast_to(wide_ref[0:1, :width], (8, width))
    li = jnp.broadcast_to(wide_ref[0:1, width:], (8, width))

    def step(k, carried):
        sr, si = carried
        at = pl.multiple_of(k * 8, 8)
        nr = lr * sr - li * si + push_ref[pl.ds(at, 8), :width]
        ni = lr * si + li * sr + push_ref[pl.ds(at, 8), width:]
        return nr, ni

    zero = jnp.zeros((8, width), F32)
    er, ei = lax.fori_loop(0, piece, step, (zero, zero), unroll=8)
    place = lax.broadcasted_iota(jnp.int32, (8, width), 0)
    for k in range(3):
        shift = 1 << k
        pr, pi = wide_ref[k + 1 : k + 2, :width], wide_ref[k + 1 : k + 2, width:]
        br = jnp.where(place >= shift, pltpu.roll(er, shift, 0), 0.0)
        bi = jnp.where(place >= shift, pltpu.roll(ei, shift, 0), 0.0)
        er, ei = er + pr * br - pi * bi, ei + pr * bi + pi * br
    init_ref[:, :width] = jnp.where(place >= 1, pltpu.roll(er, 1, 0), 0.0)
    init_ref[:, width:] = jnp.where(place >= 1, pltpu.roll(ei, 1, 0), 0.0)
    half = width // 2
    end = [er[7:8, :half], er[7:8, half:], ei[7:8, :half], ei[7:8, half:]]
    highs = [e.astype(BF16).astype(F32) for e in end]
    lows = [e - h for e, h in zip(end, highs)]
    tail = jnp.concatenate([bias_ref[...].astype(F32)] + highs + lows, axis=0)
    payload_ref[rows : rows + 16, :] = tail.astype(BF16)


def read_states(states_ref, ct_hi, ct_lo):
    high, low = split(states_ref[...])
    return nt_dot(high, ct_hi) + nt_dot(low, ct_hi) + nt_dot(high, ct_lo)


def local_state_kernel(
    u_ref, init_ref, lines_ref, wide_ref, reads_ref, skip_ref, y_ref, push_ref
):
    make_push(u_ref[...], *drive_matrices(lines_ref, u_ref.shape[1]), push_ref)
    width = push_ref.shape[1] // 2
    lr = jnp.broadcast_to(wide_ref[0:1, :width], (8, width))
    li = jnp.broadcast_to(wide_ref[0:1, width:], (8, width))

    def step(k, carried):
        sr, si = carried
        at = pl.multiple_of(k * 8, 8)
        nr = lr * sr - li * si + push_ref[pl.ds(at, 8), :width]
        ni = lr * si + li * sr + push_ref[pl.ds(at, 8), width:]
        push_ref[pl.ds(at, 8), :width] = nr
        push_ref[pl.ds(at, 8), width:] = ni
        return nr, ni

    lax.fori_loop(
        0, push_ref.shape[0] // 8, step, (init_ref[:, :width], init_ref[:, width:]), unroll=8
    )
    y_ref[...] = (
        read_states(push_ref, *read_matrices(reads_ref, width))
        + skip_ref[...] * u_ref[...].astype(F32)
    )


def score_block(q_ref, payload_ref, later_ref, diagonal):
    rows = q_ref.shape[1]
    keys, values = payload_ref[0:rows, 0:128], payload_ref[0:rows, 128:256]
    tail = payload_ref[rows : rows + 16, :].astype(F32)
    biases = (
        jnp.concatenate([tail[0:1, :], tail[1:2, 0:128]], axis=1),
        jnp.concatenate([tail[1:2, 128:256], tail[2:3, :]], axis=1),
    )
    outs, totals = [], []
    for h in range(2):
        z = nt_dot(q_ref[h], keys) + biases[h]
        loss = jnp.log(1.0 + jnp.exp(z))
        if diagonal:
            causal = lax.broadcasted_iota(jnp.int32, z.shape, 1) < lax.broadcasted_iota(
                jnp.int32, z.shape, 0
            )
            masked = jnp.where(causal, loss, 0.0)
        else:
            masked = loss
        later = nn_dot(masked.astype(BF16), later_ref[...])
        weights = jnp.exp((z - loss) - later)
        if diagonal:
            weights = jnp.where(causal, weights, 0.0)
        outs.append(nn_dot(weights.astype(BF16), values))
        totals.append(later[:, 0:1] + masked[:, 0:1])
    low = lanes_low((rows, 128))
    return jnp.where(low, outs[0], outs[1]), jnp.where(low, totals[0], totals[1])


def first_kernel(q_ref, payload_ref, later_ref, *refs):
    *state_refs, acc_ref, tot_ref, y_ref, states_ref = refs
    local_state_kernel(*state_refs, y_ref, states_ref)
    out, total = score_block(q_ref, payload_ref, later_ref, True)
    acc_ref[...] = out
    tot_ref[...] = total


def entering_state(payload_ref, tab_ref, carry_ref, power):
    rows = payload_ref.shape[0] - 16
    tail = payload_ref[rows : rows + 16, :].astype(F32)
    er, ei = tail[8:10] + tail[12:14], tail[10:12] + tail[14:16]
    wr, wi = tab_ref[4 * power : 4 * power + 2, :], tab_ref[4 * power + 2 : 4 * power + 4, :]
    carry_ref[0:2, :] += wr * er - wi * ei
    carry_ref[2:4, :] += wr * ei + wi * er


def step_kernel(
    place_ref, q_ref, later_ref, tab_ref, up_ref, down_ref,
    acc_in, tot_in, wrap_in, carry_in, acc_ref, tot_ref, wrap_ref, carry_ref, *, step, blocks, ups,
):
    here = place_ref[0]
    acc_ref[...] = acc_in[...]
    tot_ref[...] = tot_in[...]
    wrap_ref[...] = wrap_in[...]
    carry_ref[...] = carry_in[...]
    if step <= ups:

        @pl.when(here >= step)
        def _():
            out, total = score_block(q_ref, up_ref, later_ref, False)
            acc_ref[...] += out * jnp.exp(-tot_ref[...])
            tot_ref[...] += total
            entering_state(up_ref, tab_ref, carry_ref, step - 1)

    if step < blocks - ups:

        @pl.when(here >= blocks - step)
        def _():
            out, total = score_block(q_ref, down_ref, later_ref, False)
            wrap_ref[...] = wrap_ref[...] * jnp.exp(-total) + out
            entering_state(down_ref, tab_ref, carry_ref, blocks - 1 - step)


def last_kernel(*refs, **sizes):
    ins, (rest, out_ref, acc_ref, tot_ref, wrap_ref, carry_ref, states_ref) = (
        refs[:10],
        (refs[10:14], *refs[14:]),
    )
    step_kernel(*ins, acc_ref, tot_ref, wrap_ref, carry_ref, **sizes)
    finish_kernel(acc_ref, tot_ref, wrap_ref, carry_ref, *rest, out_ref, states_ref)


def finish_kernel(
    acc_ref, tot_ref, wrap_ref, carry_ref, y_ref, chunk_ref, wide_ref, reads_ref,
    out_ref, states_ref,
):
    rows = acc_ref.shape[0]
    width = states_ref.shape[1] // 2
    sr = jnp.concatenate([carry_ref[0:1, :], carry_ref[1:2, :]], axis=1)
    si = jnp.concatenate([carry_ref[2:3, :], carry_ref[3:4, :]], axis=1)
    zr, zi = cmul(chunk_ref[:, :width], chunk_ref[:, width:], sr, si)
    lr = jnp.broadcast_to(wide_ref[0:1, :width], (8, width))
    li = jnp.broadcast_to(wide_ref[0:1, width:], (8, width))

    def step(k, carried):
        zr, zi = carried
        at = pl.multiple_of(k * 8, 8)
        states_ref[pl.ds(at, 8), :width] = zr
        states_ref[pl.ds(at, 8), width:] = zi
        return cmul(lr, li, zr, zi)

    lax.fori_loop(0, rows // 8, step, (zr, zi), unroll=8)
    mixed = y_ref[...] + read_states(states_ref, *read_matrices(reads_ref, width))
    state_out = jax.nn.gelu(mixed).astype(BF16)
    state_out = nn_dot(reorder_matrix(rows, 8, True), state_out).astype(BF16)
    attended = acc_ref[...] + wrap_ref[...] * jnp.exp(-tot_ref[...])
    low = lanes_low(attended.shape)
    square = attended * attended
    first = jnp.sum(jnp.where(low, square, 0.0), axis=1, keepdims=True)
    second = jnp.sum(jnp.where(low, 0.0, square), axis=1, keepdims=True)
    scale = jnp.where(
        low,
        lax.rsqrt(first * (1.0 / HEAD_DIM) + EPSILON),
        lax.rsqrt(second * (1.0 / HEAD_DIM) + EPSILON),
    )
    attn_out = (attended * scale).astype(BF16)
    out_ref[:, 0:128] = state_out
    out_ref[:, 128:256] = attn_out


def call(kernel, outs, args, scratch=(), smem=0, flops=1, aliases={}, limit=16):
    return pl.pallas_call(
        kernel,
        out_shape=outs,
        in_specs=[SMEM] * smem + [VMEM] * (len(args) - smem),
        out_specs=jax.tree.map(lambda _: VMEM, outs),
        scratch_shapes=list(scratch),
        input_output_aliases=aliases,
        compiler_params=pltpu.CompilerParams(vmem_limit_bytes=limit * 2**20),
        cost_estimate=pl.CostEstimate(flops=flops, bytes_accessed=10**6, transcendentals=0),
    )(*args)


def shape(dims, dtype=F32):
    return jax.ShapeDtypeStruct(dims, dtype)


def on_device(
    tokens,
    norm_gain,
    w_input,
    w_query,
    w_key,
    w_value,
    query_gain,
    key_gain,
    key_bias,
    eigen_real,
    eigen_imag,
    log_step,
    input_real,
    input_imag,
    read_real,
    read_imag,
    skip_gain,
    w_out_state,
    w_out_attn,
):
    blocks = lax.axis_size("sp")
    rows = key_bias.shape[0]
    piece = rows // 8
    groups = eigen_real.shape[0]
    width = groups * STATE
    channels = groups * GROUP
    place = jnp.stack([lax.axis_index("sp"), lax.axis_index("tp_1")]).astype(jnp.int32)

    copies = call(
        norm_kernel,
        shape((4, *tokens.shape), BF16),
        (tokens, norm_gain.reshape(1, -1)),
        limit=60,
    )
    mine = lax.all_to_all(copies, "tp_0", 0, 0, tiled=True).reshape(4 * piece, -1)

    w_joined = jnp.concatenate([w_input, w_query, w_key, w_value], axis=1)
    w_out = jnp.concatenate([w_out_state, w_out_attn], axis=0)
    w_out_copies = jnp.broadcast_to(w_out[None], (4, *w_out.shape))
    decay_r, decay_i, drive_r, drive_i = discretize(
        eigen_real, eigen_imag, log_step, input_real, input_imag
    )
    lines = jnp.concatenate(
        [jnp.transpose(part, (2, 0, 1)).reshape(GROUP, width) for part in (drive_r, drive_i)]
    )
    reads = [part.reshape(channels, STATE) for part in (read_real, read_imag)]
    reads = jnp.concatenate([jnp.concatenate([part, part], axis=1) for part in reads])
    decay = jnp.stack([decay_r.reshape(-1), decay_i.reshape(-1)])
    bias8 = jnp.pad(jnp.transpose(key_bias).reshape(-1, 256), ((0, 5), (0, 0)))
    gains = [jnp.tile(g, 2).reshape(1, 128) for g in (query_gain, key_gain)]
    skip = skip_gain.reshape(1, -1)
    decay, lines, reads, w_joined, w_out_copies, bias8, gains, skip, place = (
        lax.optimization_barrier(
            (decay, lines, reads, w_joined, w_out_copies, bias8, gains, skip, place)
        )
    )
    tables = call(
        lambda *refs: prepare_kernel(*refs, blocks=blocks, chunk=piece),
        (
            shape((4 * blocks, width // 2)),
            shape((8, 2 * width)),
            shape((8, 2 * width)),
            shape((rows, rows), BF16),
        ),
        (decay,),
    )
    mine, tables = lax.optimization_barrier((mine, tables))
    tab, chunk, wide, later = tables
    other = lax.ppermute(mine, "tp_1", [(0, 1), (1, 0)])

    found = call(
        half_project_kernel, shape((4 * piece, 512), BF16), (mine, w_joined), flops=10**9
    )
    q, payload, u_perm, init = call(
        project_kernel,
        (
            shape((2, rows, 128), BF16),
            shape((rows + 16, 256), BF16),
            shape((rows, channels), BF16),
            shape((8, 2 * width)),
        ),
        (place, found, other, w_joined, *gains, bias8, lines, wide),
        scratch=(pltpu.VMEM((rows, 512), BF16), pltpu.VMEM((rows, 2 * width), F32)),
        smem=1,
        flops=4 * 10**9,
    )

    acc, tot, y_local = call(
        first_kernel,
        (shape((rows, 128)), shape((rows, 128)), shape((rows, channels))),
        (q, payload, later, u_perm, init, lines, wide, reads, skip),
        scratch=(pltpu.VMEM((rows, 2 * width), F32),),
        flops=4 * 10**9,
    )
    wrap = jnp.zeros((rows, 128), F32)
    carry = jnp.zeros((8, width // 2), F32)
    up = down = payload
    half = blocks // 2
    for step in range(1, half + 1):
        up = lax.ppermute(up, "sp", [(i - 1, i) for i in range(step, blocks)])
        if step < half:
            hops = [((j - step + 1) % blocks, (j - step) % blocks) for j in range(half - 1)]
            down = lax.ppermute(down, "sp", hops)
        if step == half:
            break
        acc, tot, wrap, carry = call(
            lambda *refs, step=step: step_kernel(*refs, step=step, blocks=blocks, ups=half),
            (shape((rows, 128)), shape((rows, 128)), shape((rows, 128)), shape(carry.shape)),
            (place, q, later, tab, up, down, acc, tot, wrap, carry),
            smem=1,
            flops=3 * 10**9,
            aliases={6: 0, 7: 1, 8: 2, 9: 3},
        )
        if step == 1:
            acc, w_out_copies = lax.optimization_barrier((acc, w_out_copies))
            w_out_mine = lax.all_to_all(w_out_copies, "tp_0", 0, 0, tiled=True)
        if step == half - 1:
            acc, w_out_mine = lax.optimization_barrier((acc, w_out_mine))
            w_out_other = lax.ppermute(w_out_mine, "tp_1", [(0, 1), (1, 0)])
    state = [shape((rows, 128)), shape((rows, 128)), shape((rows, 128)), shape(carry.shape)]
    both = call(
        lambda *refs: last_kernel(*refs, step=half, blocks=blocks, ups=half),
        shape((rows, 2 * channels), BF16),
        (place, q, later, tab, up, down, acc, tot, wrap, carry, y_local, chunk, wide, reads),
        scratch=[pltpu.VMEM(s.shape, F32) for s in state]
        + [pltpu.VMEM((rows, 2 * width), F32)],
        smem=1,
        flops=3 * 10**9,
    )
    parts = lax.all_to_all(both.reshape(8, piece, -1), TP, 0, 0, tiled=True)
    columns = w_out.shape[1]
    return pl.pallas_call(
        merge_kernel,
        out_shape=shape((piece, columns), BF16),
        grid=(4,),
        in_specs=[
            SMEM,
            VMEM,
            pl.BlockSpec((1, w_out.shape[0], columns), lambda a: (a, 0, 0)),
            VMEM,
        ],
        out_specs=pl.BlockSpec((piece, columns), lambda a: (0, 0)),
        scratch_shapes=[pltpu.VMEM((piece, columns), F32)],
        compiler_params=pltpu.CompilerParams(vmem_limit_bytes=16 * 2**20),
        cost_estimate=pl.CostEstimate(flops=10**9, bytes_accessed=10**7, transcendentals=0),
    )(place, parts, w_out_mine, w_out_other)


def solution(mesh):
    torus = Mesh(
        mesh.devices.reshape(mesh.shape["sp"], mesh.shape["fs"], 4, 2), ("sp", "fs", "tp_0", "tp_1")
    )
    placed = (
        P(FS_SP_TP, None),
        P(),
        P(None, TP),
        P(None, TP),
        P(None, TP),
        P(None, TP),
        P(),
        P(),
        P(("fs", "sp"), TP),
        P(TP, None),
        P(TP, None),
        P(TP),
        P(TP, None, None),
        P(TP, None, None),
        P(TP, None, None),
        P(TP, None, None),
        P(TP),
        P(TP, None),
        P(TP, None),
    )

    return jax.shard_map(
        on_device, mesh=torus, in_specs=placed, out_specs=P(FS_SP_TP, None), check_vma=False
    )
```

```python
import jax
import jax.numpy as jnp
from jax import lax
from jax.experimental import pallas as pl
from jax.experimental.pallas import tpu as pltpu
from jax.sharding import Mesh
from jax.sharding import PartitionSpec as P


GROUP = 16
STATE = 64
HEAD_DIM = 64
TP = ("tp_0", "tp_1")
FS_SP_TP = ("fs", "sp", "tp_0", "tp_1")
EPSILON = 1e-06
F32 = jnp.float32
BF16 = jnp.bfloat16


VMEM = pl.BlockSpec(memory_space=pltpu.VMEM)
SMEM = pl.BlockSpec(memory_space=pltpu.SMEM)


def discretize(eigen_real, eigen_imag, log_step, input_real, input_imag):
    step_size = jnp.exp(log_step)[:, None]
    rotation = eigen_imag * step_size
    shrink = jnp.expm1(eigen_real * step_size)
    cosine = jnp.cos(rotation)
    sine_part = jnp.sin(rotation)
    decay_r = (1.0 + shrink) * cosine
    decay_i = (1.0 + shrink) * sine_part
    minus_r = shrink * cosine - 2.0 * jnp.square(jnp.sin(0.5 * rotation))
    modulus = jnp.square(eigen_real) + jnp.square(eigen_imag)
    factor_r = (minus_r * eigen_real + decay_i * eigen_imag) / modulus
    factor_i = (decay_i * eigen_real - minus_r * eigen_imag) / modulus
    drive_r = factor_r[..., None] * input_real - factor_i[..., None] * input_imag
    drive_i = factor_r[..., None] * input_imag + factor_i[..., None] * input_real
    return (decay_r, decay_i, drive_r, drive_i)


def split(value):
    high = value.astype(BF16)
    low = (value - high.astype(F32)).astype(BF16)
    return high, low


def cmul(ar, ai, br, bi):
    return ar * br - ai * bi, ar * bi + ai * br


def nt_dot(a, b):
    return lax.dot_general(a, b, (((1,), (1,)), ((), ())), preferred_element_type=F32)


def nn_dot(a, b):
    return jnp.dot(a, b, preferred_element_type=F32)


def lanes_low(shape):
    return lax.broadcasted_iota(jnp.int32, shape, len(shape) - 1) < HEAD_DIM


def reorder_matrix(rows, chunks, inverse):
    length = rows // chunks
    r = lax.broadcasted_iota(jnp.int32, (rows, rows), 1 if inverse else 0)
    t = lax.broadcasted_iota(jnp.int32, (rows, rows), 0 if inverse else 1)
    source = (r & (chunks - 1)) * length + (r >> 3)
    return jnp.where(t == source, 1.0, 0.0).astype(BF16)


def norm_kernel(tokens_ref, gain_ref, out_ref):
    wide = tokens_ref[...].astype(F32)
    mean = jnp.sum(wide * wide, axis=1, keepdims=True) * (1.0 / wide.shape[1])
    normed = (wide * lax.rsqrt(mean + EPSILON) * gain_ref[...]).astype(BF16)
    for k in range(out_ref.shape[0]):
        out_ref[k] = normed


def half_project_kernel(mine_ref, w_ref, found_ref):
    found_ref[...] = nn_dot(mine_ref[...], w_ref[...]).astype(BF16)


def merge_kernel(place_ref, parts_ref, mine_ref, other_ref, out_ref, total_ref):
    a = pl.program_id(0)
    core = place_ref[1]

    @pl.when(a == 0)
    def _():
        total_ref[...] = jnp.zeros_like(total_ref)

    total_ref[...] += nn_dot(parts_ref[2 * a + core], mine_ref[0]) + nn_dot(
        parts_ref[2 * a + 1 - core], other_ref[0]
    )

    @pl.when(a == pl.num_programs(0) - 1)
    def _():
        out_ref[...] = total_ref[...].astype(BF16)


def block_diagonal(parts, channels, width):
    row = lax.broadcasted_iota(jnp.int32, (channels, width), 0) >> 4
    lane = lax.broadcasted_iota(jnp.int32, (channels, width), 1) >> 6
    return split(jnp.concatenate([jnp.where(row == lane, p, 0.0) for p in parts], axis=1))


def drive_matrices(lines_ref, channels):
    width = lines_ref.shape[1]
    parts = [lines_ref[j * GROUP : (j + 1) * GROUP, :] for j in range(2)]
    parts = [jnp.concatenate([p] * (channels // GROUP), axis=0) for p in parts]
    return block_diagonal(parts, channels, width)


def read_matrices(reads_ref, width):
    channels = reads_ref.shape[0] // 2
    parts = [reads_ref[j * channels : (j + 1) * channels, :] for j in range(2)]
    parts = [jnp.concatenate([p] * (width // 128), axis=1) for p in (parts[0], -parts[1])]
    return block_diagonal(parts, channels, width)


def prepare_kernel(decay_ref, tab_ref, chunk_ref, wide_ref, later_ref, *, blocks, chunk):
    rows = later_ref.shape
    below = lax.broadcasted_iota(jnp.int32, rows, 0) > lax.broadcasted_iota(jnp.int32, rows, 1)
    later_ref[...] = jnp.where(below, 1.0, 0.0).astype(BF16)
    dr, di = decay_ref[0:1, :], decay_ref[1:2, :]
    width = dr.shape[1]
    half = width // 2
    squares = [(dr, di)]
    for _ in range(9):
        a, b = squares[-1]
        squares.append(cmul(a, b, a, b))

    def power(n):
        out = None
        for k in range(10):
            if n >> k & 1:
                out = squares[k] if out is None else cmul(*out, *squares[k])
        return out

    p_chunk = power(chunk)
    p_block = power(chunk * 8)
    now = (jnp.ones_like(dr), jnp.zeros_like(dr))
    for k in range(blocks):
        for j, part in enumerate(now):
            tab_ref[4 * k + 2 * j : 4 * k + 2 * j + 1, :] = part[:, :half]
            tab_ref[4 * k + 2 * j + 1 : 4 * k + 2 * j + 2, :] = part[:, half:]
        now = cmul(*now, *p_block)
    now = (dr, di)
    for c in range(8):
        chunk_ref[c : c + 1, :width] = now[0]
        chunk_ref[c : c + 1, width:] = now[1]
        now = cmul(*now, *p_chunk)
    p2 = cmul(*p_chunk, *p_chunk)
    p4 = cmul(*p2, *p2)
    for k, (a, b) in enumerate([(dr, di), p_chunk, p2, p4]):
        wide_ref[k : k + 1, :width] = a
        wide_ref[k : k + 1, width:] = b
    wide_ref[4:8, :] = jnp.zeros((4, 2 * width), F32)


def make_push(u_perm, b_hi, b_lo, push_ref):
    push_ref[...] = nn_dot(u_perm, b_hi) + nn_dot(u_perm, b_lo)


def project_kernel(
    place_ref, found_ref, other_ref, w_ref, qg_ref, kg_ref, bias_ref, lines_ref, wide_ref,
    q_ref, payload_ref, u_ref, init_ref, rows_ref, push_ref,
):
    rows = payload_ref.shape[0] - 16
    piece = rows // 8
    core = place_ref[1]
    found_other = nn_dot(other_ref[...], w_ref[...]).astype(BF16)
    for found, where in ((found_ref[...], core), (found_other, 1 - core)):
        for a in range(4):
            at = pl.multiple_of((2 * a + where) * piece, 16)
            rows_ref[pl.ds(at, piece), :] = found[a * piece : (a + 1) * piece, :]
    low = lanes_low((rows, 2 * HEAD_DIM))

    def normed(raw, gain):
        wide = raw.astype(F32)
        square = wide * wide
        first = jnp.sum(jnp.where(low, square, 0.0), axis=1, keepdims=True)
        second = jnp.sum(jnp.where(low, 0.0, square), axis=1, keepdims=True)
        scale = jnp.where(
            low,
            lax.rsqrt(first * (1.0 / HEAD_DIM) + EPSILON),
            lax.rsqrt(second * (1.0 / HEAD_DIM) + EPSILON),
        )
        return (wide * scale * gain).astype(BF16)

    u = rows_ref[:, 0:128]
    u_perm = nn_dot(reorder_matrix(rows, 8, False), u).astype(BF16)
    u_ref[...] = u_perm
    make_push(u_perm, *drive_matrices(lines_ref, u_perm.shape[1]), push_ref)
    queries = normed(rows_ref[:, 128:256], qg_ref[...]).astype(F32) * HEAD_DIM ** (-0.5)
    q_ref[0] = jnp.where(low, queries, 0.0).astype(BF16)
    q_ref[1] = jnp.where(low, 0.0, queries).astype(BF16)
    payload_ref[0:rows, 0:128] = normed(rows_ref[:, 256:384], kg_ref[...])
    payload_ref[0:rows, 128:256] = rows_ref[:, 384:512]
    width = push_ref.shape[1] // 2
    lr = jnp.broadcast_to(wide_ref[0:1, :width], (8, width))
    li = jnp.broadcast_to(wide_ref[0:1, width:], (8, width))

    def step(k, carried):
        sr, si = carried
        at = pl.multiple_of(k * 8, 8)
        nr = lr * sr - li * si + push_ref[pl.ds(at, 8), :width]
        ni = lr * si + li * sr + push_ref[pl.ds(at, 8), width:]
        return nr, ni

    zero = jnp.zeros((8, width), F32)
    er, ei = lax.fori_loop(0, piece, step, (zero, zero), unroll=8)
    place = lax.broadcasted_iota(jnp.int32, (8, width), 0)
    for k in range(3):
        shift = 1 << k
        pr, pi = wide_ref[k + 1 : k + 2, :width], wide_ref[k + 1 : k + 2, width:]
        br = jnp.where(place >= shift, pltpu.roll(er, shift, 0), 0.0)
        bi = jnp.where(place >= shift, pltpu.roll(ei, shift, 0), 0.0)
        er, ei = er + pr * br - pi * bi, ei + pr * bi + pi * br
    init_ref[:, :width] = jnp.where(place >= 1, pltpu.roll(er, 1, 0), 0.0)
    init_ref[:, width:] = jnp.where(place >= 1, pltpu.roll(ei, 1, 0), 0.0)
    half = width // 2
    end = [er[7:8, :half], er[7:8, half:], ei[7:8, :half], ei[7:8, half:]]
    highs = [e.astype(BF16).astype(F32) for e in end]
    lows = [e - h for e, h in zip(end, highs)]
    tail = jnp.concatenate([bias_ref[...].astype(F32)] + highs + lows, axis=0)
    payload_ref[rows : rows + 16, :] = tail.astype(BF16)


def read_states(states_ref, ct_hi, ct_lo):
    high, low = split(states_ref[...])
    return nt_dot(high, ct_hi) + nt_dot(low, ct_hi) + nt_dot(high, ct_lo)


def local_state_kernel(
    u_ref, init_ref, lines_ref, wide_ref, reads_ref, skip_ref, y_ref, push_ref
):
    make_push(u_ref[...], *drive_matrices(lines_ref, u_ref.shape[1]), push_ref)
    width = push_ref.shape[1] // 2
    lr = jnp.broadcast_to(wide_ref[0:1, :width], (8, width))
    li = jnp.broadcast_to(wide_ref[0:1, width:], (8, width))

    def step(k, carried):
        sr, si = carried
        at = pl.multiple_of(k * 8, 8)
        nr = lr * sr - li * si + push_ref[pl.ds(at, 8), :width]
        ni = lr * si + li * sr + push_ref[pl.ds(at, 8), width:]
        push_ref[pl.ds(at, 8), :width] = nr
        push_ref[pl.ds(at, 8), width:] = ni
        return nr, ni

    lax.fori_loop(
        0, push_ref.shape[0] // 8, step, (init_ref[:, :width], init_ref[:, width:]), unroll=8
    )
    y_ref[...] = (
        read_states(push_ref, *read_matrices(reads_ref, width))
        + skip_ref[...] * u_ref[...].astype(F32)
    )


def score_block(q_ref, payload_ref, later_ref, diagonal):
    rows = q_ref.shape[1]
    keys, values = payload_ref[0:rows, 0:128], payload_ref[0:rows, 128:256]
    tail = payload_ref[rows : rows + 16, :].astype(F32)
    biases = (
        jnp.concatenate([tail[0:1, :], tail[1:2, 0:128]], axis=1),
        jnp.concatenate([tail[1:2, 128:256], tail[2:3, :]], axis=1),
    )
    outs, totals = [], []
    for h in range(2):
        z = nt_dot(q_ref[h], keys) + biases[h]
        loss = jnp.log(1.0 + jnp.exp(z))
        if diagonal:
            causal = lax.broadcasted_iota(jnp.int32, z.shape, 1) < lax.broadcasted_iota(
                jnp.int32, z.shape, 0
            )
            masked = jnp.where(causal, loss, 0.0)
        else:
            masked = loss
        later = nn_dot(masked.astype(BF16), later_ref[...])
        weights = jnp.exp((z - loss) - later)
        if diagonal:
            weights = jnp.where(causal, weights, 0.0)
        outs.append(nn_dot(weights.astype(BF16), values))
        totals.append(later[:, 0:1] + masked[:, 0:1])
    low = lanes_low((rows, 128))
    return jnp.where(low, outs[0], outs[1]), jnp.where(low, totals[0], totals[1])


def first_kernel(q_ref, payload_ref, later_ref, *refs):
    *state_refs, acc_ref, tot_ref, y_ref, states_ref = refs
    local_state_kernel(*state_refs, y_ref, states_ref)
    out, total = score_block(q_ref, payload_ref, later_ref, True)
    acc_ref[...] = out
    tot_ref[...] = total


def entering_state(payload_ref, tab_ref, carry_ref, power):
    rows = payload_ref.shape[0] - 16
    tail = payload_ref[rows : rows + 16, :].astype(F32)
    er, ei = tail[8:10] + tail[12:14], tail[10:12] + tail[14:16]
    wr, wi = tab_ref[4 * power : 4 * power + 2, :], tab_ref[4 * power + 2 : 4 * power + 4, :]
    carry_ref[0:2, :] += wr * er - wi * ei
    carry_ref[2:4, :] += wr * ei + wi * er


def step_kernel(
    place_ref, q_ref, later_ref, tab_ref, up_ref, down_ref,
    acc_in, tot_in, wrap_in, carry_in, acc_ref, tot_ref, wrap_ref, carry_ref, *, step, blocks, ups,
):
    here = place_ref[0]
    acc_ref[...] = acc_in[...]
    tot_ref[...] = tot_in[...]
    wrap_ref[...] = wrap_in[...]
    carry_ref[...] = carry_in[...]
    if step <= ups:

        @pl.when(here >= step)
        def _():
            out, total = score_block(q_ref, up_ref, later_ref, False)
            acc_ref[...] += out * jnp.exp(-tot_ref[...])
            tot_ref[...] += total
            entering_state(up_ref, tab_ref, carry_ref, step - 1)

    if step < blocks - ups:

        @pl.when(here >= blocks - step)
        def _():
            out, total = score_block(q_ref, down_ref, later_ref, False)
            wrap_ref[...] = wrap_ref[...] * jnp.exp(-total) + out
            entering_state(down_ref, tab_ref, carry_ref, blocks - 1 - step)


def last_kernel(*refs, **sizes):
    ins, (rest, out_ref, acc_ref, tot_ref, wrap_ref, carry_ref, states_ref) = (
        refs[:10],
        (refs[10:14], *refs[14:]),
    )
    step_kernel(*ins, acc_ref, tot_ref, wrap_ref, carry_ref, **sizes)
    finish_kernel(acc_ref, tot_ref, wrap_ref, carry_ref, *rest, out_ref, states_ref)


def finish_kernel(
    acc_ref, tot_ref, wrap_ref, carry_ref, y_ref, chunk_ref, wide_ref, reads_ref,
    out_ref, states_ref,
):
    rows = acc_ref.shape[0]
    width = states_ref.shape[1] // 2
    sr = jnp.concatenate([carry_ref[0:1, :], carry_ref[1:2, :]], axis=1)
    si = jnp.concatenate([carry_ref[2:3, :], carry_ref[3:4, :]], axis=1)
    zr, zi = cmul(chunk_ref[:, :width], chunk_ref[:, width:], sr, si)
    lr = jnp.broadcast_to(wide_ref[0:1, :width], (8, width))
    li = jnp.broadcast_to(wide_ref[0:1, width:], (8, width))

    def step(k, carried):
        zr, zi = carried
        at = pl.multiple_of(k * 8, 8)
        states_ref[pl.ds(at, 8), :width] = zr
        states_ref[pl.ds(at, 8), width:] = zi
        return cmul(lr, li, zr, zi)

    lax.fori_loop(0, rows // 8, step, (zr, zi), unroll=8)
    mixed = y_ref[...] + read_states(states_ref, *read_matrices(reads_ref, width))
    state_out = jax.nn.gelu(mixed).astype(BF16)
    state_out = nn_dot(reorder_matrix(rows, 8, True), state_out).astype(BF16)
    attended = acc_ref[...] + wrap_ref[...] * jnp.exp(-tot_ref[...])
    low = lanes_low(attended.shape)
    square = attended * attended
    first = jnp.sum(jnp.where(low, square, 0.0), axis=1, keepdims=True)
    second = jnp.sum(jnp.where(low, 0.0, square), axis=1, keepdims=True)
    scale = jnp.where(
        low,
        lax.rsqrt(first * (1.0 / HEAD_DIM) + EPSILON),
        lax.rsqrt(second * (1.0 / HEAD_DIM) + EPSILON),
    )
    attn_out = (attended * scale).astype(BF16)
    out_ref[:, 0:128] = state_out
    out_ref[:, 128:256] = attn_out


def call(kernel, outs, args, scratch=(), smem=0, flops=1, aliases={}, limit=16):
    return pl.pallas_call(
        kernel,
        out_shape=outs,
        in_specs=[SMEM] * smem + [VMEM] * (len(args) - smem),
        out_specs=jax.tree.map(lambda _: VMEM, outs),
        scratch_shapes=list(scratch),
        input_output_aliases=aliases,
        compiler_params=pltpu.CompilerParams(vmem_limit_bytes=limit * 2**20),
        cost_estimate=pl.CostEstimate(flops=flops, bytes_accessed=10**6, transcendentals=0),
    )(*args)


def shape(dims, dtype=F32):
    return jax.ShapeDtypeStruct(dims, dtype)


def on_device(
    tokens,
    norm_gain,
    w_input,
    w_query,
    w_key,
    w_value,
    query_gain,
    key_gain,
    key_bias,
    eigen_real,
    eigen_imag,
    log_step,
    input_real,
    input_imag,
    read_real,
    read_imag,
    skip_gain,
    w_out_state,
    w_out_attn,
):
    blocks = lax.axis_size("sp")
    rows = key_bias.shape[0]
    piece = rows // 8
    groups = eigen_real.shape[0]
    width = groups * STATE
    channels = groups * GROUP
    place = jnp.stack([lax.axis_index("sp"), lax.axis_index("tp_1")]).astype(jnp.int32)

    copies = call(
        norm_kernel,
        shape((4, *tokens.shape), BF16),
        (tokens, norm_gain.reshape(1, -1)),
        limit=60,
    )
    mine = lax.all_to_all(copies, "tp_0", 0, 0, tiled=True).reshape(4 * piece, -1)

    w_joined = jnp.concatenate([w_input, w_query, w_key, w_value], axis=1)
    w_out = jnp.concatenate([w_out_state, w_out_attn], axis=0)
    w_out_copies = jnp.broadcast_to(w_out[None], (4, *w_out.shape))
    decay_r, decay_i, drive_r, drive_i = discretize(
        eigen_real, eigen_imag, log_step, input_real, input_imag
    )
    lines = jnp.concatenate(
        [jnp.transpose(part, (2, 0, 1)).reshape(GROUP, width) for part in (drive_r, drive_i)]
    )
    reads = [part.reshape(channels, STATE) for part in (read_real, read_imag)]
    reads = jnp.concatenate([jnp.concatenate([part, part], axis=1) for part in reads])
    decay = jnp.stack([decay_r.reshape(-1), decay_i.reshape(-1)])
    bias8 = jnp.pad(jnp.transpose(key_bias).reshape(-1, 256), ((0, 5), (0, 0)))
    gains = [jnp.tile(g, 2).reshape(1, 128) for g in (query_gain, key_gain)]
    skip = skip_gain.reshape(1, -1)
    decay, lines, reads, w_joined, w_out_copies, bias8, gains, skip, place = (
        lax.optimization_barrier(
            (decay, lines, reads, w_joined, w_out_copies, bias8, gains, skip, place)
        )
    )
    tables = call(
        lambda *refs: prepare_kernel(*refs, blocks=blocks, chunk=piece),
        (
            shape((4 * blocks, width // 2)),
            shape((8, 2 * width)),
            shape((8, 2 * width)),
            shape((rows, rows), BF16),
        ),
        (decay,),
    )
    mine, tables = lax.optimization_barrier((mine, tables))
    tab, chunk, wide, later = tables
    other = lax.ppermute(mine, "tp_1", [(0, 1), (1, 0)])

    found = call(
        half_project_kernel, shape((4 * piece, 512), BF16), (mine, w_joined), flops=10**9
    )
    q, payload, u_perm, init = call(
        project_kernel,
        (
            shape((2, rows, 128), BF16),
            shape((rows + 16, 256), BF16),
            shape((rows, channels), BF16),
            shape((8, 2 * width)),
        ),
        (place, found, other, w_joined, *gains, bias8, lines, wide),
        scratch=(pltpu.VMEM((rows, 512), BF16), pltpu.VMEM((rows, 2 * width), F32)),
        smem=1,
        flops=4 * 10**9,
    )

    acc, tot, y_local = call(
        first_kernel,
        (shape((rows, 128)), shape((rows, 128)), shape((rows, channels))),
        (q, payload, later, u_perm, init, lines, wide, reads, skip),
        scratch=(pltpu.VMEM((rows, 2 * width), F32),),
        flops=4 * 10**9,
    )
    acc, w_out_copies = lax.optimization_barrier((acc, w_out_copies))
    w_out_mine = lax.all_to_all(w_out_copies, "tp_0", 0, 0, tiled=True)
    wrap = jnp.zeros((rows, 128), F32)
    carry = jnp.zeros((8, width // 2), F32)
    up = down = payload
    half = blocks // 2
    for step in range(1, half + 1):
        up = lax.ppermute(up, "sp", [(i - 1, i) for i in range(step, blocks)])
        if step < half:
            hops = [((j - step + 1) % blocks, (j - step) % blocks) for j in range(half - 1)]
            down = lax.ppermute(down, "sp", hops)
        if step == half:
            break
        acc, tot, wrap, carry = call(
            lambda *refs, step=step: step_kernel(*refs, step=step, blocks=blocks, ups=half),
            (shape((rows, 128)), shape((rows, 128)), shape((rows, 128)), shape(carry.shape)),
            (place, q, later, tab, up, down, acc, tot, wrap, carry),
            smem=1,
            flops=3 * 10**9,
            aliases={6: 0, 7: 1, 8: 2, 9: 3},
        )
        if step == half - 2:
            acc, w_out_mine = lax.optimization_barrier((acc, w_out_mine))
            w_out_other = lax.ppermute(w_out_mine, "tp_1", [(0, 1), (1, 0)])
    state = [shape((rows, 128)), shape((rows, 128)), shape((rows, 128)), shape(carry.shape)]
    both = call(
        lambda *refs: last_kernel(*refs, step=half, blocks=blocks, ups=half),
        shape((rows, 2 * channels), BF16),
        (place, q, later, tab, up, down, acc, tot, wrap, carry, y_local, chunk, wide, reads),
        scratch=[pltpu.VMEM(s.shape, F32) for s in state]
        + [pltpu.VMEM((rows, 2 * width), F32)],
        smem=1,
        flops=3 * 10**9,
    )
    parts = lax.all_to_all(both.reshape(8, piece, -1), TP, 0, 0, tiled=True)
    columns = w_out.shape[1]
    return pl.pallas_call(
        merge_kernel,
        out_shape=shape((piece, columns), BF16),
        grid=(4,),
        in_specs=[
            SMEM,
            VMEM,
            pl.BlockSpec((1, w_out.shape[0], columns), lambda a: (a, 0, 0)),
            pl.BlockSpec((1, w_out.shape[0], columns), lambda a: (a, 0, 0)),
        ],
        out_specs=pl.BlockSpec((piece, columns), lambda a: (0, 0)),
        scratch_shapes=[pltpu.VMEM((piece, columns), F32)],
        compiler_params=pltpu.CompilerParams(vmem_limit_bytes=16 * 2**20),
        cost_estimate=pl.CostEstimate(flops=10**9, bytes_accessed=10**7, transcendentals=0),
    )(place, parts, w_out_mine, w_out_other)


def solution(mesh):
    torus = Mesh(
        mesh.devices.reshape(mesh.shape["sp"], mesh.shape["fs"], 4, 2), ("sp", "fs", "tp_0", "tp_1")
    )
    placed = (
        P(FS_SP_TP, None),
        P(),
        P(None, TP),
        P(None, TP),
        P(None, TP),
        P(None, TP),
        P(),
        P(),
        P(("fs", "sp"), TP),
        P(TP, None),
        P(TP, None),
        P(TP),
        P(TP, None, None),
        P(TP, None, None),
        P(TP, None, None),
        P(TP, None, None),
        P(TP),
        P(TP, None),
        P(TP, None),
    )

    return jax.shard_map(
        on_device, mesh=torus, in_specs=placed, out_specs=P(FS_SP_TP, None), check_vma=False
    )
```

```python
import jax
import jax.numpy as jnp
from jax import lax
from jax.experimental import pallas as pl
from jax.experimental.pallas import tpu as pltpu
from jax.sharding import Mesh
from jax.sharding import PartitionSpec as P


GROUP = 16
STATE = 64
HEAD_DIM = 64
TP = ("tp_0", "tp_1")
FS_SP_TP = ("fs", "sp", "tp_0", "tp_1")
EPSILON = 1e-06
F32 = jnp.float32
BF16 = jnp.bfloat16


PIECES = (4, 3, 5, 2)

VMEM = pl.BlockSpec(memory_space=pltpu.VMEM)
SMEM = pl.BlockSpec(memory_space=pltpu.SMEM)


def discretize(eigen_real, eigen_imag, log_step, input_real, input_imag):
    step_size = jnp.exp(log_step)[:, None]
    rotation = eigen_imag * step_size
    shrink = jnp.expm1(eigen_real * step_size)
    cosine = jnp.cos(rotation)
    sine_part = jnp.sin(rotation)
    decay_r = (1.0 + shrink) * cosine
    decay_i = (1.0 + shrink) * sine_part
    minus_r = shrink * cosine - 2.0 * jnp.square(jnp.sin(0.5 * rotation))
    modulus = jnp.square(eigen_real) + jnp.square(eigen_imag)
    factor_r = (minus_r * eigen_real + decay_i * eigen_imag) / modulus
    factor_i = (decay_i * eigen_real - minus_r * eigen_imag) / modulus
    drive_r = factor_r[..., None] * input_real - factor_i[..., None] * input_imag
    drive_i = factor_r[..., None] * input_imag + factor_i[..., None] * input_real
    return (decay_r, decay_i, drive_r, drive_i)


def split(value):
    high = value.astype(BF16)
    low = (value - high.astype(F32)).astype(BF16)
    return high, low


def cmul(ar, ai, br, bi):
    return ar * br - ai * bi, ar * bi + ai * br


def nt_dot(a, b):
    return lax.dot_general(a, b, (((1,), (1,)), ((), ())), preferred_element_type=F32)


def nn_dot(a, b):
    return jnp.dot(a, b, preferred_element_type=F32)


def lanes_low(shape):
    return lax.broadcasted_iota(jnp.int32, shape, len(shape) - 1) < HEAD_DIM


def reorder_matrix(rows, chunks, inverse):
    length = rows // chunks
    r = lax.broadcasted_iota(jnp.int32, (rows, rows), 1 if inverse else 0)
    t = lax.broadcasted_iota(jnp.int32, (rows, rows), 0 if inverse else 1)
    source = (r & (chunks - 1)) * length + (r >> 3)
    return jnp.where(t == source, 1.0, 0.0).astype(BF16)


def norm_kernel(tokens_ref, gain_ref, out_ref):
    wide = tokens_ref[...].astype(F32)
    mean = jnp.sum(wide * wide, axis=1, keepdims=True) * (1.0 / wide.shape[1])
    normed = (wide * lax.rsqrt(mean + EPSILON) * gain_ref[...]).astype(BF16)
    for k in range(out_ref.shape[0]):
        out_ref[k] = normed


def half_project_kernel(mine_ref, w_ref, found_ref):
    found_ref[...] = nn_dot(mine_ref[...], w_ref[...]).astype(BF16)


def merge_kernel(place_ref, parts_ref, *refs):
    *weights, out_ref, held_ref, sems = refs
    copies = [
        pltpu.make_async_copy(ref, held_ref.at[k], sems.at[k]) for k, ref in enumerate(weights)
    ]
    for copy in copies:
        copy.start()
    core, line = place_ref[1], place_ref[2]
    total = None
    for k, away in enumerate(PIECES):
        owner = (line + away) & 3
        for j, where in ((2 * k, core), (2 * k + 1, 1 - core)):
            copies[j].wait()
            term = nn_dot(parts_ref[2 * owner + where], held_ref[j])
            total = term if total is None else total + term
    out_ref[...] = total.astype(BF16)


def block_diagonal(parts, channels, width):
    row = lax.broadcasted_iota(jnp.int32, (channels, width), 0) >> 4
    lane = lax.broadcasted_iota(jnp.int32, (channels, width), 1) >> 6
    return split(jnp.concatenate([jnp.where(row == lane, p, 0.0) for p in parts], axis=1))


def drive_matrices(lines_ref, channels):
    width = lines_ref.shape[1]
    parts = [lines_ref[j * GROUP : (j + 1) * GROUP, :] for j in range(2)]
    parts = [jnp.concatenate([p] * (channels // GROUP), axis=0) for p in parts]
    return block_diagonal(parts, channels, width)


def read_matrices(reads_ref, width):
    channels = reads_ref.shape[0] // 2
    parts = [reads_ref[j * channels : (j + 1) * channels, :] for j in range(2)]
    parts = [jnp.concatenate([p] * (width // 128), axis=1) for p in (parts[0], -parts[1])]
    return block_diagonal(parts, channels, width)


def prepare_kernel(decay_ref, tab_ref, chunk_ref, wide_ref, later_ref, *, blocks, chunk):
    rows = later_ref.shape
    below = lax.broadcasted_iota(jnp.int32, rows, 0) > lax.broadcasted_iota(jnp.int32, rows, 1)
    later_ref[...] = jnp.where(below, 1.0, 0.0).astype(BF16)
    dr, di = decay_ref[0:1, :], decay_ref[1:2, :]
    width = dr.shape[1]
    half = width // 2
    squares = [(dr, di)]
    for _ in range(9):
        a, b = squares[-1]
        squares.append(cmul(a, b, a, b))

    def power(n):
        out = None
        for k in range(10):
            if n >> k & 1:
                out = squares[k] if out is None else cmul(*out, *squares[k])
        return out

    p_chunk = power(chunk)
    p_block = power(chunk * 8)
    now = (jnp.ones_like(dr), jnp.zeros_like(dr))
    for k in range(blocks):
        for j, part in enumerate(now):
            tab_ref[4 * k + 2 * j : 4 * k + 2 * j + 1, :] = part[:, :half]
            tab_ref[4 * k + 2 * j + 1 : 4 * k + 2 * j + 2, :] = part[:, half:]
        now = cmul(*now, *p_block)
    now = (dr, di)
    for c in range(8):
        chunk_ref[c : c + 1, :width] = now[0]
        chunk_ref[c : c + 1, width:] = now[1]
        now = cmul(*now, *p_chunk)
    p2 = cmul(*p_chunk, *p_chunk)
    p4 = cmul(*p2, *p2)
    for k, (a, b) in enumerate([(dr, di), p_chunk, p2, p4]):
        wide_ref[k : k + 1, :width] = a
        wide_ref[k : k + 1, width:] = b
    wide_ref[4:8, :] = jnp.zeros((4, 2 * width), F32)


def make_push(u_perm, b_hi, b_lo, push_ref):
    push_ref[...] = nn_dot(u_perm, b_hi) + nn_dot(u_perm, b_lo)


def project_kernel(
    place_ref, found_ref, other_ref, w_ref, qg_ref, kg_ref, bias_ref, lines_ref, wide_ref,
    q_ref, payload_ref, u_ref, init_ref, rows_ref, push_ref,
):
    rows = payload_ref.shape[0] - 16
    piece = rows // 8
    core = place_ref[1]
    found_other = nn_dot(other_ref[...], w_ref[...]).astype(BF16)
    for found, where in ((found_ref[...], core), (found_other, 1 - core)):
        for a in range(4):
            at = pl.multiple_of((2 * a + where) * piece, 16)
            rows_ref[pl.ds(at, piece), :] = found[a * piece : (a + 1) * piece, :]
    low = lanes_low((rows, 2 * HEAD_DIM))

    def normed(raw, gain):
        wide = raw.astype(F32)
        square = wide * wide
        first = jnp.sum(jnp.where(low, square, 0.0), axis=1, keepdims=True)
        second = jnp.sum(jnp.where(low, 0.0, square), axis=1, keepdims=True)
        scale = jnp.where(
            low,
            lax.rsqrt(first * (1.0 / HEAD_DIM) + EPSILON),
            lax.rsqrt(second * (1.0 / HEAD_DIM) + EPSILON),
        )
        return (wide * scale * gain).astype(BF16)

    u = rows_ref[:, 0:128]
    u_perm = nn_dot(reorder_matrix(rows, 8, False), u).astype(BF16)
    u_ref[...] = u_perm
    make_push(u_perm, *drive_matrices(lines_ref, u_perm.shape[1]), push_ref)
    queries = normed(rows_ref[:, 128:256], qg_ref[...]).astype(F32) * HEAD_DIM ** (-0.5)
    q_ref[0] = jnp.where(low, queries, 0.0).astype(BF16)
    q_ref[1] = jnp.where(low, 0.0, queries).astype(BF16)
    payload_ref[0:rows, 0:128] = normed(rows_ref[:, 256:384], kg_ref[...])
    payload_ref[0:rows, 128:256] = rows_ref[:, 384:512]
    width = push_ref.shape[1] // 2
    lr = jnp.broadcast_to(wide_ref[0:1, :width], (8, width))
    li = jnp.broadcast_to(wide_ref[0:1, width:], (8, width))

    def step(k, carried):
        sr, si = carried
        at = pl.multiple_of(k * 8, 8)
        nr = lr * sr - li * si + push_ref[pl.ds(at, 8), :width]
        ni = lr * si + li * sr + push_ref[pl.ds(at, 8), width:]
        return nr, ni

    zero = jnp.zeros((8, width), F32)
    er, ei = lax.fori_loop(0, piece, step, (zero, zero), unroll=8)
    place = lax.broadcasted_iota(jnp.int32, (8, width), 0)
    for k in range(3):
        shift = 1 << k
        pr, pi = wide_ref[k + 1 : k + 2, :width], wide_ref[k + 1 : k + 2, width:]
        br = jnp.where(place >= shift, pltpu.roll(er, shift, 0), 0.0)
        bi = jnp.where(place >= shift, pltpu.roll(ei, shift, 0), 0.0)
        er, ei = er + pr * br - pi * bi, ei + pr * bi + pi * br
    init_ref[:, :width] = jnp.where(place >= 1, pltpu.roll(er, 1, 0), 0.0)
    init_ref[:, width:] = jnp.where(place >= 1, pltpu.roll(ei, 1, 0), 0.0)
    half = width // 2
    end = [er[7:8, :half], er[7:8, half:], ei[7:8, :half], ei[7:8, half:]]
    highs = [e.astype(BF16).astype(F32) for e in end]
    lows = [e - h for e, h in zip(end, highs)]
    tail = jnp.concatenate([bias_ref[...].astype(F32)] + highs + lows, axis=0)
    payload_ref[rows : rows + 16, :] = tail.astype(BF16)


def read_states(states_ref, ct_hi, ct_lo):
    high, low = split(states_ref[...])
    return nt_dot(high, ct_hi) + nt_dot(low, ct_hi) + nt_dot(high, ct_lo)


def local_state_kernel(
    u_ref, init_ref, lines_ref, wide_ref, reads_ref, skip_ref, y_ref, push_ref
):
    make_push(u_ref[...], *drive_matrices(lines_ref, u_ref.shape[1]), push_ref)
    width = push_ref.shape[1] // 2
    lr = jnp.broadcast_to(wide_ref[0:1, :width], (8, width))
    li = jnp.broadcast_to(wide_ref[0:1, width:], (8, width))

    def step(k, carried):
        sr, si = carried
        at = pl.multiple_of(k * 8, 8)
        nr = lr * sr - li * si + push_ref[pl.ds(at, 8), :width]
        ni = lr * si + li * sr + push_ref[pl.ds(at, 8), width:]
        push_ref[pl.ds(at, 8), :width] = nr
        push_ref[pl.ds(at, 8), width:] = ni
        return nr, ni

    lax.fori_loop(
        0, push_ref.shape[0] // 8, step, (init_ref[:, :width], init_ref[:, width:]), unroll=8
    )
    y_ref[...] = (
        read_states(push_ref, *read_matrices(reads_ref, width))
        + skip_ref[...] * u_ref[...].astype(F32)
    )


def score_block(q_ref, payload_ref, later_ref, diagonal):
    rows = q_ref.shape[1]
    keys, values = payload_ref[0:rows, 0:128], payload_ref[0:rows, 128:256]
    tail = payload_ref[rows : rows + 16, :].astype(F32)
    biases = (
        jnp.concatenate([tail[0:1, :], tail[1:2, 0:128]], axis=1),
        jnp.concatenate([tail[1:2, 128:256], tail[2:3, :]], axis=1),
    )
    outs, totals = [], []
    for h in range(2):
        z = nt_dot(q_ref[h], keys) + biases[h]
        loss = jnp.log(1.0 + jnp.exp(z))
        if diagonal:
            causal = lax.broadcasted_iota(jnp.int32, z.shape, 1) < lax.broadcasted_iota(
                jnp.int32, z.shape, 0
            )
            masked = jnp.where(causal, loss, 0.0)
        else:
            masked = loss
        later = nn_dot(masked.astype(BF16), later_ref[...])
        weights = jnp.exp((z - loss) - later)
        if diagonal:
            weights = jnp.where(causal, weights, 0.0)
        outs.append(nn_dot(weights.astype(BF16), values))
        totals.append(later[:, 0:1] + masked[:, 0:1])
    low = lanes_low((rows, 128))
    return jnp.where(low, outs[0], outs[1]), jnp.where(low, totals[0], totals[1])


def first_kernel(q_ref, payload_ref, later_ref, *refs):
    *state_refs, acc_ref, tot_ref, y_ref, states_ref = refs
    local_state_kernel(*state_refs, y_ref, states_ref)
    out, total = score_block(q_ref, payload_ref, later_ref, True)
    acc_ref[...] = out
    tot_ref[...] = total


def entering_state(payload_ref, tab_ref, carry_ref, power):
    rows = payload_ref.shape[0] - 16
    tail = payload_ref[rows : rows + 16, :].astype(F32)
    er, ei = tail[8:10] + tail[12:14], tail[10:12] + tail[14:16]
    wr, wi = tab_ref[4 * power : 4 * power + 2, :], tab_ref[4 * power + 2 : 4 * power + 4, :]
    carry_ref[0:2, :] += wr * er - wi * ei
    carry_ref[2:4, :] += wr * ei + wi * er


def step_kernel(
    place_ref, q_ref, later_ref, tab_ref, up_ref, down_ref,
    acc_in, tot_in, wrap_in, carry_in, acc_ref, tot_ref, wrap_ref, carry_ref, *, step, blocks, ups,
):
    here = place_ref[0]
    acc_ref[...] = acc_in[...]
    tot_ref[...] = tot_in[...]
    wrap_ref[...] = wrap_in[...]
    carry_ref[...] = carry_in[...]
    if step <= ups:

        @pl.when(here >= step)
        def _():
            out, total = score_block(q_ref, up_ref, later_ref, False)
            acc_ref[...] += out * jnp.exp(-tot_ref[...])
            tot_ref[...] += total
            entering_state(up_ref, tab_ref, carry_ref, step - 1)

    if step < blocks - ups:

        @pl.when(here >= blocks - step)
        def _():
            out, total = score_block(q_ref, down_ref, later_ref, False)
            wrap_ref[...] = wrap_ref[...] * jnp.exp(-total) + out
            entering_state(down_ref, tab_ref, carry_ref, blocks - 1 - step)


def last_kernel(*refs, **sizes):
    ins, (rest, out_ref, acc_ref, tot_ref, wrap_ref, carry_ref, states_ref) = (
        refs[:10],
        (refs[10:14], *refs[14:]),
    )
    step_kernel(*ins, acc_ref, tot_ref, wrap_ref, carry_ref, **sizes)
    finish_kernel(acc_ref, tot_ref, wrap_ref, carry_ref, *rest, out_ref, states_ref)


def finish_kernel(
    acc_ref, tot_ref, wrap_ref, carry_ref, y_ref, chunk_ref, wide_ref, reads_ref,
    out_ref, states_ref,
):
    rows = acc_ref.shape[0]
    width = states_ref.shape[1] // 2
    sr = jnp.concatenate([carry_ref[0:1, :], carry_ref[1:2, :]], axis=1)
    si = jnp.concatenate([carry_ref[2:3, :], carry_ref[3:4, :]], axis=1)
    zr, zi = cmul(chunk_ref[:, :width], chunk_ref[:, width:], sr, si)
    lr = jnp.broadcast_to(wide_ref[0:1, :width], (8, width))
    li = jnp.broadcast_to(wide_ref[0:1, width:], (8, width))

    def step(k, carried):
        zr, zi = carried
        at = pl.multiple_of(k * 8, 8)
        states_ref[pl.ds(at, 8), :width] = zr
        states_ref[pl.ds(at, 8), width:] = zi
        return cmul(lr, li, zr, zi)

    lax.fori_loop(0, rows // 8, step, (zr, zi), unroll=8)
    mixed = y_ref[...] + read_states(states_ref, *read_matrices(reads_ref, width))
    state_out = jax.nn.gelu(mixed).astype(BF16)
    state_out = nn_dot(reorder_matrix(rows, 8, True), state_out).astype(BF16)
    attended = acc_ref[...] + wrap_ref[...] * jnp.exp(-tot_ref[...])
    low = lanes_low(attended.shape)
    square = attended * attended
    first = jnp.sum(jnp.where(low, square, 0.0), axis=1, keepdims=True)
    second = jnp.sum(jnp.where(low, 0.0, square), axis=1, keepdims=True)
    scale = jnp.where(
        low,
        lax.rsqrt(first * (1.0 / HEAD_DIM) + EPSILON),
        lax.rsqrt(second * (1.0 / HEAD_DIM) + EPSILON),
    )
    attn_out = (attended * scale).astype(BF16)
    out_ref[:, 0:128] = state_out
    out_ref[:, 128:256] = attn_out


def call(kernel, outs, args, scratch=(), smem=0, flops=1, aliases={}, limit=16):
    return pl.pallas_call(
        kernel,
        out_shape=outs,
        in_specs=[SMEM] * smem + [VMEM] * (len(args) - smem),
        out_specs=jax.tree.map(lambda _: VMEM, outs),
        scratch_shapes=list(scratch),
        input_output_aliases=aliases,
        compiler_params=pltpu.CompilerParams(vmem_limit_bytes=limit * 2**20),
        cost_estimate=pl.CostEstimate(flops=flops, bytes_accessed=10**6, transcendentals=0),
    )(*args)


def shape(dims, dtype=F32):
    return jax.ShapeDtypeStruct(dims, dtype)


def on_device(
    tokens,
    norm_gain,
    w_input,
    w_query,
    w_key,
    w_value,
    query_gain,
    key_gain,
    key_bias,
    eigen_real,
    eigen_imag,
    log_step,
    input_real,
    input_imag,
    read_real,
    read_imag,
    skip_gain,
    w_out_state,
    w_out_attn,
):
    blocks = lax.axis_size("sp")
    rows = key_bias.shape[0]
    piece = rows // 8
    groups = eigen_real.shape[0]
    width = groups * STATE
    channels = groups * GROUP
    place = jnp.stack([lax.axis_index("sp"), lax.axis_index("tp_1"), lax.axis_index("tp_0")]).astype(jnp.int32)

    copies = call(
        norm_kernel,
        shape((4, *tokens.shape), BF16),
        (tokens, norm_gain.reshape(1, -1)),
        limit=60,
    )
    mine = lax.all_to_all(copies, "tp_0", 0, 0, tiled=True).reshape(4 * piece, -1)

    w_joined = jnp.concatenate([w_input, w_query, w_key, w_value], axis=1)
    w_out = jnp.concatenate([w_out_state, w_out_attn], axis=0)
    decay_r, decay_i, drive_r, drive_i = discretize(
        eigen_real, eigen_imag, log_step, input_real, input_imag
    )
    lines = jnp.concatenate(
        [jnp.transpose(part, (2, 0, 1)).reshape(GROUP, width) for part in (drive_r, drive_i)]
    )
    reads = [part.reshape(channels, STATE) for part in (read_real, read_imag)]
    reads = jnp.concatenate([jnp.concatenate([part, part], axis=1) for part in reads])
    decay = jnp.stack([decay_r.reshape(-1), decay_i.reshape(-1)])
    bias8 = jnp.pad(jnp.transpose(key_bias).reshape(-1, 256), ((0, 5), (0, 0)))
    gains = [jnp.tile(g, 2).reshape(1, 128) for g in (query_gain, key_gain)]
    skip = skip_gain.reshape(1, -1)
    decay, lines, reads, w_joined, w_out, bias8, gains, skip, place = (
        lax.optimization_barrier(
            (decay, lines, reads, w_joined, w_out, bias8, gains, skip, place)
        )
    )
    tables = call(
        lambda *refs: prepare_kernel(*refs, blocks=blocks, chunk=piece),
        (
            shape((4 * blocks, width // 2)),
            shape((8, 2 * width)),
            shape((8, 2 * width)),
            shape((rows, rows), BF16),
        ),
        (decay,),
    )
    mine, tables = lax.optimization_barrier((mine, tables))
    tab, chunk, wide, later = tables
    other = lax.ppermute(mine, "tp_1", [(0, 1), (1, 0)])

    found = call(
        half_project_kernel, shape((4 * piece, 512), BF16), (mine, w_joined), flops=10**9
    )
    q, payload, u_perm, init = call(
        project_kernel,
        (
            shape((2, rows, 128), BF16),
            shape((rows + 16, 256), BF16),
            shape((rows, channels), BF16),
            shape((8, 2 * width)),
        ),
        (place, found, other, w_joined, *gains, bias8, lines, wide),
        scratch=(pltpu.VMEM((rows, 512), BF16), pltpu.VMEM((rows, 2 * width), F32)),
        smem=1,
        flops=4 * 10**9,
    )

    acc, tot, y_local = call(
        first_kernel,
        (shape((rows, 128)), shape((rows, 128)), shape((rows, channels))),
        (q, payload, later, u_perm, init, lines, wide, reads, skip),
        scratch=(pltpu.VMEM((rows, 2 * width), F32),),
        flops=4 * 10**9,
    )
    held = {"own": w_out}
    moves = (
        ("left", "own", "tp_0", 1),
        ("right", "own", "tp_0", 3),
        ("own_swap", "own", "tp_1", 1),
        ("far", "left", "tp_0", 1),
        ("left_swap", "left", "tp_1", 1),
        ("right_swap", "right", "tp_1", 1),
        ("far_swap", "far", "tp_1", 1),
    )

    def move_weights(slot, acc):
        name, source, axis, by = moves[slot]
        acc, held[source] = lax.optimization_barrier((acc, held[source]))
        size = lax.axis_size(axis)
        held[name] = lax.ppermute(held[source], axis, [(i, (i + by) % size) for i in range(size)])
        return acc

    acc = move_weights(0, acc)
    wrap = jnp.zeros((rows, 128), F32)
    carry = jnp.zeros((8, width // 2), F32)
    up = down = payload
    half = blocks // 2
    for step in range(1, half + 1):
        up = lax.ppermute(up, "sp", [(i - 1, i) for i in range(step, blocks)])
        if step < half:
            hops = [((j - step + 1) % blocks, (j - step) % blocks) for j in range(half - 1)]
            down = lax.ppermute(down, "sp", hops)
        if step == half:
            break
        acc, tot, wrap, carry = call(
            lambda *refs, step=step: step_kernel(*refs, step=step, blocks=blocks, ups=half),
            (shape((rows, 128)), shape((rows, 128)), shape((rows, 128)), shape(carry.shape)),
            (place, q, later, tab, up, down, acc, tot, wrap, carry),
            smem=1,
            flops=3 * 10**9,
            aliases={6: 0, 7: 1, 8: 2, 9: 3},
        )
        if step < len(moves):
            acc = move_weights(step, acc)
    state = [shape((rows, 128)), shape((rows, 128)), shape((rows, 128)), shape(carry.shape)]
    both = call(
        lambda *refs: last_kernel(*refs, step=half, blocks=blocks, ups=half),
        shape((rows, 2 * channels), BF16),
        (place, q, later, tab, up, down, acc, tot, wrap, carry, y_local, chunk, wide, reads),
        scratch=[pltpu.VMEM(s.shape, F32) for s in state]
        + [pltpu.VMEM((rows, 2 * width), F32)],
        smem=1,
        flops=3 * 10**9,
    )
    parts = lax.all_to_all(both.reshape(8, piece, -1), TP, 0, 0, tiled=True)
    pieces = [held[n + end] for n in ("own", "left", "right", "far") for end in ("", "_swap")]
    return pl.pallas_call(
        merge_kernel,
        out_shape=shape((piece, w_out.shape[1]), BF16),
        in_specs=[SMEM, VMEM] + [pl.BlockSpec(memory_space=pl.ANY)] * len(pieces),
        out_specs=VMEM,
        scratch_shapes=[
            pltpu.VMEM((len(pieces), *w_out.shape), BF16),
            pltpu.SemaphoreType.DMA((len(pieces),)),
        ],
        compiler_params=pltpu.CompilerParams(vmem_limit_bytes=24 * 2**20),
        cost_estimate=pl.CostEstimate(flops=10**9, bytes_accessed=10**7, transcendentals=0),
    )(place, parts, *pieces)


def solution(mesh):
    torus = Mesh(
        mesh.devices.reshape(mesh.shape["sp"], mesh.shape["fs"], 4, 2), ("sp", "fs", "tp_0", "tp_1")
    )
    placed = (
        P(FS_SP_TP, None),
        P(),
        P(None, TP),
        P(None, TP),
        P(None, TP),
        P(None, TP),
        P(),
        P(),
        P(("fs", "sp"), TP),
        P(TP, None),
        P(TP, None),
        P(TP),
        P(TP, None, None),
        P(TP, None, None),
        P(TP, None, None),
        P(TP, None, None),
        P(TP),
        P(TP, None),
        P(TP, None),
    )

    return jax.shard_map(
        on_device, mesh=torus, in_specs=placed, out_specs=P(FS_SP_TP, None), check_vma=False
    )
```

```python
import jax
import jax.numpy as jnp
from jax import lax
from jax.experimental import pallas as pl
from jax.experimental.pallas import tpu as pltpu
from jax.sharding import Mesh
from jax.sharding import PartitionSpec as P


GROUP = 16
STATE = 64
HEAD_DIM = 64
TP = ("tp_0", "tp_1")
FS_SP_TP = ("fs", "sp", "tp_0", "tp_1")
EPSILON = 1e-06
F32 = jnp.float32
BF16 = jnp.bfloat16


VMEM = pl.BlockSpec(memory_space=pltpu.VMEM)
SMEM = pl.BlockSpec(memory_space=pltpu.SMEM)


def discretize(eigen_real, eigen_imag, log_step, input_real, input_imag):
    step_size = jnp.exp(log_step)[:, None]
    rotation = eigen_imag * step_size
    shrink = jnp.expm1(eigen_real * step_size)
    cosine = jnp.cos(rotation)
    sine_part = jnp.sin(rotation)
    decay_r = (1.0 + shrink) * cosine
    decay_i = (1.0 + shrink) * sine_part
    minus_r = shrink * cosine - 2.0 * jnp.square(jnp.sin(0.5 * rotation))
    modulus = jnp.square(eigen_real) + jnp.square(eigen_imag)
    factor_r = (minus_r * eigen_real + decay_i * eigen_imag) / modulus
    factor_i = (decay_i * eigen_real - minus_r * eigen_imag) / modulus
    drive_r = factor_r[..., None] * input_real - factor_i[..., None] * input_imag
    drive_i = factor_r[..., None] * input_imag + factor_i[..., None] * input_real
    return (decay_r, decay_i, drive_r, drive_i)


def split(value):
    high = value.astype(BF16)
    low = (value - high.astype(F32)).astype(BF16)
    return high, low


def cmul(ar, ai, br, bi):
    return ar * br - ai * bi, ar * bi + ai * br


def nt_dot(a, b):
    return lax.dot_general(a, b, (((1,), (1,)), ((), ())), preferred_element_type=F32)


def nn_dot(a, b):
    return jnp.dot(a, b, preferred_element_type=F32)


def lanes_low(shape):
    return lax.broadcasted_iota(jnp.int32, shape, len(shape) - 1) < HEAD_DIM


def reorder_matrix(rows, chunks, inverse):
    length = rows // chunks
    r = lax.broadcasted_iota(jnp.int32, (rows, rows), 1 if inverse else 0)
    t = lax.broadcasted_iota(jnp.int32, (rows, rows), 0 if inverse else 1)
    source = (r & (chunks - 1)) * length + (r >> 3)
    return jnp.where(t == source, 1.0, 0.0).astype(BF16)


def norm_kernel(tokens_ref, gain_ref, out_ref):
    wide = tokens_ref[...].astype(F32)
    mean = jnp.sum(wide * wide, axis=1, keepdims=True) * (1.0 / wide.shape[1])
    normed = (wide * lax.rsqrt(mean + EPSILON) * gain_ref[...]).astype(BF16)
    for k in range(out_ref.shape[0]):
        out_ref[k] = normed


def half_project_kernel(mine_ref, w_ref, found_ref):
    found_ref[...] = nn_dot(mine_ref[...], w_ref[...]).astype(BF16)


def merge_kernel(place_ref, parts_ref, mine_ref, other_ref, out_ref, held_ref, sems):
    count = mine_ref.shape[0]
    copies = [
        pltpu.make_async_copy(mine_ref.at[a], held_ref.at[a], sems.at[a]) for a in range(count)
    ]
    for copy in copies:
        copy.start()
    core = place_ref[1]
    total = nn_dot(parts_ref[1 - core], other_ref[0])
    for a in range(1, count):
        total += nn_dot(parts_ref[2 * a + 1 - core], other_ref[a])
    for a in range(count):
        copies[a].wait()
        total += nn_dot(parts_ref[2 * a + core], held_ref[a])
    out_ref[...] = total.astype(BF16)


def block_diagonal(parts, channels, width):
    row = lax.broadcasted_iota(jnp.int32, (channels, width), 0) >> 4
    lane = lax.broadcasted_iota(jnp.int32, (channels, width), 1) >> 6
    return split(jnp.concatenate([jnp.where(row == lane, p, 0.0) for p in parts], axis=1))


def drive_matrices(lines_ref, channels):
    width = lines_ref.shape[1]
    parts = [lines_ref[j * GROUP : (j + 1) * GROUP, :] for j in range(2)]
    parts = [jnp.concatenate([p] * (channels // GROUP), axis=0) for p in parts]
    return block_diagonal(parts, channels, width)


def read_matrices(reads_ref, width):
    channels = reads_ref.shape[0] // 2
    parts = [reads_ref[j * channels : (j + 1) * channels, :] for j in range(2)]
    parts = [jnp.concatenate([p] * (width // 128), axis=1) for p in (parts[0], -parts[1])]
    return block_diagonal(parts, channels, width)


def prepare_kernel(decay_ref, tab_ref, chunk_ref, wide_ref, later_ref, *, blocks, chunk):
    rows = later_ref.shape
    below = lax.broadcasted_iota(jnp.int32, rows, 0) > lax.broadcasted_iota(jnp.int32, rows, 1)
    later_ref[...] = jnp.where(below, 1.0, 0.0).astype(BF16)
    dr, di = decay_ref[0:1, :], decay_ref[1:2, :]
    width = dr.shape[1]
    half = width // 2
    squares = [(dr, di)]
    for _ in range(9):
        a, b = squares[-1]
        squares.append(cmul(a, b, a, b))

    def power(n):
        out = None
        for k in range(10):
            if n >> k & 1:
                out = squares[k] if out is None else cmul(*out, *squares[k])
        return out

    p_chunk = power(chunk)
    p_block = power(chunk * 8)
    now = (jnp.ones_like(dr), jnp.zeros_like(dr))
    for k in range(blocks):
        for j, part in enumerate(now):
            tab_ref[4 * k + 2 * j : 4 * k + 2 * j + 1, :] = part[:, :half]
            tab_ref[4 * k + 2 * j + 1 : 4 * k + 2 * j + 2, :] = part[:, half:]
        now = cmul(*now, *p_block)
    now = (dr, di)
    for c in range(8):
        chunk_ref[c : c + 1, :width] = now[0]
        chunk_ref[c : c + 1, width:] = now[1]
        now = cmul(*now, *p_chunk)
    p2 = cmul(*p_chunk, *p_chunk)
    p4 = cmul(*p2, *p2)
    for k, (a, b) in enumerate([(dr, di), p_chunk, p2, p4]):
        wide_ref[k : k + 1, :width] = a
        wide_ref[k : k + 1, width:] = b
    wide_ref[4:8, :] = jnp.zeros((4, 2 * width), F32)


def make_push(u_perm, b_hi, b_lo, push_ref):
    push_ref[...] = nn_dot(u_perm, b_hi) + nn_dot(u_perm, b_lo)


def project_kernel(
    place_ref, found_ref, other_ref, w_ref, qg_ref, kg_ref, bias_ref, lines_ref, wide_ref,
    q_ref, payload_ref, u_ref, init_ref, rows_ref, push_ref,
):
    rows = payload_ref.shape[0] - 16
    piece = rows // 8
    core = place_ref[1]
    found_other = nn_dot(other_ref[...], w_ref[...]).astype(BF16)
    for found, where in ((found_ref[...], core), (found_other, 1 - core)):
        for a in range(4):
            at = pl.multiple_of((2 * a + where) * piece, 16)
            rows_ref[pl.ds(at, piece), :] = found[a * piece : (a + 1) * piece, :]
    low = lanes_low((rows, 2 * HEAD_DIM))

    def normed(raw, gain):
        wide = raw.astype(F32)
        square = wide * wide
        first = jnp.sum(jnp.where(low, square, 0.0), axis=1, keepdims=True)
        second = jnp.sum(jnp.where(low, 0.0, square), axis=1, keepdims=True)
        scale = jnp.where(
            low,
            lax.rsqrt(first * (1.0 / HEAD_DIM) + EPSILON),
            lax.rsqrt(second * (1.0 / HEAD_DIM) + EPSILON),
        )
        return (wide * scale * gain).astype(BF16)

    u = rows_ref[:, 0:128]
    u_perm = nn_dot(reorder_matrix(rows, 8, False), u).astype(BF16)
    u_ref[...] = u_perm
    make_push(u_perm, *drive_matrices(lines_ref, u_perm.shape[1]), push_ref)
    queries = normed(rows_ref[:, 128:256], qg_ref[...]).astype(F32) * HEAD_DIM ** (-0.5)
    q_ref[0] = jnp.where(low, queries, 0.0).astype(BF16)
    q_ref[1] = jnp.where(low, 0.0, queries).astype(BF16)
    payload_ref[0:rows, 0:128] = normed(rows_ref[:, 256:384], kg_ref[...])
    payload_ref[0:rows, 128:256] = rows_ref[:, 384:512]
    width = push_ref.shape[1] // 2
    lr = jnp.broadcast_to(wide_ref[0:1, :width], (8, width))
    li = jnp.broadcast_to(wide_ref[0:1, width:], (8, width))

    def step(k, carried):
        sr, si = carried
        at = pl.multiple_of(k * 8, 8)
        nr = lr * sr - li * si + push_ref[pl.ds(at, 8), :width]
        ni = lr * si + li * sr + push_ref[pl.ds(at, 8), width:]
        return nr, ni

    zero = jnp.zeros((8, width), F32)
    er, ei = lax.fori_loop(0, piece, step, (zero, zero), unroll=8)
    place = lax.broadcasted_iota(jnp.int32, (8, width), 0)
    for k in range(3):
        shift = 1 << k
        pr, pi = wide_ref[k + 1 : k + 2, :width], wide_ref[k + 1 : k + 2, width:]
        br = jnp.where(place >= shift, pltpu.roll(er, shift, 0), 0.0)
        bi = jnp.where(place >= shift, pltpu.roll(ei, shift, 0), 0.0)
        er, ei = er + pr * br - pi * bi, ei + pr * bi + pi * br
    init_ref[:, :width] = jnp.where(place >= 1, pltpu.roll(er, 1, 0), 0.0)
    init_ref[:, width:] = jnp.where(place >= 1, pltpu.roll(ei, 1, 0), 0.0)
    half = width // 2
    end = [er[7:8, :half], er[7:8, half:], ei[7:8, :half], ei[7:8, half:]]
    highs = [e.astype(BF16).astype(F32) for e in end]
    lows = [e - h for e, h in zip(end, highs)]
    tail = jnp.concatenate([bias_ref[...].astype(F32)] + highs + lows, axis=0)
    payload_ref[rows : rows + 16, :] = tail.astype(BF16)


def read_states(states_ref, ct_hi, ct_lo):
    high, low = split(states_ref[...])
    return nt_dot(high, ct_hi) + nt_dot(low, ct_hi) + nt_dot(high, ct_lo)


def local_state_kernel(
    u_ref, init_ref, lines_ref, wide_ref, reads_ref, skip_ref, y_ref, push_ref
):
    make_push(u_ref[...], *drive_matrices(lines_ref, u_ref.shape[1]), push_ref)
    width = push_ref.shape[1] // 2
    lr = jnp.broadcast_to(wide_ref[0:1, :width], (8, width))
    li = jnp.broadcast_to(wide_ref[0:1, width:], (8, width))

    def step(k, carried):
        sr, si = carried
        at = pl.multiple_of(k * 8, 8)
        nr = lr * sr - li * si + push_ref[pl.ds(at, 8), :width]
        ni = lr * si + li * sr + push_ref[pl.ds(at, 8), width:]
        push_ref[pl.ds(at, 8), :width] = nr
        push_ref[pl.ds(at, 8), width:] = ni
        return nr, ni

    lax.fori_loop(
        0, push_ref.shape[0] // 8, step, (init_ref[:, :width], init_ref[:, width:]), unroll=8
    )
    y_ref[...] = (
        read_states(push_ref, *read_matrices(reads_ref, width))
        + skip_ref[...] * u_ref[...].astype(F32)
    )


def score_block(q_ref, payload_ref, later_ref, diagonal):
    rows = q_ref.shape[1]
    keys, values = payload_ref[0:rows, 0:128], payload_ref[0:rows, 128:256]
    tail = payload_ref[rows : rows + 16, :].astype(F32)
    biases = (
        jnp.concatenate([tail[0:1, :], tail[1:2, 0:128]], axis=1),
        jnp.concatenate([tail[1:2, 128:256], tail[2:3, :]], axis=1),
    )
    outs, totals = [], []
    for h in range(2):
        z = nt_dot(q_ref[h], keys) + biases[h]
        loss = jnp.log(1.0 + jnp.exp(z))
        if diagonal:
            causal = lax.broadcasted_iota(jnp.int32, z.shape, 1) < lax.broadcasted_iota(
                jnp.int32, z.shape, 0
            )
            masked = jnp.where(causal, loss, 0.0)
        else:
            masked = loss
        later = nn_dot(masked.astype(BF16), later_ref[...])
        weights = jnp.exp((z - loss) - later)
        if diagonal:
            weights = jnp.where(causal, weights, 0.0)
        outs.append(nn_dot(weights.astype(BF16), values))
        totals.append(later[:, 0:1] + masked[:, 0:1])
    low = lanes_low((rows, 128))
    return jnp.where(low, outs[0], outs[1]), jnp.where(low, totals[0], totals[1])


def first_kernel(q_ref, payload_ref, later_ref, *refs):
    *state_refs, acc_ref, tot_ref, y_ref, states_ref = refs
    local_state_kernel(*state_refs, y_ref, states_ref)
    out, total = score_block(q_ref, payload_ref, later_ref, True)
    acc_ref[...] = out
    tot_ref[...] = total


def entering_state(payload_ref, tab_ref, carry_ref, power):
    rows = payload_ref.shape[0] - 16
    tail = payload_ref[rows : rows + 16, :].astype(F32)
    er, ei = tail[8:10] + tail[12:14], tail[10:12] + tail[14:16]
    wr, wi = tab_ref[4 * power : 4 * power + 2, :], tab_ref[4 * power + 2 : 4 * power + 4, :]
    carry_ref[0:2, :] += wr * er - wi * ei
    carry_ref[2:4, :] += wr * ei + wi * er


def step_kernel(
    place_ref, q_ref, later_ref, tab_ref, up_ref, down_ref,
    acc_in, tot_in, wrap_in, carry_in, acc_ref, tot_ref, wrap_ref, carry_ref, *, step, blocks, ups,
):
    here = place_ref[0]
    acc_ref[...] = acc_in[...]
    tot_ref[...] = tot_in[...]
    wrap_ref[...] = wrap_in[...]
    carry_ref[...] = carry_in[...]
    if step <= ups:

        @pl.when(here >= step)
        def _():
            out, total = score_block(q_ref, up_ref, later_ref, False)
            acc_ref[...] += out * jnp.exp(-tot_ref[...])
            tot_ref[...] += total
            entering_state(up_ref, tab_ref, carry_ref, step - 1)

    if step < blocks - ups:

        @pl.when(here >= blocks - step)
        def _():
            out, total = score_block(q_ref, down_ref, later_ref, False)
            wrap_ref[...] = wrap_ref[...] * jnp.exp(-total) + out
            entering_state(down_ref, tab_ref, carry_ref, blocks - 1 - step)


def last_kernel(*refs, **sizes):
    ins, (rest, out_ref, acc_ref, tot_ref, wrap_ref, carry_ref, states_ref) = (
        refs[:10],
        (refs[10:14], *refs[14:]),
    )
    step_kernel(*ins, acc_ref, tot_ref, wrap_ref, carry_ref, **sizes)
    finish_kernel(acc_ref, tot_ref, wrap_ref, carry_ref, *rest, out_ref, states_ref)


def finish_kernel(
    acc_ref, tot_ref, wrap_ref, carry_ref, y_ref, chunk_ref, wide_ref, reads_ref,
    out_ref, states_ref,
):
    rows = acc_ref.shape[0]
    width = states_ref.shape[1] // 2
    sr = jnp.concatenate([carry_ref[0:1, :], carry_ref[1:2, :]], axis=1)
    si = jnp.concatenate([carry_ref[2:3, :], carry_ref[3:4, :]], axis=1)
    zr, zi = cmul(chunk_ref[:, :width], chunk_ref[:, width:], sr, si)
    lr = jnp.broadcast_to(wide_ref[0:1, :width], (8, width))
    li = jnp.broadcast_to(wide_ref[0:1, width:], (8, width))

    def step(k, carried):
        zr, zi = carried
        at = pl.multiple_of(k * 8, 8)
        states_ref[pl.ds(at, 8), :width] = zr
        states_ref[pl.ds(at, 8), width:] = zi
        return cmul(lr, li, zr, zi)

    lax.fori_loop(0, rows // 8, step, (zr, zi), unroll=8)
    mixed = y_ref[...] + read_states(states_ref, *read_matrices(reads_ref, width))
    state_out = jax.nn.gelu(mixed).astype(BF16)
    state_out = nn_dot(reorder_matrix(rows, 8, True), state_out).astype(BF16)
    attended = acc_ref[...] + wrap_ref[...] * jnp.exp(-tot_ref[...])
    low = lanes_low(attended.shape)
    square = attended * attended
    first = jnp.sum(jnp.where(low, square, 0.0), axis=1, keepdims=True)
    second = jnp.sum(jnp.where(low, 0.0, square), axis=1, keepdims=True)
    scale = jnp.where(
        low,
        lax.rsqrt(first * (1.0 / HEAD_DIM) + EPSILON),
        lax.rsqrt(second * (1.0 / HEAD_DIM) + EPSILON),
    )
    attn_out = (attended * scale).astype(BF16)
    out_ref[:, 0:128] = state_out
    out_ref[:, 128:256] = attn_out


def call(kernel, outs, args, scratch=(), smem=0, flops=1, aliases={}, limit=16):
    return pl.pallas_call(
        kernel,
        out_shape=outs,
        in_specs=[SMEM] * smem + [VMEM] * (len(args) - smem),
        out_specs=jax.tree.map(lambda _: VMEM, outs),
        scratch_shapes=list(scratch),
        input_output_aliases=aliases,
        compiler_params=pltpu.CompilerParams(vmem_limit_bytes=limit * 2**20),
        cost_estimate=pl.CostEstimate(flops=flops, bytes_accessed=10**6, transcendentals=0),
    )(*args)


def shape(dims, dtype=F32):
    return jax.ShapeDtypeStruct(dims, dtype)


def on_device(
    tokens,
    norm_gain,
    w_input,
    w_query,
    w_key,
    w_value,
    query_gain,
    key_gain,
    key_bias,
    eigen_real,
    eigen_imag,
    log_step,
    input_real,
    input_imag,
    read_real,
    read_imag,
    skip_gain,
    w_out_state,
    w_out_attn,
):
    blocks = lax.axis_size("sp")
    rows = key_bias.shape[0]
    piece = rows // 8
    groups = eigen_real.shape[0]
    width = groups * STATE
    channels = groups * GROUP
    place = jnp.stack([lax.axis_index("sp"), lax.axis_index("tp_1")]).astype(jnp.int32)

    copies = call(
        norm_kernel,
        shape((4, *tokens.shape), BF16),
        (tokens, norm_gain.reshape(1, -1)),
        limit=60,
    )
    mine = lax.all_to_all(copies, "tp_0", 0, 0, tiled=True).reshape(4 * piece, -1)

    w_joined = jnp.concatenate([w_input, w_query, w_key, w_value], axis=1)
    w_out = jnp.concatenate([w_out_state, w_out_attn], axis=0)
    w_out_copies = jnp.broadcast_to(w_out[None], (4, *w_out.shape))
    decay_r, decay_i, drive_r, drive_i = discretize(
        eigen_real, eigen_imag, log_step, input_real, input_imag
    )
    lines = jnp.concatenate(
        [jnp.transpose(part, (2, 0, 1)).reshape(GROUP, width) for part in (drive_r, drive_i)]
    )
    reads = [part.reshape(channels, STATE) for part in (read_real, read_imag)]
    reads = jnp.concatenate([jnp.concatenate([part, part], axis=1) for part in reads])
    decay = jnp.stack([decay_r.reshape(-1), decay_i.reshape(-1)])
    bias8 = jnp.pad(jnp.transpose(key_bias).reshape(-1, 256), ((0, 5), (0, 0)))
    gains = [jnp.tile(g, 2).reshape(1, 128) for g in (query_gain, key_gain)]
    skip = skip_gain.reshape(1, -1)
    decay, lines, reads, w_joined, w_out_copies, bias8, gains, skip, place = (
        lax.optimization_barrier(
            (decay, lines, reads, w_joined, w_out_copies, bias8, gains, skip, place)
        )
    )
    tables = call(
        lambda *refs: prepare_kernel(*refs, blocks=blocks, chunk=piece),
        (
            shape((4 * blocks, width // 2)),
            shape((8, 2 * width)),
            shape((8, 2 * width)),
            shape((rows, rows), BF16),
        ),
        (decay,),
    )
    mine, tables = lax.optimization_barrier((mine, tables))
    tab, chunk, wide, later = tables
    other = lax.ppermute(mine, "tp_1", [(0, 1), (1, 0)])

    found = call(
        half_project_kernel, shape((4 * piece, 512), BF16), (mine, w_joined), flops=10**9
    )
    q, payload, u_perm, init = call(
        project_kernel,
        (
            shape((2, rows, 128), BF16),
            shape((rows + 16, 256), BF16),
            shape((rows, channels), BF16),
            shape((8, 2 * width)),
        ),
        (place, found, other, w_joined, *gains, bias8, lines, wide),
        scratch=(pltpu.VMEM((rows, 512), BF16), pltpu.VMEM((rows, 2 * width), F32)),
        smem=1,
        flops=4 * 10**9,
    )

    u_perm, w_out_copies = lax.optimization_barrier((u_perm, w_out_copies))
    w_out_mine = lax.all_to_all(w_out_copies, "tp_0", 0, 0, tiled=True)
    acc, tot, y_local = call(
        first_kernel,
        (shape((rows, 128)), shape((rows, 128)), shape((rows, channels))),
        (q, payload, later, u_perm, init, lines, wide, reads, skip),
        scratch=(pltpu.VMEM((rows, 2 * width), F32),),
        flops=4 * 10**9,
    )
    wrap = jnp.zeros((rows, 128), F32)
    carry = jnp.zeros((8, width // 2), F32)
    up = down = payload
    half = blocks // 2
    for step in range(1, half + 1):
        up = lax.ppermute(up, "sp", [(i - 1, i) for i in range(step, blocks)])
        if step < half:
            hops = [((j - step + 1) % blocks, (j - step) % blocks) for j in range(half - 1)]
            down = lax.ppermute(down, "sp", hops)
        if step == half:
            break
        acc, tot, wrap, carry = call(
            lambda *refs, step=step: step_kernel(*refs, step=step, blocks=blocks, ups=half),
            (shape((rows, 128)), shape((rows, 128)), shape((rows, 128)), shape(carry.shape)),
            (place, q, later, tab, up, down, acc, tot, wrap, carry),
            smem=1,
            flops=3 * 10**9,
            aliases={6: 0, 7: 1, 8: 2, 9: 3},
        )
        if step == half - 2:
            acc, w_out_mine = lax.optimization_barrier((acc, w_out_mine))
            w_out_other = lax.ppermute(w_out_mine, "tp_1", [(0, 1), (1, 0)])
    state = [shape((rows, 128)), shape((rows, 128)), shape((rows, 128)), shape(carry.shape)]
    both = call(
        lambda *refs: last_kernel(*refs, step=half, blocks=blocks, ups=half),
        shape((rows, 2 * channels), BF16),
        (place, q, later, tab, up, down, acc, tot, wrap, carry, y_local, chunk, wide, reads),
        scratch=[pltpu.VMEM(s.shape, F32) for s in state]
        + [pltpu.VMEM((rows, 2 * width), F32)],
        smem=1,
        flops=3 * 10**9,
    )
    parts = lax.all_to_all(both.reshape(8, piece, -1), TP, 0, 0, tiled=True)
    return pl.pallas_call(
        merge_kernel,
        out_shape=shape((piece, w_out.shape[1]), BF16),
        in_specs=[SMEM, VMEM, pl.BlockSpec(memory_space=pl.ANY), VMEM],
        out_specs=VMEM,
        scratch_shapes=[
            pltpu.VMEM(w_out_mine.shape, BF16),
            pltpu.SemaphoreType.DMA((w_out_mine.shape[0],)),
        ],
        compiler_params=pltpu.CompilerParams(vmem_limit_bytes=16 * 2**20),
        cost_estimate=pl.CostEstimate(flops=10**9, bytes_accessed=10**7, transcendentals=0),
    )(place, parts, w_out_mine, w_out_other)


def solution(mesh):
    torus = Mesh(
        mesh.devices.reshape(mesh.shape["sp"], mesh.shape["fs"], 4, 2), ("sp", "fs", "tp_0", "tp_1")
    )
    placed = (
        P(FS_SP_TP, None),
        P(),
        P(None, TP),
        P(None, TP),
        P(None, TP),
        P(None, TP),
        P(),
        P(),
        P(("fs", "sp"), TP),
        P(TP, None),
        P(TP, None),
        P(TP),
        P(TP, None, None),
        P(TP, None, None),
        P(TP, None, None),
        P(TP, None, None),
        P(TP),
        P(TP, None),
        P(TP, None),
    )

    return jax.shard_map(
        on_device, mesh=torus, in_specs=placed, out_specs=P(FS_SP_TP, None), check_vma=False
    )
```

```python
import jax
import jax.numpy as jnp
from jax import lax
from jax.experimental import pallas as pl
from jax.experimental.pallas import tpu as pltpu
from jax.sharding import Mesh
from jax.sharding import PartitionSpec as P


GROUP = 16
STATE = 64
HEAD_DIM = 64
TP = ("tp_0", "tp_1")
FS_SP_TP = ("fs", "sp", "tp_0", "tp_1")
EPSILON = 1e-06
F32 = jnp.float32
BF16 = jnp.bfloat16


VMEM = pl.BlockSpec(memory_space=pltpu.VMEM)
SMEM = pl.BlockSpec(memory_space=pltpu.SMEM)


def discretize(eigen_real, eigen_imag, log_step, input_real, input_imag):
    step_size = jnp.exp(log_step)[:, None]
    rotation = eigen_imag * step_size
    shrink = jnp.expm1(eigen_real * step_size)
    cosine = jnp.cos(rotation)
    sine_part = jnp.sin(rotation)
    decay_r = (1.0 + shrink) * cosine
    decay_i = (1.0 + shrink) * sine_part
    minus_r = shrink * cosine - 2.0 * jnp.square(jnp.sin(0.5 * rotation))
    modulus = jnp.square(eigen_real) + jnp.square(eigen_imag)
    factor_r = (minus_r * eigen_real + decay_i * eigen_imag) / modulus
    factor_i = (decay_i * eigen_real - minus_r * eigen_imag) / modulus
    drive_r = factor_r[..., None] * input_real - factor_i[..., None] * input_imag
    drive_i = factor_r[..., None] * input_imag + factor_i[..., None] * input_real
    return (decay_r, decay_i, drive_r, drive_i)


def split(value):
    high = value.astype(BF16)
    low = (value - high.astype(F32)).astype(BF16)
    return high, low


def cmul(ar, ai, br, bi):
    return ar * br - ai * bi, ar * bi + ai * br


def nt_dot(a, b):
    return lax.dot_general(a, b, (((1,), (1,)), ((), ())), preferred_element_type=F32)


def nn_dot(a, b):
    return jnp.dot(a, b, preferred_element_type=F32)


def lanes_low(shape):
    return lax.broadcasted_iota(jnp.int32, shape, len(shape) - 1) < HEAD_DIM


def reorder_matrix(rows, chunks, inverse):
    length = rows // chunks
    r = lax.broadcasted_iota(jnp.int32, (rows, rows), 1 if inverse else 0)
    t = lax.broadcasted_iota(jnp.int32, (rows, rows), 0 if inverse else 1)
    source = (r & (chunks - 1)) * length + (r >> 3)
    return jnp.where(t == source, 1.0, 0.0).astype(BF16)


def norm_kernel(tokens_ref, gain_ref, out_ref):
    wide = tokens_ref[...].astype(F32)
    mean = jnp.sum(wide * wide, axis=1, keepdims=True) * (1.0 / wide.shape[1])
    normed = (wide * lax.rsqrt(mean + EPSILON) * gain_ref[...]).astype(BF16)
    for k in range(out_ref.shape[0]):
        out_ref[k] = normed


def half_project_kernel(mine_ref, w_ref, found_ref):
    found_ref[...] = nn_dot(mine_ref[...], w_ref[...]).astype(BF16)


def merge_kernel(place_ref, parts_ref, mine_ref, other_ref, out_ref, held_ref, sems):
    count = mine_ref.shape[0]
    copies = [
        pltpu.make_async_copy(mine_ref.at[a], held_ref.at[a], sems.at[a]) for a in range(count)
    ]
    for copy in copies:
        copy.start()
    core = place_ref[1]
    total = nn_dot(parts_ref[1 - core], other_ref[0])
    for a in range(1, count):
        total += nn_dot(parts_ref[2 * a + 1 - core], other_ref[a])
    for a in range(count):
        copies[a].wait()
        total += nn_dot(parts_ref[2 * a + core], held_ref[a])
    out_ref[...] = total.astype(BF16)


def block_diagonal(parts, channels, width):
    row = lax.broadcasted_iota(jnp.int32, (channels, width), 0) >> 4
    lane = lax.broadcasted_iota(jnp.int32, (channels, width), 1) >> 6
    return split(jnp.concatenate([jnp.where(row == lane, p, 0.0) for p in parts], axis=1))


def drive_matrices(lines_ref, channels):
    width = lines_ref.shape[1]
    parts = [lines_ref[j * GROUP : (j + 1) * GROUP, :] for j in range(2)]
    parts = [jnp.concatenate([p] * (channels // GROUP), axis=0) for p in parts]
    return block_diagonal(parts, channels, width)


def read_matrices(reads_ref, width):
    channels = reads_ref.shape[0] // 2
    parts = [reads_ref[j * channels : (j + 1) * channels, :] for j in range(2)]
    parts = [jnp.concatenate([p] * (width // 128), axis=1) for p in (parts[0], -parts[1])]
    return block_diagonal(parts, channels, width)


def prepare_kernel(decay_ref, tab_ref, chunk_ref, wide_ref, later_ref, *, blocks, chunk):
    rows = later_ref.shape
    below = lax.broadcasted_iota(jnp.int32, rows, 0) > lax.broadcasted_iota(jnp.int32, rows, 1)
    later_ref[...] = jnp.where(below, 1.0, 0.0).astype(BF16)
    dr, di = decay_ref[0:1, :], decay_ref[1:2, :]
    width = dr.shape[1]
    half = width // 2
    squares = [(dr, di)]
    for _ in range(9):
        a, b = squares[-1]
        squares.append(cmul(a, b, a, b))

    def power(n):
        out = None
        for k in range(10):
            if n >> k & 1:
                out = squares[k] if out is None else cmul(*out, *squares[k])
        return out

    p_chunk = power(chunk)
    p_block = power(chunk * 8)
    now = (jnp.ones_like(dr), jnp.zeros_like(dr))
    for k in range(blocks):
        for j, part in enumerate(now):
            tab_ref[4 * k + 2 * j : 4 * k + 2 * j + 1, :] = part[:, :half]
            tab_ref[4 * k + 2 * j + 1 : 4 * k + 2 * j + 2, :] = part[:, half:]
        now = cmul(*now, *p_block)
    now = (dr, di)
    for c in range(8):
        chunk_ref[c : c + 1, :width] = now[0]
        chunk_ref[c : c + 1, width:] = now[1]
        now = cmul(*now, *p_chunk)
    p2 = cmul(*p_chunk, *p_chunk)
    p4 = cmul(*p2, *p2)
    for k, (a, b) in enumerate([(dr, di), p_chunk, p2, p4]):
        wide_ref[k : k + 1, :width] = a
        wide_ref[k : k + 1, width:] = b
    wide_ref[4:8, :] = jnp.zeros((4, 2 * width), F32)


def make_push(u_perm, b_hi, b_lo, push_ref):
    push_ref[...] = nn_dot(u_perm, b_hi) + nn_dot(u_perm, b_lo)


def project_kernel(
    place_ref, found_ref, other_ref, w_ref, qg_ref, kg_ref, bias_ref, lines_ref, wide_ref,
    q_ref, payload_ref, u_ref, init_ref, rows_ref, push_ref,
):
    rows = payload_ref.shape[0] - 16
    piece = rows // 8
    core = place_ref[1]
    found_other = nn_dot(other_ref[...], w_ref[...]).astype(BF16)
    for found, where in ((found_ref[...], core), (found_other, 1 - core)):
        for a in range(4):
            at = pl.multiple_of((2 * a + where) * piece, 16)
            rows_ref[pl.ds(at, piece), :] = found[a * piece : (a + 1) * piece, :]
    low = lanes_low((rows, 2 * HEAD_DIM))

    def normed(raw, gain):
        wide = raw.astype(F32)
        square = wide * wide
        first = jnp.sum(jnp.where(low, square, 0.0), axis=1, keepdims=True)
        second = jnp.sum(jnp.where(low, 0.0, square), axis=1, keepdims=True)
        scale = jnp.where(
            low,
            lax.rsqrt(first * (1.0 / HEAD_DIM) + EPSILON),
            lax.rsqrt(second * (1.0 / HEAD_DIM) + EPSILON),
        )
        return (wide * scale * gain).astype(BF16)

    u = rows_ref[:, 0:128]
    u_perm = nn_dot(reorder_matrix(rows, 8, False), u).astype(BF16)
    u_ref[...] = u_perm
    make_push(u_perm, *drive_matrices(lines_ref, u_perm.shape[1]), push_ref)
    queries = normed(rows_ref[:, 128:256], qg_ref[...]).astype(F32) * HEAD_DIM ** (-0.5)
    q_ref[0] = jnp.where(low, queries, 0.0).astype(BF16)
    q_ref[1] = jnp.where(low, 0.0, queries).astype(BF16)
    payload_ref[0:rows, 0:128] = normed(rows_ref[:, 256:384], kg_ref[...])
    payload_ref[0:rows, 128:256] = rows_ref[:, 384:512]
    width = push_ref.shape[1] // 2
    lr = jnp.broadcast_to(wide_ref[0:1, :width], (8, width))
    li = jnp.broadcast_to(wide_ref[0:1, width:], (8, width))

    def step(k, carried):
        sr, si = carried
        at = pl.multiple_of(k * 8, 8)
        nr = lr * sr - li * si + push_ref[pl.ds(at, 8), :width]
        ni = lr * si + li * sr + push_ref[pl.ds(at, 8), width:]
        return nr, ni

    zero = jnp.zeros((8, width), F32)
    er, ei = lax.fori_loop(0, piece, step, (zero, zero), unroll=8)
    place = lax.broadcasted_iota(jnp.int32, (8, width), 0)
    for k in range(3):
        shift = 1 << k
        pr, pi = wide_ref[k + 1 : k + 2, :width], wide_ref[k + 1 : k + 2, width:]
        br = jnp.where(place >= shift, pltpu.roll(er, shift, 0), 0.0)
        bi = jnp.where(place >= shift, pltpu.roll(ei, shift, 0), 0.0)
        er, ei = er + pr * br - pi * bi, ei + pr * bi + pi * br
    init_ref[:, :width] = jnp.where(place >= 1, pltpu.roll(er, 1, 0), 0.0)
    init_ref[:, width:] = jnp.where(place >= 1, pltpu.roll(ei, 1, 0), 0.0)
    half = width // 2
    end = [er[7:8, :half], er[7:8, half:], ei[7:8, :half], ei[7:8, half:]]
    highs = [e.astype(BF16).astype(F32) for e in end]
    lows = [e - h for e, h in zip(end, highs)]
    tail = jnp.concatenate([bias_ref[...].astype(F32)] + highs + lows, axis=0)
    payload_ref[rows : rows + 16, :] = tail.astype(BF16)


def read_states(states_ref, ct_hi, ct_lo):
    high, low = split(states_ref[...])
    return nt_dot(high, ct_hi) + nt_dot(low, ct_hi) + nt_dot(high, ct_lo)


def local_state_kernel(
    u_ref, init_ref, lines_ref, wide_ref, reads_ref, skip_ref, y_ref, push_ref
):
    make_push(u_ref[...], *drive_matrices(lines_ref, u_ref.shape[1]), push_ref)
    width = push_ref.shape[1] // 2
    lr = jnp.broadcast_to(wide_ref[0:1, :width], (8, width))
    li = jnp.broadcast_to(wide_ref[0:1, width:], (8, width))

    def step(k, carried):
        sr, si = carried
        at = pl.multiple_of(k * 8, 8)
        nr = lr * sr - li * si + push_ref[pl.ds(at, 8), :width]
        ni = lr * si + li * sr + push_ref[pl.ds(at, 8), width:]
        push_ref[pl.ds(at, 8), :width] = nr
        push_ref[pl.ds(at, 8), width:] = ni
        return nr, ni

    lax.fori_loop(
        0, push_ref.shape[0] // 8, step, (init_ref[:, :width], init_ref[:, width:]), unroll=8
    )
    y_ref[...] = (
        read_states(push_ref, *read_matrices(reads_ref, width))
        + skip_ref[...] * u_ref[...].astype(F32)
    )


def score_block(q_ref, payload_ref, later_ref, diagonal):
    rows = q_ref.shape[1]
    keys, values = payload_ref[0:rows, 0:128], payload_ref[0:rows, 128:256]
    tail = payload_ref[rows : rows + 16, :].astype(F32)
    biases = (
        jnp.concatenate([tail[0:1, :], tail[1:2, 0:128]], axis=1),
        jnp.concatenate([tail[1:2, 128:256], tail[2:3, :]], axis=1),
    )
    outs, totals = [], []
    for h in range(2):
        z = nt_dot(q_ref[h], keys) + biases[h]
        loss = jnp.log(1.0 + jnp.exp(z))
        if diagonal:
            causal = lax.broadcasted_iota(jnp.int32, z.shape, 1) < lax.broadcasted_iota(
                jnp.int32, z.shape, 0
            )
            masked = jnp.where(causal, loss, 0.0)
        else:
            masked = loss
        later = nn_dot(masked.astype(BF16), later_ref[...])
        weights = jnp.exp((z - loss) - later)
        if diagonal:
            weights = jnp.where(causal, weights, 0.0)
        outs.append(nn_dot(weights.astype(BF16), values))
        totals.append(later[:, 0:1] + masked[:, 0:1])
    low = lanes_low((rows, 128))
    return jnp.where(low, outs[0], outs[1]), jnp.where(low, totals[0], totals[1])


def first_kernel(q_ref, payload_ref, later_ref, acc_ref, tot_ref):
    out, total = score_block(q_ref, payload_ref, later_ref, True)
    acc_ref[...] = out
    tot_ref[...] = total


def entering_state(payload_ref, tab_ref, carry_ref, power):
    rows = payload_ref.shape[0] - 16
    tail = payload_ref[rows : rows + 16, :].astype(F32)
    er, ei = tail[8:10] + tail[12:14], tail[10:12] + tail[14:16]
    wr, wi = tab_ref[4 * power : 4 * power + 2, :], tab_ref[4 * power + 2 : 4 * power + 4, :]
    carry_ref[0:2, :] += wr * er - wi * ei
    carry_ref[2:4, :] += wr * ei + wi * er


def step_kernel(
    place_ref, q_ref, later_ref, tab_ref, up_ref, down_ref,
    acc_in, tot_in, wrap_in, carry_in, acc_ref, tot_ref, wrap_ref, carry_ref, *, step, blocks, ups,
):
    here = place_ref[0]
    acc_ref[...] = acc_in[...]
    tot_ref[...] = tot_in[...]
    wrap_ref[...] = wrap_in[...]
    carry_ref[...] = carry_in[...]
    if step <= ups:

        @pl.when(here >= step)
        def _():
            out, total = score_block(q_ref, up_ref, later_ref, False)
            acc_ref[...] += out * jnp.exp(-tot_ref[...])
            tot_ref[...] += total
            entering_state(up_ref, tab_ref, carry_ref, step - 1)

    if step < blocks - ups:

        @pl.when(here >= blocks - step)
        def _():
            out, total = score_block(q_ref, down_ref, later_ref, False)
            wrap_ref[...] = wrap_ref[...] * jnp.exp(-total) + out
            entering_state(down_ref, tab_ref, carry_ref, blocks - 1 - step)


def last_kernel(*refs, **sizes):
    ins, (rest, out_ref, acc_ref, tot_ref, wrap_ref, carry_ref, states_ref) = (
        refs[:10],
        (refs[10:14], *refs[14:]),
    )
    step_kernel(*ins, acc_ref, tot_ref, wrap_ref, carry_ref, **sizes)
    finish_kernel(acc_ref, tot_ref, wrap_ref, carry_ref, *rest, out_ref, states_ref)


def finish_kernel(
    acc_ref, tot_ref, wrap_ref, carry_ref, y_ref, chunk_ref, wide_ref, reads_ref,
    out_ref, states_ref,
):
    rows = acc_ref.shape[0]
    width = states_ref.shape[1] // 2
    sr = jnp.concatenate([carry_ref[0:1, :], carry_ref[1:2, :]], axis=1)
    si = jnp.concatenate([carry_ref[2:3, :], carry_ref[3:4, :]], axis=1)
    zr, zi = cmul(chunk_ref[:, :width], chunk_ref[:, width:], sr, si)
    lr = jnp.broadcast_to(wide_ref[0:1, :width], (8, width))
    li = jnp.broadcast_to(wide_ref[0:1, width:], (8, width))

    def step(k, carried):
        zr, zi = carried
        at = pl.multiple_of(k * 8, 8)
        states_ref[pl.ds(at, 8), :width] = zr
        states_ref[pl.ds(at, 8), width:] = zi
        return cmul(lr, li, zr, zi)

    lax.fori_loop(0, rows // 8, step, (zr, zi), unroll=8)
    mixed = y_ref[...] + read_states(states_ref, *read_matrices(reads_ref, width))
    state_out = jax.nn.gelu(mixed).astype(BF16)
    state_out = nn_dot(reorder_matrix(rows, 8, True), state_out).astype(BF16)
    attended = acc_ref[...] + wrap_ref[...] * jnp.exp(-tot_ref[...])
    low = lanes_low(attended.shape)
    square = attended * attended
    first = jnp.sum(jnp.where(low, square, 0.0), axis=1, keepdims=True)
    second = jnp.sum(jnp.where(low, 0.0, square), axis=1, keepdims=True)
    scale = jnp.where(
        low,
        lax.rsqrt(first * (1.0 / HEAD_DIM) + EPSILON),
        lax.rsqrt(second * (1.0 / HEAD_DIM) + EPSILON),
    )
    attn_out = (attended * scale).astype(BF16)
    out_ref[:, 0:128] = state_out
    out_ref[:, 128:256] = attn_out


def call(kernel, outs, args, scratch=(), smem=0, flops=1, aliases={}, limit=16):
    return pl.pallas_call(
        kernel,
        out_shape=outs,
        in_specs=[SMEM] * smem + [VMEM] * (len(args) - smem),
        out_specs=jax.tree.map(lambda _: VMEM, outs),
        scratch_shapes=list(scratch),
        input_output_aliases=aliases,
        compiler_params=pltpu.CompilerParams(vmem_limit_bytes=limit * 2**20),
        cost_estimate=pl.CostEstimate(flops=flops, bytes_accessed=10**6, transcendentals=0),
    )(*args)


def shape(dims, dtype=F32):
    return jax.ShapeDtypeStruct(dims, dtype)


def on_device(
    tokens,
    norm_gain,
    w_input,
    w_query,
    w_key,
    w_value,
    query_gain,
    key_gain,
    key_bias,
    eigen_real,
    eigen_imag,
    log_step,
    input_real,
    input_imag,
    read_real,
    read_imag,
    skip_gain,
    w_out_state,
    w_out_attn,
):
    blocks = lax.axis_size("sp")
    rows = key_bias.shape[0]
    piece = rows // 8
    groups = eigen_real.shape[0]
    width = groups * STATE
    channels = groups * GROUP
    place = jnp.stack([lax.axis_index("sp"), lax.axis_index("tp_1")]).astype(jnp.int32)

    copies = call(
        norm_kernel,
        shape((4, *tokens.shape), BF16),
        (tokens, norm_gain.reshape(1, -1)),
        limit=60,
    )
    mine = lax.all_to_all(copies, "tp_0", 0, 0, tiled=True).reshape(4 * piece, -1)

    w_joined = jnp.concatenate([w_input, w_query, w_key, w_value], axis=1)
    w_out = jnp.concatenate([w_out_state, w_out_attn], axis=0)
    w_out_copies = jnp.broadcast_to(w_out[None], (4, *w_out.shape))
    decay_r, decay_i, drive_r, drive_i = discretize(
        eigen_real, eigen_imag, log_step, input_real, input_imag
    )
    lines = jnp.concatenate(
        [jnp.transpose(part, (2, 0, 1)).reshape(GROUP, width) for part in (drive_r, drive_i)]
    )
    reads = [part.reshape(channels, STATE) for part in (read_real, read_imag)]
    reads = jnp.concatenate([jnp.concatenate([part, part], axis=1) for part in reads])
    decay = jnp.stack([decay_r.reshape(-1), decay_i.reshape(-1)])
    bias8 = jnp.pad(jnp.transpose(key_bias).reshape(-1, 256), ((0, 5), (0, 0)))
    gains = [jnp.tile(g, 2).reshape(1, 128) for g in (query_gain, key_gain)]
    skip = skip_gain.reshape(1, -1)
    decay, lines, reads, w_joined, w_out_copies, bias8, gains, skip, place = (
        lax.optimization_barrier(
            (decay, lines, reads, w_joined, w_out_copies, bias8, gains, skip, place)
        )
    )
    tables = call(
        lambda *refs: prepare_kernel(*refs, blocks=blocks, chunk=piece),
        (
            shape((4 * blocks, width // 2)),
            shape((8, 2 * width)),
            shape((8, 2 * width)),
            shape((rows, rows), BF16),
        ),
        (decay,),
    )
    mine, tables = lax.optimization_barrier((mine, tables))
    tab, chunk, wide, later = tables
    other = lax.ppermute(mine, "tp_1", [(0, 1), (1, 0)])

    found = call(
        half_project_kernel, shape((4 * piece, 512), BF16), (mine, w_joined), flops=10**9
    )
    q, payload, u_perm, init = call(
        project_kernel,
        (
            shape((2, rows, 128), BF16),
            shape((rows + 16, 256), BF16),
            shape((rows, channels), BF16),
            shape((8, 2 * width)),
        ),
        (place, found, other, w_joined, *gains, bias8, lines, wide),
        scratch=(pltpu.VMEM((rows, 512), BF16), pltpu.VMEM((rows, 2 * width), F32)),
        smem=1,
        flops=4 * 10**9,
    )

    u_perm, w_out_copies = lax.optimization_barrier((u_perm, w_out_copies))
    w_out_mine = lax.all_to_all(w_out_copies, "tp_0", 0, 0, tiled=True)
    acc, tot = call(
        first_kernel, (shape((rows, 128)), shape((rows, 128))), (q, payload, later), flops=2 * 10**9
    )
    wrap = jnp.zeros((rows, 128), F32)
    carry = jnp.zeros((8, width // 2), F32)
    up = down = payload
    half = blocks // 2
    for step in range(1, half + 1):
        up = lax.ppermute(up, "sp", [(i - 1, i) for i in range(step, blocks)])
        if step < half:
            hops = [((j - step + 1) % blocks, (j - step) % blocks) for j in range(half - 1)]
            down = lax.ppermute(down, "sp", hops)
        if step == half:
            break
        acc, tot, wrap, carry = call(
            lambda *refs, step=step: step_kernel(*refs, step=step, blocks=blocks, ups=half),
            (shape((rows, 128)), shape((rows, 128)), shape((rows, 128)), shape(carry.shape)),
            (place, q, later, tab, up, down, acc, tot, wrap, carry),
            smem=1,
            flops=3 * 10**9,
            aliases={6: 0, 7: 1, 8: 2, 9: 3},
        )
    acc, u_perm = lax.optimization_barrier((acc, u_perm))
    y_local = call(
        local_state_kernel,
        shape((rows, channels)),
        (u_perm, init, lines, wide, reads, skip),
        scratch=(pltpu.VMEM((rows, 2 * width), F32),),
        flops=2 * 10**9,
    )
    y_local, w_out_mine = lax.optimization_barrier((y_local, w_out_mine))
    w_out_other = lax.ppermute(w_out_mine, "tp_1", [(0, 1), (1, 0)])
    state = [shape((rows, 128)), shape((rows, 128)), shape((rows, 128)), shape(carry.shape)]
    both = call(
        lambda *refs: last_kernel(*refs, step=half, blocks=blocks, ups=half),
        shape((rows, 2 * channels), BF16),
        (place, q, later, tab, up, down, acc, tot, wrap, carry, y_local, chunk, wide, reads),
        scratch=[pltpu.VMEM(s.shape, F32) for s in state]
        + [pltpu.VMEM((rows, 2 * width), F32)],
        smem=1,
        flops=3 * 10**9,
    )
    parts = lax.all_to_all(both.reshape(8, piece, -1), TP, 0, 0, tiled=True)
    return pl.pallas_call(
        merge_kernel,
        out_shape=shape((piece, w_out.shape[1]), BF16),
        in_specs=[SMEM, VMEM, pl.BlockSpec(memory_space=pl.ANY), VMEM],
        out_specs=VMEM,
        scratch_shapes=[
            pltpu.VMEM(w_out_mine.shape, BF16),
            pltpu.SemaphoreType.DMA((w_out_mine.shape[0],)),
        ],
        compiler_params=pltpu.CompilerParams(vmem_limit_bytes=16 * 2**20),
        cost_estimate=pl.CostEstimate(flops=10**9, bytes_accessed=10**7, transcendentals=0),
    )(place, parts, w_out_mine, w_out_other)


def solution(mesh):
    torus = Mesh(
        mesh.devices.reshape(mesh.shape["sp"], mesh.shape["fs"], 4, 2), ("sp", "fs", "tp_0", "tp_1")
    )
    placed = (
        P(FS_SP_TP, None),
        P(),
        P(None, TP),
        P(None, TP),
        P(None, TP),
        P(None, TP),
        P(),
        P(),
        P(("fs", "sp"), TP),
        P(TP, None),
        P(TP, None),
        P(TP),
        P(TP, None, None),
        P(TP, None, None),
        P(TP, None, None),
        P(TP, None, None),
        P(TP),
        P(TP, None),
        P(TP, None),
    )

    return jax.shard_map(
        on_device, mesh=torus, in_specs=placed, out_specs=P(FS_SP_TP, None), check_vma=False
    )
```
